32 devices in a mesh: sp: 8 (over z, y), tp: 4 (over x, core).
Axes of the slice: x: 2, y: 2, z: 4, core: 2. Of those that a mesh axis runs over, the one named last changes fastest.
Arguments:
- cotangent: bfloat16 [2048, 2048], P('sp'), may hold values from -6 to 6
- stream_in: bfloat16 [2048, 2048], P('sp'), may hold values from -6 to 6
- norm_gain: float32 [2048], replicated, may hold values from 0.1 to 1.9
- out_gate: bfloat16 [2048, 1024], P('sp', 'tp'), may hold values from -6 to 6
- in_gate: bfloat16 [2048, 1024], P('sp', 'tp'), may hold values from -6 to 6
- conv_input: bfloat16 [2048, 1024], P('sp', 'tp'), may hold values from -6 to 6
- conv_taps: float32 [3, 1024], P(None, 'tp'), may hold values from -3 to 3
- out_weight: bfloat16 [2048, 1024], P(None, 'tp'), may hold values from -0.1875 to 0.1875
- expert_gate: bfloat16 [8, 2048, 1024], P('sp', None, 'tp'), may hold values from -0.125 to 0.125
- expert_up: bfloat16 [8, 2048, 1024], P('sp', None, 'tp'), may hold values from -0.125 to 0.125
- expert_down: bfloat16 [8, 1024, 2048], P('sp', 'tp'), may hold values from -0.1875 to 0.1875
- expert_choice: int32 [2048, 2], P('sp'), may hold values from 0 to 7, all different within a row; in each aligned block of 256 rows (0 to 255, 256 to 511, ...) at most 128 rows name the same one
- route_scale: float32 [2048, 2], P('sp'), may hold values from 0.05 to 0.6
Outputs:
- grad_stream: bfloat16 [2048, 2048], P('sp', 'tp')
- grad_out_gate: bfloat16 [2048, 1024], P('sp', 'tp')
- grad_in_gate: bfloat16 [2048, 1024], P('sp', 'tp')
- grad_conv_input: bfloat16 [2048, 1024], P('sp', 'tp')
- grad_out_weight: float32 [2048, 1024], P('sp', 'tp')
- grad_expert_gate: float32 [8, 2048, 1024], P('sp', None, 'tp')
- grad_expert_up: float32 [8, 2048, 1024], P('sp', None, 'tp')
- grad_expert_down: float32 [8, 1024, 2048], P('sp', 'tp')
The draws below stay inside these ranges and needn't reach their ends.
Inputs may be any that keep to these rules, and one draw needn't show every extreme that they name: `expert_choice`: each row names two different experts. Within the rows of one device no expert is named more than 128 times, a bound that some block reaches in some devices' rows.
All inputs are finite; a program needn't handle non-finite values.
Results may differ from the reference program's by a relative error of at most 0.01.
Values may be sent and summed in bfloat16 or wider, within the bound.
A program may use at most 128 MiB of HBM per device.

```python
import math
import jax
import jax.numpy as jnp
import numpy as np
from jax import lax

D = 2048
CW = 1024
FF = 1024
TAPS = 3
TOK_DEV = 256
TOKENS = 2048
EXPERTS = 8
CAP = 128
N_SP = 8
N_TP = 4


def raised(drawn, rng, source, target, shards_of, factor):
    def block_of(dim):
        return (jnp.arange(drawn.shape[dim]) // (drawn.shape[dim] // shards_of)).reshape((-1,) + (1,) * (drawn.ndim - 1 - dim))

    first = jax.random.permutation(rng, shards_of)[block_of(target)]
    other_side = (block_of(target) + shards_of // 2) % shards_of
    return jnp.where((block_of(source) == first) | (block_of(source) == other_side), factor * drawn, drawn)


def shard_levels(rng, dims, cuts, low, top_value):
    def one(axis_at, blocks):
        heights = jax.random.uniform(jax.random.fold_in(jax.random.fold_in(rng, 6), axis_at), (blocks,), jnp.float32, low / len(cuts), top_value / len(cuts))
        return jnp.repeat(jnp.exp(heights), dims[axis_at] // blocks).reshape((-1,) + (1,) * (len(dims) - axis_at - 1))

    factor_of = one(*cuts[0])
    for cut in cuts[1:]:
        factor_of = factor_of * one(*cut)
    return factor_of


def deal_out(key, own, number, rows, count, top, reach, slope):
    sequence = jax.random.permutation(key, count)
    heavy_load, common = load_shares(count, rows * top, reach, slope, True), load_shares(count, rows * top, reach, slope, False)
    places = jnp.arange(count)

    def named(lengths, offset_by):
        used = int((lengths > 0).sum())
        fixed = max(1, used // 4)
        passed = fixed + (places - fixed + offset_by * (used - fixed)) % max(1, count - fixed)
        return jnp.zeros((count,), jnp.int32).at[sequence[jnp.where(places < fixed, places, passed)]].set(jnp.asarray(lengths, jnp.int32))

    lengths = jnp.where(number % 4 == 0, named(heavy_load, number // 4), named(common, number - number // 4 - 1))
    mixed = jax.random.permutation(jax.random.fold_in(own, 3), count)
    source_of, sink = mixed[0:count // 2 * 2:2], mixed[1:count // 2 * 2:2]
    slack = jnp.minimum(lengths[source_of] - 1, reach - lengths[sink]) // 2
    slack = jnp.where((source_of == sequence[0]) | (sink == sequence[0]) | (lengths[sink] == 0), 0, jnp.maximum(slack, 0))
    passed = jax.random.randint(jax.random.fold_in(own, 4), (count // 2,), 0, 1 << 20) % (slack + 1)
    lengths = lengths.at[source_of].add(-passed).at[sink].add(passed)
    members = jnp.searchsorted(jnp.cumsum(lengths), jnp.arange(rows * top), side="right").astype(jnp.int32)
    grid = members.reshape(top, rows).T
    grid = grid[jax.random.permutation(jax.random.fold_in(own, 1), rows)]
    offset_by = jax.random.randint(jax.random.fold_in(own, 2), (rows, 1), 0, top)
    return jnp.take_along_axis(grid, (jnp.arange(top)[None, :] + offset_by) % top, axis=1)


def load_shares(number_of, total, most, slope, full):
    loads = [(1 << 20) // math.isqrt(standing ** slope) + 1 for standing in range(1, number_of + 1)]
    largest = most if full else min(most, max(-(-total // number_of), total * loads[0] // sum(loads)))
    least = 1 if total - largest >= number_of - 1 else 0
    holding, surplus = [largest] + [least] * (number_of - 1), total - largest - least * (number_of - 1)
    while surplus > 0:
        free = [i for i in range(1, number_of) if holding[i] < largest] or [i for i in range(1, number_of) if holding[i] < most]
        pool, left = sum([loads[i] for i in free]), surplus
        for i in free:
            more = min(most - holding[i], max(1, left * loads[i] // pool), surplus)
            holding[i] = holding[i] + more
            surplus = surplus - more
    return np.array(holding)


def normal_values(rng, shape, spread, reach, cuts=(), kind=jnp.bfloat16):
    array = spread * jax.random.normal(rng, shape, jnp.float32)
    if cuts:
        array = array * shard_levels(rng, shape, cuts, -0.22, 0.18)
    return jnp.clip(array, -reach, reach).astype(kind)


def gaussian_with(own_key, extent, width, most, pieces, heavy, kind=jnp.bfloat16):
    values = width * jax.random.normal(own_key, extent, jnp.float32)
    if pieces:
        values = values * shard_levels(own_key, extent, pieces, -0.22, 0.18)
    return jnp.clip(raised(values, jax.random.fold_in(own_key, 3), *heavy), -most, most).astype(kind)


def setup_inputs(seed: int = 0) -> dict:
    streams_of = jax.random.split(jax.random.key(seed), 14)
    cotangent = gaussian_with(streams_of[0], (TOKENS, D), 1.0, 6.0, ((0, 8),), (0, 1, 8, 2.0))
    stream_in = normal_values(streams_of[1], (TOKENS, D), 1.0, 6.0, ((0, 8),))
    norm_gain = jnp.clip(1.0 + 0.18 * jax.random.normal(streams_of[2], (D,), jnp.float32), 0.1, 1.9)
    out_gate = normal_values(streams_of[3], (TOKENS, CW), 1.0, 6.0, ((0, 8), (1, 4)))
    in_gate = normal_values(streams_of[4], (TOKENS, CW), 1.0, 6.0, ((0, 8), (1, 4)))
    conv_input = normal_values(streams_of[5], (TOKENS, CW), 1.0, 6.0, ((0, 8), (1, 4)))
    conv_taps = normal_values(streams_of[6], (TAPS, CW), 0.577, 3.0, ((1, 4),), jnp.float32)
    out_weight = normal_values(streams_of[7], (D, CW), CW ** -0.5, 0.1875, ((1, 4),))
    expert_gate = normal_values(streams_of[8], (EXPERTS, D, FF), D ** -0.5, 0.125, ((0, 8), (2, 4)))
    expert_up = normal_values(streams_of[9], (EXPERTS, D, FF), D ** -0.5, 0.125, ((0, 8), (2, 4)))
    expert_down = normal_values(streams_of[10], (EXPERTS, FF, D), FF ** -0.5, 0.1875, ((0, 8), (1, 4)))
    expert_choice_keys = jax.random.split(jax.random.fold_in(streams_of[11], 1), TOKENS // TOK_DEV)
    expert_choice_turns = jax.random.permutation(jax.random.fold_in(streams_of[11], 3), TOKENS // TOK_DEV)
    expert_choice = jax.vmap(lambda own, number: deal_out(jax.random.fold_in(streams_of[11], 2), own, number, TOK_DEV, EXPERTS, 2, CAP, 2))(expert_choice_keys, expert_choice_turns).reshape((TOKENS, 2))
    route_scale = jnp.clip(0.05 + 0.55 * jax.random.uniform(streams_of[12], (TOKENS, 2), jnp.float32) ** shard_levels(streams_of[12], (TOKENS, 2), ((0, 8),), -0.2, 0.2), 0.05, 0.6)
    return {"cotangent": cotangent, "stream_in": stream_in, "norm_gain": norm_gain, "out_gate": out_gate, "in_gate": in_gate, "conv_input": conv_input, "conv_taps": conv_taps, "out_weight": out_weight, "expert_gate": expert_gate, "expert_up": expert_up, "expert_down": expert_down, "expert_choice": expert_choice, "route_scale": route_scale}


norm_eps = 1e-06

def slot_table(choice_rows, expert_count, capacity):
    flat_ids = choice_rows.reshape(-1).astype(jnp.int32)
    route_count = flat_ids.shape[0]
    onehot = (flat_ids[:, None] == jnp.arange(expert_count, dtype=jnp.int32)[None, :]).astype(jnp.int32)
    earlier = jnp.cumsum(onehot, axis=0) - onehot
    position = lax.optimization_barrier(jnp.sum(earlier * onehot, axis=1)).astype(jnp.int32)
    slot_of_route = (flat_ids * capacity + position).astype(jnp.int32)
    route_of_slot = jnp.full((expert_count * capacity,), route_count, jnp.int32)
    route_of_slot = route_of_slot.at[slot_of_route].set(jnp.arange(route_count, dtype=jnp.int32))
    return (slot_of_route, route_of_slot)

def rows_product(left, right):
    return lax.dot_general(left, right, (((0,), (0,)), ((), ())), preferred_element_type=jnp.float32)

def cols_product(left, right):
    return lax.dot_general(left, right, (((1,), (1,)), ((), ())), preferred_element_type=jnp.float32)

def reference(cotangent, stream_in, norm_gain, out_gate, in_gate, conv_input, conv_taps, out_weight, expert_gate, expert_up, expert_down, expert_choice, route_scale):
    stream = stream_in.astype(jnp.float32)
    inverse_rms = lax.rsqrt(lax.optimization_barrier(jnp.mean(stream * stream, axis=-1, keepdims=True)) + norm_eps)
    unit_stream = stream * inverse_rms
    normed = (unit_stream * norm_gain.astype(jnp.float32)).astype(jnp.bfloat16)
    capacity = 4 * TOK_DEV // N_SP
    route_count = 2 * TOK_DEV
    block_ids = expert_choice.reshape(N_SP, TOK_DEV, 2)
    tables = jax.vmap(lambda choice_block: slot_table(choice_block, EXPERTS, capacity)[1])(block_ids)
    flat_scale = route_scale.reshape(-1)
    source_base = (jnp.arange(N_SP, dtype=jnp.int32) * route_count)[:, None]
    width_tp = FF // N_TP

    def expert_step(accum, inputs):
        w_gate, w_up, w_down, expert = inputs
        chosen = lax.dynamic_slice_in_dim(tables, (expert * capacity).astype(jnp.int32), capacity, 1)
        present = chosen < route_count
        routes = (source_base + jnp.where(present, chosen, 0)).reshape(-1).astype(jnp.int32)
        present = present.reshape(-1)
        token = (routes // 2).astype(jnp.int32)
        weight = jnp.where(present, flat_scale[routes], jnp.zeros((), jnp.float32))
        scaled_cot = (cotangent[token].astype(jnp.float32) * weight[:, None]).astype(jnp.bfloat16)
        expert_rows = jnp.where(present[:, None], normed[token], jnp.zeros((), jnp.bfloat16))
        gate_pre = jnp.dot(expert_rows, w_gate, preferred_element_type=jnp.float32)
        up_pre = jnp.dot(expert_rows, w_up, preferred_element_type=jnp.float32)
        sigmoid_gate = jax.nn.sigmoid(gate_pre)
        silu_gate = gate_pre * sigmoid_gate
        hidden = (silu_gate * up_pre).astype(jnp.bfloat16)
        grad_down = rows_product(hidden, scaled_cot)
        hidden_grad = cols_product(scaled_cot, w_down)
        gate_grad = (hidden_grad * up_pre * sigmoid_gate * (1.0 + gate_pre * (1.0 - sigmoid_gate))).astype(jnp.bfloat16)
        up_grad = (hidden_grad * silu_gate).astype(jnp.bfloat16)
        grad_gate = rows_product(expert_rows, gate_grad)
        grad_up = rows_product(expert_rows, up_grad)
        slot_rows = expert_rows.shape[0]
        shares = jnp.einsum('rpf,dpf->prd', gate_grad.astype(jnp.float32).reshape(slot_rows, N_TP, width_tp), w_gate.astype(jnp.float32).reshape(D, N_TP, width_tp))
        shares = shares + jnp.einsum('rpf,dpf->prd', up_grad.astype(jnp.float32).reshape(slot_rows, N_TP, width_tp), w_up.astype(jnp.float32).reshape(D, N_TP, width_tp))
        rounded = lax.optimization_barrier(shares.astype(jnp.bfloat16))
        slot_grad = lax.optimization_barrier(jnp.sum(rounded.astype(jnp.float32), axis=0)).astype(jnp.bfloat16)
        slot_grad = lax.optimization_barrier(slot_grad)
        accum = accum.at[token].add(jnp.where(present[:, None], slot_grad.astype(jnp.float32), jnp.zeros((), jnp.float32)))
        return (accum, (grad_gate, grad_up, grad_down))
    start_accum = jnp.zeros((TOKENS, D), jnp.float32)
    accum, grads = lax.scan(expert_step, start_accum, (expert_gate, expert_up, expert_down, jnp.arange(EXPERTS, dtype=jnp.int32)))
    grad_gate, grad_up, grad_down = grads
    token_grad = lax.optimization_barrier(accum.astype(jnp.bfloat16))
    unit_grad = token_grad.astype(jnp.float32) * norm_gain.astype(jnp.float32)
    along = lax.optimization_barrier(jnp.mean(unit_stream * unit_grad, axis=-1, keepdims=True))
    stream_grad = (cotangent.astype(jnp.float32) + inverse_rms * (unit_grad - unit_stream * along)).astype(jnp.bfloat16)
    taps = conv_taps.astype(jnp.float32)
    product = in_gate.astype(jnp.float32) * conv_input.astype(jnp.float32)
    padded = jnp.pad(product, ((2, 0), (0, 0)))
    filtered = taps[0] * product + taps[1] * padded[1:-1] + taps[2] * padded[:-2]
    mixed_in = (out_gate.astype(jnp.float32) * filtered).astype(jnp.bfloat16)
    mixed_grad = jnp.dot(stream_grad, out_weight, preferred_element_type=jnp.float32)
    grad_out_gate = (mixed_grad * filtered).astype(jnp.bfloat16)
    filtered_grad = mixed_grad * out_gate.astype(jnp.float32)
    padded_grad = jnp.pad(filtered_grad, ((0, 2), (0, 0)))
    product_grad = taps[0] * filtered_grad + taps[1] * padded_grad[1:-1] + taps[2] * padded_grad[2:]
    grad_in_gate = (product_grad * conv_input.astype(jnp.float32)).astype(jnp.bfloat16)
    grad_conv_input = (product_grad * in_gate.astype(jnp.float32)).astype(jnp.bfloat16)
    grad_out_weight = rows_product(stream_grad, mixed_in)
    return (stream_grad, grad_out_gate, grad_in_gate, grad_conv_input, grad_out_weight, grad_gate, grad_up, grad_down)
```

```python
import functools

import jax
import jax.numpy as jnp
from jax import lax
from jax.experimental import pallas as pl
from jax.experimental.pallas import tpu as pltpu
from jax.sharding import PartitionSpec as P

norm_eps = 1e-06


def passed_along(value, axis, steps):
    count = lax.axis_size(axis)
    first, last = (max(0, -steps), min(count, count - steps))
    return lax.ppermute(value, axis, [(source, source + steps) for source in range(first, last)])


def rows_product(left, right):
    return lax.dot_general(
        left, right, (((0,), (0,)), ((), ())), preferred_element_type=jnp.float32
    )


def cols_product(left, right):
    return lax.dot_general(
        left, right, (((1,), (1,)), ((), ())), preferred_element_type=jnp.float32
    )


MESH = pl.DeviceIdType.MESH


def remote(source, target, send_sem, recv_sem, device):
    return pltpu.make_async_remote_copy(
        src_ref=source,
        dst_ref=target,
        send_sem=send_sem,
        recv_sem=recv_sem,
        device_id=device,
        device_id_type=MESH,
    )


def columns(index, width):
    return pl.ds(pl.multiple_of(index * width, width), width)


def mirrored(me, mask, n):
    found, unit = 0, 1
    while unit < n:
        found = found + lax.rem(lax.div(me, unit) + lax.div(mask, unit), 2) * unit
        unit = 2 * unit
    return found


def tp_places():
    tp, count = lax.axis_index("tp"), lax.axis_size("tp")
    cross = lax.rem(tp + count // 2, count)
    partner = tp + 1 - 2 * lax.rem(tp, 2)
    return (tp, cross, partner, lax.rem(partner + count // 2, count))


def greet(cross, partner):
    barrier = pltpu.get_barrier_semaphore()
    for peer in (cross, partner):
        pl.semaphore_signal(barrier, inc=1, device_id={"tp": peer}, device_id_type=MESH)
    me, n = lax.axis_index("sp"), lax.axis_size("sp")

    def greet_one(k, carry):
        peer = lax.rem(me + k, n)
        pl.semaphore_signal(barrier, inc=1, device_id={"sp": peer}, device_id_type=MESH)
        return carry

    lax.fori_loop(1, n, greet_one, 0)
    return lambda: pl.semaphore_wait(barrier, n + 1)


def loop(low, high, body):
    def step(k, carry):
        body(k)
        return carry

    lax.fori_loop(low, high, step, 0)


def experts_kernel(
    n,
    normed,
    cot,
    route,
    w_gate,
    w_up,
    w_down,
    token,
    rows_out,
    cots_out,
    hidden_out,
    gate_out,
    up_out,
    keys,
    weights,
    arrived,
    arrived_route,
    sending,
    slots,
    hidden,
    gate_grad,
    up_grad,
    partial,
    near,
    far_out,
    far_in,
    total,
    back,
    acc,
    tok_send,
    tok_recv,
    slot_send,
    slot_recv,
    cross_send,
    cross_recv,
    near_send,
    fwd_send,
    near_recv,
    hand_send,
    hand_recv,
    far_send,
    far_recv,
    out_send,
    out_recv,
    all_send,
    all_cross,
    all_near,
    local,
):
    me = lax.axis_index("sp")
    tp, cross, partner, diagonal = tp_places()
    half = n // 2
    count, wide = normed.shape
    width = acc.shape[1]
    depth = near.shape[1] // n
    group = max(1, 256 // depth)
    span = group * depth
    wait_all = greet(cross, partner)
    sources = (normed, cot)

    def other(s):
        return mirrored(me, jnp.int32(s), n)

    def at(s):
        return pl.ds(pl.multiple_of(s * depth, depth), depth)

    def table(which, source):
        c0, c1, s0, s1 = (source[i : i + 1, :] for i in range(4))
        expert = lax.broadcasted_iota(jnp.int32, (n, count), 0).astype(jnp.float32)
        first, second = (c0 == expert, c1 == expert)
        member = jnp.where(first | second, 1.0, 0.0)
        row = lax.broadcasted_iota(jnp.int32, (count, count), 0)
        column = lax.broadcasted_iota(jnp.int32, (count, count), 1)
        before = jnp.where(row < column, 1.0, 0.0).astype(jnp.bfloat16)
        earlier = jnp.dot(
            member.astype(jnp.bfloat16), before, preferred_element_type=jnp.float32
        )
        keys[which] = jnp.where(member > 0.0, earlier, -1.0)
        weights[which] = jnp.where(first, s0, 0.0) + jnp.where(second, s1, 0.0)

    def placing(which, expert):
        slot = lax.broadcasted_iota(jnp.int32, (depth, count), 0).astype(jnp.float32)
        return slot == keys[which, pl.ds(expert, 1), :]

    def chosen(a, which, expert, values):
        mask = placing(which, expert)
        found = jnp.dot(
            jnp.where(mask, 1.0, 0.0).astype(jnp.bfloat16),
            values,
            preferred_element_type=jnp.float32,
        )
        if a == 1:
            weight = jnp.where(mask, weights[which, pl.ds(expert, 1), :], 0.0)
            found = found * jnp.sum(weight, axis=1, keepdims=True)
        return found.astype(jnp.bfloat16)

    def token_copy(a):
        return remote(
            sources[a].at[:, columns(tp, width)],
            arrived.at[a],
            tok_send.at[a],
            tok_recv.at[a],
            {"sp": other(half)},
        )

    def route_copy():
        return remote(route, arrived_route, tok_send.at[2], tok_recv.at[2], {"sp": other(half)})

    def slot_copy(a, s, k):
        return remote(
            sending.at[a, at(s)],
            slots.at[a, at(s), columns(tp, width)],
            slot_send.at[a],
            slot_recv.at[a, s],
            {"sp": other(k)},
        )

    def spread(a, s):
        block = slots.at[a, at(s), columns(tp, width)]
        remote(block, block, cross_send.at[a], cross_recv.at[a, s], {"tp": cross}).start()
        remote(block, block, near_send.at[a], near_recv.at[a, s], {"tp": partner}).start()

    def forward(a, s):
        block = slots.at[a, at(s), columns(cross, width)]
        remote(block, block, cross_send.at[a], cross_recv.at[a, s], {"tp": cross}).wait_recv()
        remote(block, block, fwd_send.at[a], near_recv.at[a, s], {"tp": partner}).start()

    def ready(s):
        for a in (0, 1):
            both = slots.at[a, at(s), pl.ds(0, 2 * width)]
            remote(both, both, near_send.at[a], near_recv.at[a, s], {"tp": partner}).wait_recv()

    def hand(j, s):
        return remote(
            partial.at[at(s), columns((partner, diagonal)[j], width)],
            near.at[j, at(s)],
            hand_send.at[j],
            hand_recv.at[j, s],
            {"tp": partner},
        )

    def across(s):
        return remote(
            far_out.at[at(s)], far_in.at[at(s)], far_send, far_recv.at[s], {"tp": cross}
        )

    def give(s):
        return remote(
            total.at[at(s)], back.at[at(s)], out_send, out_recv.at[s], {"sp": other(s)}
        )

    table(0, route)
    wait_all()
    token_copy(0).start()
    route_copy().start()
    token_copy(1).start()

    def send_own(k):
        for a in (0, 1):
            values = sources[a][:, columns(tp, width)]
            sending[a, at(k), :] = chosen(a, 0, other(k), values)
            slot_copy(a, k, k).start()

    loop(1, half, send_own)
    for a in (0, 1):
        for piece in range(wide // width):
            where = pl.ds(piece * width, width)
            slots[a, pl.ds(0, depth), where] = chosen(a, 0, me, sources[a][:, where])

    def land(s, k):
        for a in (0, 1):
            slot_copy(a, s, k).wait_recv()
            spread(a, s)

    def land_own(k):
        land(k, k)

    loop(1, half, land_own)
    for a in (0, 1):
        if a == 0:
            route_copy().wait_recv()
            table(1, arrived_route)
        token_copy(a).wait_recv()

        def send_other(k):
            sending[a, at(half + k), :] = chosen(a, 1, other(k), arrived[a])
            slot_copy(a, half + k, k).start()

        loop(1, half, send_other)
        slots[a, at(half), columns(tp, width)] = chosen(a, 1, me, arrived[a])
        spread(a, half)

    def forward_both(s):
        for a in (0, 1):
            forward(a, s)

    loop(1, half, forward_both)

    def compute(g):
        rows = pl.ds(pl.multiple_of(g * span, span), span)
        picked, scaled = (slots[0, rows, :], slots[1, rows, :])
        gate_pre = jnp.dot(picked, w_gate[...], preferred_element_type=jnp.float32)
        up_pre = jnp.dot(picked, w_up[...], preferred_element_type=jnp.float32)
        hidden_grad = cols_product(scaled, w_down[...])
        sigmoid_gate = jax.nn.sigmoid(gate_pre)
        silu_gate = gate_pre * sigmoid_gate
        hidden[rows, :] = (silu_gate * up_pre).astype(jnp.bfloat16)
        gate = (
            hidden_grad * up_pre * sigmoid_gate * (1.0 + gate_pre * (1.0 - sigmoid_gate))
        ).astype(jnp.bfloat16)
        up = (hidden_grad * silu_gate).astype(jnp.bfloat16)
        gate_grad[rows, :] = gate
        up_grad[rows, :] = up
        for piece in range(wide // width):
            where = pl.ds(piece * width, width)
            partial[rows, where] = (
                cols_product(gate, w_gate[where, :]) + cols_product(up, w_up[where, :])
            ).astype(jnp.bfloat16)
        for kind, (source, target) in enumerate(kept):
            pltpu.make_async_copy(source.at[rows, :], target.at[rows, :], local.at[kind]).start()

    kept = (
        (slots.at[0], rows_out),
        (slots.at[1], cots_out),
        (hidden, hidden_out),
        (gate_grad, gate_out),
        (up_grad, up_out),
    )

    def work(g):
        def await_one(i):
            s = g * group + i
            @pl.when(s > 0)
            def _():
                ready(s)

        loop(0, group, await_one)
        compute(g)

        def hand_one(i):
            s = g * group + i
            hand(1, s).start()
            hand(0, s).start()

        loop(0, group, hand_one)

    groups = n // group
    loop(0, groups // 2, work)

    def land_other(k):
        land(half + k, k)

        @pl.when(k == 1)
        def _():
            forward_both(half)

        @pl.when(k > 1)
        def _():
            forward_both(half + k - 1)

    loop(1, half, land_other)

    def pair(s):
        hand(1, s).wait_recv()
        mine = partial[at(s), columns(cross, width)].astype(jnp.float32)
        far_out[at(s), :] = (mine + near[1, at(s), :].astype(jnp.float32)).astype(jnp.bfloat16)
        across(s).start()

    loop(0, half, pair)
    forward_both(n - 1)
    loop(groups // 2, groups, work)
    loop(half, n, pair)

    def finish(s):
        hand(0, s).wait_recv()
        across(s).wait_recv()
        mine = partial[at(s), columns(tp, width)].astype(jnp.float32)
        return (
            mine + near[0, at(s), :].astype(jnp.float32) + far_in[at(s), :].astype(jnp.float32)
        ).astype(jnp.bfloat16)

    def finish_one(s):
        total[at(s), :] = finish(s)
        give(s).start()

    loop(1, n, finish_one)
    back[pl.ds(0, depth), :] = finish(0)
    acc[...] = jnp.zeros_like(acc)

    def combine(s):
        @pl.when(s > 0)
        def _():
            give(s).wait_recv()

        mask = jnp.where(placing(0, other(s)), 1.0, 0.0).astype(jnp.bfloat16)
        acc[...] += rows_product(mask, back[at(s), :])

    loop(0, n, combine)
    pieces = all_cross.shape[0]
    tall = count // pieces

    def shared(i, column, send, recv, peer):
        block = token.at[pl.ds(i * tall, tall), columns(column, width)]
        return remote(block, block, send, recv, {"tp": peer})

    token[:, columns(tp, width)] = acc[...].astype(jnp.bfloat16)
    for i in range(pieces):
        shared(i, tp, all_send.at[0, i], all_cross.at[i], cross).start()
        shared(i, tp, all_send.at[1, i], all_near.at[0, i], partner).start()
    for i in range(pieces):
        shared(i, cross, all_send.at[0, i], all_cross.at[i], cross).wait_recv()
        shared(i, cross, all_send.at[2, i], all_near.at[1, i], partner).start()
    for i in range(pieces):
        for j in (0, 1):
            shared(i, tp, all_send.at[j + 1, i], all_near.at[j, i], partner).wait()
        shared(i, tp, all_send.at[0, i], all_cross.at[i], cross).wait_send()
    route_copy().wait_send()
    for a in (0, 1):
        token_copy(a).wait_send()
        sent = sending.at[a, pl.ds(0, (n - 2) * depth)]
        remote(sent, sent, slot_send.at[a], slot_recv.at[a, 0], {"tp": partner}).wait_send()
        most = slots.at[a, pl.ds(0, (n - 1) * depth), pl.ds(0, width)]
        for sem in (cross_send, near_send, fwd_send):
            remote(most, most, sem.at[a], near_recv.at[a, 0], {"tp": partner}).wait_send()
        remote(far_out, far_in, hand_send.at[a], hand_recv.at[a, 0], {"tp": partner}).wait_send()
    remote(far_out, far_in, far_send, far_recv.at[0], {"tp": cross}).wait_send()
    rest = total.at[pl.ds(0, (n - 1) * depth)]
    remote(rest, rest, out_send, out_recv.at[0], {"tp": partner}).wait_send()
    for kind, (source, target) in enumerate(kept):
        pltpu.make_async_copy(source, target, local.at[kind]).wait()


def experts(normed, cot, route, w_gate, w_up, w_down, n):
    count, wide = normed.shape
    hidden = w_gate.shape[1]
    width = wide // lax.axis_size("tp")
    depth = 4 * count // n
    rows = n * depth
    pieces = 2
    kind = normed.dtype

    def out(*shape):
        return jax.ShapeDtypeStruct(shape, kind)

    vmem, anywhere = (pl.BlockSpec(memory_space=pltpu.VMEM), pl.BlockSpec(memory_space=pl.ANY))
    dma = pltpu.SemaphoreType.DMA
    return pl.pallas_call(
        functools.partial(experts_kernel, n),
        out_shape=[
            out(count, wide),
            out(rows, wide),
            out(rows, wide),
            out(rows, hidden),
            out(rows, hidden),
            out(rows, hidden),
        ],
        in_specs=[vmem] * 6,
        out_specs=[vmem] + [anywhere] * 5,
        scratch_shapes=[
            pltpu.VMEM((2, n, count), jnp.float32),
            pltpu.VMEM((2, n, count), jnp.float32),
            pltpu.VMEM((2, count, width), kind),
            pltpu.VMEM(route.shape, jnp.float32),
            pltpu.VMEM((2, rows, width), kind),
            pltpu.VMEM((2, rows, wide), kind),
            pltpu.VMEM((rows, hidden), kind),
            pltpu.VMEM((rows, hidden), kind),
            pltpu.VMEM((rows, hidden), kind),
            pltpu.VMEM((rows, wide), kind),
            pltpu.VMEM((2, rows, width), kind),
            pltpu.VMEM((rows, width), kind),
            pltpu.VMEM((rows, width), kind),
            pltpu.VMEM((rows, width), kind),
            pltpu.VMEM((rows, width), kind),
            pltpu.VMEM((count, width), jnp.float32),
            dma((3,)),
            dma((3,)),
            dma((2,)),
            dma((2, n)),
            dma((2,)),
            dma((2, n)),
            dma((2,)),
            dma((2,)),
            dma((2, n)),
            dma((2,)),
            dma((2, n)),
            dma,
            dma((n,)),
            dma,
            dma((n,)),
            dma((3, pieces)),
            dma((pieces,)),
            dma((2, pieces)),
            dma((5,)),
        ],
        compiler_params=pltpu.CompilerParams(
            collective_id=1, has_side_effects=True, vmem_limit_bytes=52 * 1024 * 1024
        ),
    )(normed, cot, route, w_gate, w_up, w_down)


def shards(
    cotangent,
    stream_in,
    norm_gain,
    out_gate,
    in_gate,
    conv_input,
    conv_taps,
    out_weight,
    expert_gate,
    expert_up,
    expert_down,
    expert_choice,
    route_scale,
):
    sp_size = lax.axis_size("sp")
    tp_size = lax.axis_size("tp")
    rows_here = stream_in.shape[0]
    model_width = stream_in.shape[1]
    column_width = model_width // tp_size
    column_start = lax.axis_index("tp") * column_width
    stream = stream_in.astype(jnp.float32)
    inverse_rms = lax.rsqrt(jnp.mean(stream * stream, axis=-1, keepdims=True) + norm_eps)
    unit_stream = stream * inverse_rms
    normed = (unit_stream * norm_gain).astype(jnp.bfloat16)
    route = jnp.concatenate(
        [expert_choice.T.astype(jnp.float32), route_scale.T, jnp.zeros((4, rows_here), jnp.float32)]
    )
    token_grad, expert_rows, scaled_cot, hidden, gate_grad, up_grad = experts(
        normed, cotangent, route, expert_gate[0], expert_up[0], expert_down[0], sp_size
    )
    grad_down = rows_product(hidden, scaled_cot)[None]
    grad_gate = rows_product(expert_rows, gate_grad)[None]
    grad_up = rows_product(expert_rows, up_grad)[None]
    product = in_gate.astype(jnp.float32) * conv_input.astype(jnp.float32)
    earlier = passed_along(product[-2:], "sp", 1)
    extended = jnp.concatenate([earlier, product], axis=0)
    filtered = conv_taps[0] * product + conv_taps[1] * extended[1:-1] + conv_taps[2] * extended[:-2]
    mixed_in = (out_gate.astype(jnp.float32) * filtered).astype(jnp.bfloat16)
    unit_grad = token_grad.astype(jnp.float32) * norm_gain
    along = jnp.mean(unit_stream * unit_grad, axis=-1, keepdims=True)
    stream_grad = (
        cotangent.astype(jnp.float32) + inverse_rms * (unit_grad - unit_stream * along)
    ).astype(jnp.bfloat16)
    grad_stream = lax.dynamic_slice_in_dim(stream_grad, column_start, column_width, 1)
    mixed_grad = jnp.dot(stream_grad, out_weight, preferred_element_type=jnp.float32)
    grad_out_gate = (mixed_grad * filtered).astype(jnp.bfloat16)
    filtered_grad = mixed_grad * out_gate.astype(jnp.float32)
    later = passed_along(filtered_grad[:2], "sp", -1)
    extended_grad = jnp.concatenate([filtered_grad, later], axis=0)
    product_grad = (
        conv_taps[0] * filtered_grad
        + conv_taps[1] * extended_grad[1:-1]
        + conv_taps[2] * extended_grad[2:]
    )
    grad_in_gate = (product_grad * conv_input.astype(jnp.float32)).astype(jnp.bfloat16)
    grad_conv_input = (product_grad * in_gate.astype(jnp.float32)).astype(jnp.bfloat16)
    shares = rows_product(stream_grad, mixed_in).astype(jnp.bfloat16)
    shares = shares.reshape(sp_size, model_width // sp_size, -1)
    shares = lax.all_to_all(shares, "sp", split_axis=0, concat_axis=0)
    grad_out_weight = jnp.sum(shares.astype(jnp.float32), axis=0)
    return (
        grad_stream,
        grad_out_gate,
        grad_in_gate,
        grad_conv_input,
        grad_out_weight,
        grad_gate,
        grad_up,
        grad_down,
    )


def solution(mesh):
    placed = (
        P("sp", None),
        P("sp", None),
        P(),
        P("sp", "tp"),
        P("sp", "tp"),
        P("sp", "tp"),
        P(None, "tp"),
        P(None, "tp"),
        P("sp", None, "tp"),
        P("sp", None, "tp"),
        P("sp", "tp", None),
        P("sp", None),
        P("sp", None),
    )
    return jax.shard_map(
        shards,
        mesh=mesh,
        in_specs=placed,
        out_specs=(
            P("sp", "tp"),
            P("sp", "tp"),
            P("sp", "tp"),
            P("sp", "tp"),
            P("sp", "tp"),
            P("sp", None, "tp"),
            P("sp", None, "tp"),
            P("sp", "tp", None),
        ),
        check_vma=False,
    )
```

```python
import functools

import jax
import jax.numpy as jnp
from jax import lax
from jax.experimental import pallas as pl
from jax.experimental.pallas import tpu as pltpu
from jax.sharding import PartitionSpec as P

norm_eps = 1e-06


def rows_product(left, right):
    return lax.dot_general(
        left, right, (((0,), (0,)), ((), ())), preferred_element_type=jnp.float32
    )


def cols_product(left, right):
    return lax.dot_general(
        left, right, (((1,), (1,)), ((), ())), preferred_element_type=jnp.float32
    )


MESH = pl.DeviceIdType.MESH


def remote(source, target, send_sem, recv_sem, device):
    return pltpu.make_async_remote_copy(
        src_ref=source,
        dst_ref=target,
        send_sem=send_sem,
        recv_sem=recv_sem,
        device_id=device,
        device_id_type=MESH,
    )


def columns(index, width):
    return pl.ds(pl.multiple_of(index * width, width), width)


def mirrored(me, mask, n):
    found, unit = 0, 1
    while unit < n:
        found = found + lax.rem(lax.div(me, unit) + lax.div(mask, unit), 2) * unit
        unit = 2 * unit
    return found


def tp_places():
    tp, count = lax.axis_index("tp"), lax.axis_size("tp")
    cross = lax.rem(tp + count // 2, count)
    partner = tp + 1 - 2 * lax.rem(tp, 2)
    return (tp, cross, partner, lax.rem(partner + count // 2, count))


def greet(cross, partner):
    barrier = pltpu.get_barrier_semaphore()
    for peer in (cross, partner):
        pl.semaphore_signal(barrier, inc=1, device_id={"tp": peer}, device_id_type=MESH)
    me, n = lax.axis_index("sp"), lax.axis_size("sp")

    def greet_one(k, carry):
        peer = lax.rem(me + k, n)
        pl.semaphore_signal(barrier, inc=1, device_id={"sp": peer}, device_id_type=MESH)
        return carry

    lax.fori_loop(1, n, greet_one, 0)
    return lambda: pl.semaphore_wait(barrier, n + 1)


def loop(low, high, body):
    def step(k, carry):
        body(k)
        return carry

    lax.fori_loop(low, high, step, 0)


def step_kernel(
    n,
    stream,
    cot,
    gain,
    route,
    out_gate,
    in_gate,
    conv_input,
    taps,
    w_out_hbm,
    w_gate_hbm,
    w_up_hbm,
    w_down_hbm,
    stream_out,
    out_gate_out,
    in_gate_out,
    conv_input_out,
    w_out_grad,
    gate_out,
    up_out,
    down_out,
    normed,
    inverse,
    along,
    w_out,
    w_gate,
    w_up,
    w_down,
    keys,
    weights,
    arrived,
    arrived_route,
    sending,
    slots,
    hidden,
    both_grad,
    partial,
    near,
    far_out,
    far_in,
    total,
    back,
    acc,
    token,
    extended,
    filtered,
    extended_grad,
    mixed,
    stream_grad,
    turned,
    turned_all,
    gate_sum,
    up_sum,
    down_sum,
    small,
    w_out_sum,
    load,
    tok_send,
    tok_recv,
    slot_send,
    slot_recv,
    cross_send,
    cross_recv,
    near_send,
    fwd_send,
    near_recv,
    hand_send,
    hand_recv,
    far_send,
    far_recv,
    out_send,
    out_recv,
    all_send,
    all_cross,
    all_near,
    halo_send,
    halo_recv,
    mix_send,
    mix_recv,
    turn_send,
    turn_recv,
    turn_cross,
    turn_near,
    local,
):
    me = lax.axis_index("sp")
    tp, cross, partner, diagonal = tp_places()
    half = n // 2
    count, wide = normed.shape
    width = acc.shape[1]
    depth = near.shape[1] // n
    group = max(1, 256 // depth)
    span = group * depth
    chunk = min(256, width)
    channels = filtered.shape[1]
    block = wide // n
    shared_parts = wide // width
    shared_parts = shared_parts if block % (16 * shared_parts) == 0 else 1
    share = block // shared_parts
    wait_all = greet(cross, partner)
    sources = (normed, cot)
    loads = [
        pltpu.make_async_copy(source, target, load.at[i])
        for i, (source, target) in enumerate(
            ((w_gate_hbm, w_gate), (w_up_hbm, w_up), (w_down_hbm, w_down), (w_out_hbm, w_out))
        )
    ]
    for one in loads:
        one.start()

    def other(s):
        return mirrored(me, jnp.int32(s), n)

    def at(s):
        return pl.ds(pl.multiple_of(s * depth, depth), depth)

    def normalize(i):
        rows = pl.ds(pl.multiple_of(i * 32, 32), 32)
        values = stream[rows, :].astype(jnp.float32)
        scale = lax.rsqrt(jnp.mean(values * values, axis=-1, keepdims=True) + norm_eps)
        inverse[rows, :] = scale
        normed[rows, :] = (values * scale * gain[...]).astype(jnp.bfloat16)

    def table(which, source):
        c0, c1, s0, s1 = (source[i : i + 1, :] for i in range(4))
        expert = lax.broadcasted_iota(jnp.int32, (n, count), 0).astype(jnp.float32)
        first, second = (c0 == expert, c1 == expert)
        member = jnp.where(first | second, 1.0, 0.0)
        row = lax.broadcasted_iota(jnp.int32, (count, count), 0)
        column = lax.broadcasted_iota(jnp.int32, (count, count), 1)
        before = jnp.where(row < column, 1.0, 0.0).astype(jnp.bfloat16)
        earlier = jnp.dot(
            member.astype(jnp.bfloat16), before, preferred_element_type=jnp.float32
        )
        keys[which] = jnp.where(member > 0.0, earlier, -1.0)
        weights[which] = jnp.where(first, s0, 0.0) + jnp.where(second, s1, 0.0)

    def placing(which, expert):
        slot = lax.broadcasted_iota(jnp.int32, (depth, count), 0).astype(jnp.float32)
        return slot == keys[which, pl.ds(expert, 1), :]

    def chosen(a, which, expert, values):
        mask = placing(which, expert)
        found = jnp.dot(
            jnp.where(mask, 1.0, 0.0).astype(jnp.bfloat16),
            values,
            preferred_element_type=jnp.float32,
        )
        if a == 1:
            weight = jnp.where(mask, weights[which, pl.ds(expert, 1), :], 0.0)
            found = found * jnp.sum(weight, axis=1, keepdims=True)
        return found.astype(jnp.bfloat16)

    def token_copy(a):
        return remote(
            sources[a].at[:, columns(tp, width)],
            arrived.at[a],
            tok_send.at[a],
            tok_recv.at[a],
            {"sp": other(half)},
        )

    def route_copy():
        return remote(route, arrived_route, tok_send.at[2], tok_recv.at[2], {"sp": other(half)})

    def slot_copy(a, s, k):
        return remote(
            sending.at[a, at(s)],
            slots.at[a, at(s), columns(tp, width)],
            slot_send.at[a],
            slot_recv.at[a, s],
            {"sp": other(k)},
        )

    def spread(a, s):
        part = slots.at[a, at(s), columns(tp, width)]
        remote(part, part, cross_send.at[a], cross_recv.at[a, s], {"tp": cross}).start()
        remote(part, part, near_send.at[a], near_recv.at[a, s], {"tp": partner}).start()

    def forward(a, s):
        part = slots.at[a, at(s), columns(cross, width)]
        remote(part, part, cross_send.at[a], cross_recv.at[a, s], {"tp": cross}).wait_recv()
        remote(part, part, fwd_send.at[a], near_recv.at[a, s], {"tp": partner}).start()

    def ready(s):
        for a in (0, 1):
            both = slots.at[a, at(s), pl.ds(0, 2 * width)]
            remote(both, both, near_send.at[a], near_recv.at[a, s], {"tp": partner}).wait_recv()

    def hand(j, s):
        return remote(
            partial.at[at(s), columns((partner, diagonal)[j], width)],
            near.at[j, at(s)],
            hand_send.at[j],
            hand_recv.at[j, s],
            {"tp": partner},
        )

    def across(s):
        return remote(
            far_out.at[at(s)], far_in.at[at(s)], far_send, far_recv.at[s], {"tp": cross}
        )

    def give(s):
        return remote(
            total.at[at(s)], back.at[at(s)], out_send, out_recv.at[s], {"sp": other(s)}
        )

    def halo_later():
        peer = lax.rem(me + 1, n)
        return remote(
            extended.at[pl.ds(count, 8)],
            extended.at[pl.ds(0, 8)],
            halo_send.at[0],
            halo_recv.at[0],
            {"sp": peer},
        )

    def halo_earlier():
        peer = lax.rem(me + n - 1, n)
        return remote(
            extended_grad.at[pl.ds(0, 8)],
            extended_grad.at[pl.ds(count, 8)],
            halo_send.at[1],
            halo_recv.at[1],
            {"sp": peer},
        )

    def mix_copy(source, target, k):
        return remote(
            mixed.at[source], mixed.at[target], mix_send, mix_recv.at[target], {"sp": other(k)}
        )

    with jax.named_scope("prep"):
        loop(0, count // 32, normalize)
        table(0, route)
        product = in_gate[...].astype(jnp.float32) * conv_input[...].astype(jnp.float32)
        extended[pl.ds(8, count), :] = product

        @pl.when(me == 0)
        def _():
            extended[pl.ds(0, 8), :] = jnp.zeros((8, channels), jnp.float32)

        @pl.when(me == n - 1)
        def _():
            extended_grad[pl.ds(count, 8), :] = jnp.zeros((8, channels), jnp.float32)

    with jax.named_scope("barrier"):
        wait_all()

    def send_own(k):
        for a in (0, 1):
            values = sources[a][:, columns(tp, width)]
            sending[a, at(k), :] = chosen(a, 0, other(k), values)
            slot_copy(a, k, k).start()

    with jax.named_scope("send_own"):
        loop(1, half, send_own)
        token_copy(0).start()
        route_copy().start()
        token_copy(1).start()

        @pl.when(me < n - 1)
        def _():
            halo_later().start()

    with jax.named_scope("own_block"):
        for a in (0, 1):
            for piece in range(wide // width):
                where = pl.ds(piece * width, width)
                slots[a, pl.ds(0, depth), where] = chosen(a, 0, me, sources[a][:, where])

    def land(s, k):
        for a in (0, 1):
            slot_copy(a, s, k).wait_recv()
            spread(a, s)

    def land_own(k):
        land(k, k)

    with jax.named_scope("land_own"):
        loop(1, half, land_own)

    with jax.named_scope("filter"):
        @pl.when(me > 0)
        def _():
            halo_later().wait_recv()

        filtered[...] = (
            taps[0:1, :] * extended[pl.ds(8, count), :]
            + taps[1:2, :] * extended[pl.ds(7, count), :]
            + taps[2:3, :] * extended[pl.ds(6, count), :]
        )
        mixed[0] = (out_gate[...].astype(jnp.float32) * filtered[...]).astype(jnp.bfloat16)

    for a in (0, 1):
        with jax.named_scope("await_tokens"):
            if a == 0:
                route_copy().wait_recv()
                table(1, arrived_route)
            token_copy(a).wait_recv()

        def send_other(k):
            sending[a, at(half + k), :] = chosen(a, 1, other(k), arrived[a])
            slot_copy(a, half + k, k).start()

        with jax.named_scope("send_other"):
            loop(1, half, send_other)
            slots[a, at(half), columns(tp, width)] = chosen(a, 1, me, arrived[a])
            spread(a, half)

    def forward_both(s):
        for a in (0, 1):
            forward(a, s)

    with jax.named_scope("forward_own"):
        mix_copy(0, half, half).start()

        def mix_own(k):
            mix_copy(0, k, k).start()

        loop(1, half, mix_own)
        loop(1, half, forward_both)

    def compute(g):
        rows = pl.ds(pl.multiple_of(g * span, span), span)
        picked, scaled = (slots[0, rows, :], slots[1, rows, :])
        gate_pre = jnp.dot(picked, w_gate[...], preferred_element_type=jnp.float32)
        up_pre = jnp.dot(picked, w_up[...], preferred_element_type=jnp.float32)
        hidden_grad = cols_product(scaled, w_down[...])
        sigmoid_gate = jax.nn.sigmoid(gate_pre)
        silu_gate = gate_pre * sigmoid_gate
        hidden[rows, :] = (silu_gate * up_pre).astype(jnp.bfloat16)
        gate = (
            hidden_grad * up_pre * sigmoid_gate * (1.0 + gate_pre * (1.0 - sigmoid_gate))
        ).astype(jnp.bfloat16)
        up = (hidden_grad * silu_gate).astype(jnp.bfloat16)
        across_hidden = gate.shape[1]
        both_grad[rows, pl.ds(0, across_hidden)] = gate
        both_grad[rows, pl.ds(across_hidden, across_hidden)] = up
        for piece in range(wide // width):
            where = pl.ds(piece * width, width)
            partial[rows, where] = (
                cols_product(gate, w_gate[where, :]) + cols_product(up, w_up[where, :])
            ).astype(jnp.bfloat16)

    def work(g):
        def await_one(i):
            s = g * group + i

            @pl.when(s > 0)
            def _():
                ready(s)

        loop(0, group, await_one)
        compute(g)

        def hand_one(i):
            s = g * group + i
            hand(1, s).start()
            hand(0, s).start()

        loop(0, group, hand_one)

    groups = n // group
    with jax.named_scope("work_own"):
        for i in range(3):
            loads[i].wait()
        loop(0, groups // 2, work)

    def land_other(k):
        land(half + k, k)

        @pl.when(k == 1)
        def _():
            forward_both(half)

        @pl.when(k > 1)
        def _():
            forward_both(half + k - 1)

    with jax.named_scope("land_other"):
        loop(1, half, land_other)

    def pair(s):
        hand(1, s).wait_recv()
        mine = partial[at(s), columns(cross, width)].astype(jnp.float32)
        far_out[at(s), :] = (mine + near[1, at(s), :].astype(jnp.float32)).astype(jnp.bfloat16)
        across(s).start()

    with jax.named_scope("pair_own"):
        loop(0, half, pair)
        mix_copy(half, half, half).wait_recv()

        def mix_other(k):
            mix_copy(half, half + k, k).start()

        loop(1, half, mix_other)
    with jax.named_scope("forward_last"):
        forward_both(n - 1)
    with jax.named_scope("work_other"):
        loop(groups // 2, groups, work)
    with jax.named_scope("pair_other"):
        loop(half, n, pair)

    def finish(s):
        hand(0, s).wait_recv()
        across(s).wait_recv()
        mine = partial[at(s), columns(tp, width)].astype(jnp.float32)
        return (
            mine + near[0, at(s), :].astype(jnp.float32) + far_in[at(s), :].astype(jnp.float32)
        ).astype(jnp.bfloat16)

    def finish_one(s):
        total[at(s), :] = finish(s)
        give(s).start()

    def grad_copies(c):
        rows = pl.ds(pl.multiple_of(c * chunk, chunk), chunk)
        return [
            pltpu.make_async_copy(source, target, local.at[i])
            for i, (source, target) in enumerate(
                (
                    (gate_sum.at[rows, :], gate_out.at[rows, :]),
                    (up_sum.at[rows, :], up_out.at[rows, :]),
                    (down_sum.at[:, rows], down_out.at[:, rows]),
                )
            )
        ]

    def grads(c):
        rows = pl.ds(pl.multiple_of(c * chunk, chunk), chunk)
        sums = rows_product(slots[0, :, rows], both_grad[...])
        gate_sum[rows, :] = sums[:, : sums.shape[1] // 2]
        up_sum[rows, :] = sums[:, sums.shape[1] // 2 :]
        down_sum[:, rows] = rows_product(hidden[...], slots[1, :, rows])
        for one in grad_copies(c):
            one.start()

    with jax.named_scope("finish_own"):
        loop(1, half, finish_one)
        back[pl.ds(0, depth), :] = finish(0)
    with jax.named_scope("grads"):
        loop(0, wide // chunk // 2, grads)
    with jax.named_scope("finish_other"):
        loop(half, n, finish_one)
    with jax.named_scope("grads"):
        loop(wide // chunk // 2, wide // chunk, grads)
    acc[...] = jnp.zeros_like(acc)

    def combine(s):
        @pl.when(s > 0)
        def _():
            give(s).wait_recv()

        mask = jnp.where(placing(0, other(s)), 1.0, 0.0).astype(jnp.bfloat16)
        acc[...] += rows_product(mask, back[at(s), :])

    with jax.named_scope("combine"):
        loop(0, n, combine)
    pieces = all_cross.shape[0]
    tall = count // pieces

    def shared(i, column, send, recv, peer):
        part = token.at[pl.ds(i * tall, tall), columns(column, width)]
        return remote(part, part, send, recv, {"tp": peer})

    with jax.named_scope("share"):
        token[:, columns(tp, width)] = acc[...].astype(jnp.bfloat16)
        for i in range(pieces):
            shared(i, tp, all_send.at[0, i], all_cross.at[i], cross).start()
            shared(i, tp, all_send.at[1, i], all_near.at[0, i], partner).start()
        for i in range(pieces):
            shared(i, cross, all_send.at[0, i], all_cross.at[i], cross).wait_recv()
            shared(i, cross, all_send.at[2, i], all_near.at[1, i], partner).start()
        for i in range(pieces):
            for j in (0, 1):
                shared(i, tp, all_send.at[j + 1, i], all_near.at[j, i], partner).wait()
            shared(i, tp, all_send.at[0, i], all_cross.at[i], cross).wait_send()

    def reduce_along(i):
        rows = pl.ds(pl.multiple_of(i * 32, 32), 32)
        unit = stream[rows, :].astype(jnp.float32) * inverse[rows, :]
        unit_grad = token[rows, :].astype(jnp.float32) * gain[...]
        along[rows, :] = jnp.mean(unit * unit_grad, axis=-1, keepdims=True)

    def total_grad(c):
        where = pl.ds(pl.multiple_of(c * chunk, chunk), chunk)
        scale = inverse[...]
        unit = stream[:, where].astype(jnp.float32) * scale
        unit_grad = token[:, where].astype(jnp.float32) * gain[:, where]
        value = cot[:, where].astype(jnp.float32) + scale * (unit_grad - unit * along[...])
        value = value.astype(jnp.bfloat16)
        stream_grad[:, where] = value
        turned[where, :] = jnp.transpose(value.astype(jnp.float32)).astype(jnp.bfloat16)

    with jax.named_scope("stream_grad"):
        loop(0, count // 32, reduce_along)
        loop(0, wide // chunk, total_grad)

    def turned_rows(owner, part):
        return pl.ds(pl.multiple_of(owner * block + part * share, share), share)

    def part_rows(part):
        return pl.ds(pl.multiple_of(part * share, share), share)

    mine_part = tp if shared_parts > 1 else 0
    cross_part = cross if shared_parts > 1 else 0

    def turn_copy(s):
        return remote(
            turned.at[turned_rows(other(s), mine_part)],
            turned_all.at[s, part_rows(mine_part)],
            turn_send.at[0],
            turn_recv.at[s],
            {"sp": other(s)},
        )

    def turn_part(s, part, send, recv, peer):
        rows = turned_all.at[s, part_rows(part)]
        return remote(rows, rows, send, recv, {"tp": peer})

    def turn_start(s):
        turn_copy(s).start()

    stream_copy = pltpu.make_async_copy(
        stream_grad.at[:, columns(tp, width)], stream_out, local.at[3]
    )
    with jax.named_scope("mixed_grad"):
        loop(1, n, turn_start)
        stream_copy.start()
        loads[3].wait()
        mixed_grad = jnp.dot(stream_grad[...], w_out[...], preferred_element_type=jnp.float32)
        small[0] = (mixed_grad * filtered[...]).astype(jnp.bfloat16)
        extended_grad[pl.ds(0, count), :] = mixed_grad * out_gate[...].astype(jnp.float32)

        @pl.when(me > 0)
        def _():
            halo_earlier().start()

    def turn_land(s):
        turn_copy(s).wait_recv()
        if shared_parts > 1:
            turn_part(s, tp, turn_send.at[1], turn_cross.at[s], cross).start()
            turn_part(s, tp, turn_send.at[2], turn_near.at[s], partner).start()

    def turn_forward(s):
        turn_part(s, cross, turn_send.at[1], turn_cross.at[s], cross).wait_recv()
        turn_part(s, cross, turn_send.at[3], turn_near.at[s], partner).start()

    def turn_step(s):
        turn_land(s)
        if shared_parts > 1:

            @pl.when(s > 1)
            def _():
                turn_forward(s - 1)

    with jax.named_scope("turn_land"):
        loop(1, n, turn_step)
        if shared_parts > 1:
            turn_forward(n - 1)

    with jax.named_scope("conv_grad"):
        @pl.when(me < n - 1)
        def _():
            halo_earlier().wait_recv()

        product_grad = (
            taps[0:1, :] * extended_grad[pl.ds(0, count), :]
            + taps[1:2, :] * extended_grad[pl.ds(1, count), :]
            + taps[2:3, :] * extended_grad[pl.ds(2, count), :]
        )
        small[1] = (product_grad * conv_input[...].astype(jnp.float32)).astype(jnp.bfloat16)
        small[2] = (product_grad * in_gate[...].astype(jnp.float32)).astype(jnp.bfloat16)
        small_copies = [
            pltpu.make_async_copy(small.at[i], target, local.at[4 + i])
            for i, target in enumerate((out_gate_out, in_gate_out, conv_input_out))
        ]
        for one in small_copies:
            one.start()

    w_out_sum[...] = jnp.dot(
        turned[pl.ds(pl.multiple_of(me * block, block), block), :],
        mixed[0],
        preferred_element_type=jnp.float32,
    )

    def out_step(s):
        if shared_parts > 1:
            pair_rows = turned_all.at[s, pl.ds(0, 2 * share)]
            remote(
                pair_rows, pair_rows, turn_send.at[2], turn_near.at[s], {"tp": partner}
            ).wait_recv()

        @pl.when(s < half)
        def _():
            mix_copy(0, s, s).wait_recv()

        @pl.when(s > half)
        def _():
            mix_copy(half, s, s - half).wait_recv()

        w_out_sum[...] += jnp.dot(turned_all[s], mixed[s], preferred_element_type=jnp.float32)

    with jax.named_scope("w_out_grad"):
        loop(1, n, out_step)
        last = pltpu.make_async_copy(w_out_sum, w_out_grad, local.at[7])
        last.start()

    with jax.named_scope("drain"):
        route_copy().wait_send()
        for a in (0, 1):
            token_copy(a).wait_send()
            sent = sending.at[a, pl.ds(0, (n - 2) * depth)]
            remote(sent, sent, slot_send.at[a], slot_recv.at[a, 0], {"tp": partner}).wait_send()
            most = slots.at[a, pl.ds(0, (n - 1) * depth), pl.ds(0, width)]
            for sem in (cross_send, near_send, fwd_send):
                remote(most, most, sem.at[a], near_recv.at[a, 0], {"tp": partner}).wait_send()
            remote(far_out, far_in, hand_send.at[a], hand_recv.at[a, 0], {"tp": partner}).wait_send()
        remote(far_out, far_in, far_send, far_recv.at[0], {"tp": cross}).wait_send()
        rest = total.at[pl.ds(0, (n - 1) * depth)]
        remote(rest, rest, out_send, out_recv.at[0], {"tp": partner}).wait_send()
        sent = mixed.at[pl.ds(0, n - 1)]
        remote(sent, sent, mix_send, mix_recv.at[0], {"tp": partner}).wait_send()
        sent = turned_all.at[pl.ds(0, n - 1), pl.ds(0, share)]
        for kind in range(4 if shared_parts > 1 else 1):
            remote(sent, sent, turn_send.at[kind], turn_recv.at[0], {"tp": partner}).wait_send()

        @pl.when(me < n - 1)
        def _():
            halo_later().wait_send()

        @pl.when(me > 0)
        def _():
            halo_earlier().wait_send()

        stream_copy.wait()
        for one in small_copies:
            one.wait()
        for i, (source, target) in enumerate(
            ((gate_sum, gate_out), (up_sum, up_out), (down_sum, down_out))
        ):
            pltpu.make_async_copy(source, target, local.at[i]).wait()
        last.wait()


def shards(
    cotangent,
    stream_in,
    norm_gain,
    out_gate,
    in_gate,
    conv_input,
    conv_taps,
    out_weight,
    expert_gate,
    expert_up,
    expert_down,
    expert_choice,
    route_scale,
):
    n = lax.axis_size("sp")
    count, wide = stream_in.shape
    channels = out_gate.shape[1]
    hidden = expert_gate.shape[2]
    width = wide // lax.axis_size("tp")
    depth = 4 * count // n
    rows = n * depth
    block = wide // n
    pieces = 2
    kind = stream_in.dtype
    route = jnp.concatenate(
        [expert_choice.T.astype(jnp.float32), route_scale.T, jnp.zeros((4, count), jnp.float32)]
    )

    def out(*shape, dtype=kind):
        return jax.ShapeDtypeStruct(shape, dtype)

    def full(*shape):
        return pltpu.VMEM(shape, jnp.float32)

    def held(*shape):
        return pltpu.VMEM(shape, kind)

    vmem, anywhere = (pl.BlockSpec(memory_space=pltpu.VMEM), pl.BlockSpec(memory_space=pl.ANY))
    dma = pltpu.SemaphoreType.DMA
    results = pl.pallas_call(
        functools.partial(step_kernel, n),
        out_shape=[
            out(count, width),
            out(count, channels),
            out(count, channels),
            out(count, channels),
            out(block, channels, dtype=jnp.float32),
            out(wide, hidden, dtype=jnp.float32),
            out(wide, hidden, dtype=jnp.float32),
            out(hidden, wide, dtype=jnp.float32),
        ],
        in_specs=[vmem] * 8 + [anywhere] * 4,
        out_specs=[anywhere] * 8,
        scratch_shapes=[
            held(count, wide),
            full(count, 1),
            full(count, 1),
            held(wide, channels),
            held(wide, hidden),
            held(wide, hidden),
            held(hidden, wide),
            full(2, n, count),
            full(2, n, count),
            held(2, count, width),
            full(*route.shape),
            held(2, rows, width),
            held(2, rows, wide),
            held(rows, hidden),
            held(rows, 2 * hidden),
            held(rows, wide),
            held(2, rows, width),
            held(rows, width),
            held(rows, width),
            held(rows, width),
            held(rows, width),
            full(count, width),
            held(count, wide),
            full(count + 8, channels),
            full(count, channels),
            full(count + 8, channels),
            held(n, count, channels),
            held(count, wide),
            held(wide, count),
            held(n, block, count),
            full(wide, hidden),
            full(wide, hidden),
            full(hidden, wide),
            held(3, count, channels),
            full(block, channels),
            dma((4,)),
            dma((3,)),
            dma((3,)),
            dma((2,)),
            dma((2, n)),
            dma((2,)),
            dma((2, n)),
            dma((2,)),
            dma((2,)),
            dma((2, n)),
            dma((2,)),
            dma((2, n)),
            dma,
            dma((n,)),
            dma,
            dma((n,)),
            dma((3, pieces)),
            dma((pieces,)),
            dma((2, pieces)),
            dma((2,)),
            dma((2,)),
            dma,
            dma((n,)),
            dma((4,)),
            dma((n,)),
            dma((n,)),
            dma((n,)),
            dma((8,)),
        ],
        compiler_params=pltpu.CompilerParams(
            collective_id=1, has_side_effects=True, vmem_limit_bytes=58 * 1024 * 1024
        ),
    )(
        stream_in,
        cotangent,
        norm_gain[None],
        route,
        out_gate,
        in_gate,
        conv_input,
        conv_taps,
        out_weight,
        expert_gate[0],
        expert_up[0],
        expert_down[0],
    )
    return (*results[:5], *(grad[None] for grad in results[5:]))


def solution(mesh):
    placed = (
        P("sp", None),
        P("sp", None),
        P(),
        P("sp", "tp"),
        P("sp", "tp"),
        P("sp", "tp"),
        P(None, "tp"),
        P(None, "tp"),
        P("sp", None, "tp"),
        P("sp", None, "tp"),
        P("sp", "tp", None),
        P("sp", None),
        P("sp", None),
    )
    return jax.shard_map(
        shards,
        mesh=mesh,
        in_specs=placed,
        out_specs=(
            P("sp", "tp"),
            P("sp", "tp"),
            P("sp", "tp"),
            P("sp", "tp"),
            P("sp", "tp"),
            P("sp", None, "tp"),
            P("sp", None, "tp"),
            P("sp", "tp", None),
        ),
        check_vma=False,
    )
```

```python
import functools

import jax
import jax.numpy as jnp
from jax import lax
from jax.experimental import pallas as pl
from jax.experimental.pallas import tpu as pltpu
from jax.sharding import PartitionSpec as P

norm_eps = 1e-06
VMEM = 39 * 1024 * 1024


def rows_product(left, right):
    return lax.dot_general(
        left, right, (((0,), (0,)), ((), ())), preferred_element_type=jnp.float32
    )


def cols_product(left, right):
    return lax.dot_general(
        left, right, (((1,), (1,)), ((), ())), preferred_element_type=jnp.float32
    )


MESH = pl.DeviceIdType.MESH


def remote(source, target, send_sem, recv_sem, device):
    return pltpu.make_async_remote_copy(
        src_ref=source,
        dst_ref=target,
        send_sem=send_sem,
        recv_sem=recv_sem,
        device_id=device,
        device_id_type=MESH,
    )


def columns(index, width):
    return pl.ds(pl.multiple_of(index * width, width), width)


def mirrored(me, mask, n):
    found, unit = 0, 1
    while unit < n:
        found = found + lax.rem(lax.div(me, unit) + lax.div(mask, unit), 2) * unit
        unit = 2 * unit
    return found


def tp_places():
    tp, count = lax.axis_index("tp"), lax.axis_size("tp")
    cross = lax.rem(tp + count // 2, count)
    partner = tp + 1 - 2 * lax.rem(tp, 2)
    return (tp, cross, partner, lax.rem(partner + count // 2, count))


def greet(cross, partner):
    barrier = pltpu.get_barrier_semaphore()
    for peer in (cross, partner):
        pl.semaphore_signal(barrier, inc=1, device_id={"tp": peer}, device_id_type=MESH)
    me, n = lax.axis_index("sp"), lax.axis_size("sp")

    def greet_one(k, carry):
        peer = lax.rem(me + k, n)
        pl.semaphore_signal(barrier, inc=1, device_id={"sp": peer}, device_id_type=MESH)
        return carry

    lax.fori_loop(1, n, greet_one, 0)
    return lambda: pl.semaphore_wait(barrier, n + 1)


def loop(low, high, body):
    def step(k, carry):
        body(k)
        return carry

    lax.fori_loop(low, high, step, 0)


def step_kernel(
    n,
    stream,
    cot,
    gain,
    choice,
    scales,
    out_gate,
    in_gate,
    conv_input,
    taps,
    w_out_hbm,
    w_gate_hbm,
    w_up_hbm,
    w_down_hbm,
    stream_out,
    small_out,
    w_out_sum,
    gate_sum,
    up_sum,
    down_sum,
    normed,
    inverse,
    along,
    w_out,
    w_gate,
    w_up,
    w_down,
    keys,
    weights,
    arrived,
    arrived_choice,
    arrived_scales,
    sending,
    slots,
    hidden,
    both_grad,
    partial,
    near,
    far_out,
    far_in,
    total,
    back,
    acc,
    token,
    extended,
    filtered,
    extended_grad,
    mixed,
    stream_grad,
    turned,
    turned_all,
    load,
    tok_send,
    tok_recv,
    slot_send,
    slot_recv,
    cross_send,
    cross_recv,
    near_send,
    fwd_send,
    near_recv,
    hand_send,
    hand_recv,
    far_send,
    far_recv,
    out_send,
    out_recv,
    all_send,
    all_cross,
    all_near,
    halo_send,
    halo_recv,
    mix_send,
    mix_recv,
    turn_send,
    turn_recv,
    turn_cross,
    turn_near,
):
    me = lax.axis_index("sp")
    tp, cross, partner, diagonal = tp_places()
    half = n // 2
    count, wide = normed.shape
    width = acc.shape[1]
    depth = near.shape[1] // n
    group = max(1, 256 // depth)
    span = group * depth
    chunk = min(256, width)
    channels = filtered.shape[1]
    block = wide // n
    shared_parts = wide // width
    shared_parts = shared_parts if block % (16 * shared_parts) == 0 else 1
    share = block // shared_parts
    wait_all = greet(cross, partner)
    sources = (normed, cot)
    loads = [
        pltpu.make_async_copy(source, target, load.at[i])
        for i, (source, target) in enumerate(
            ((w_gate_hbm, w_gate), (w_up_hbm, w_up), (w_down_hbm, w_down), (w_out_hbm, w_out))
        )
    ]
    for one in loads:
        one.start()

    def other(s):
        return mirrored(me, jnp.int32(s), n)

    def at(s):
        return pl.ds(pl.multiple_of(s * depth, depth), depth)

    def normalize(i):
        rows = pl.ds(pl.multiple_of(i * 32, 32), 32)
        values = stream[rows, :].astype(jnp.float32)
        scale = lax.rsqrt(jnp.mean(values * values, axis=-1, keepdims=True) + norm_eps)
        inverse[rows, :] = scale
        normed[rows, :] = (values * scale * gain[...]).astype(jnp.bfloat16)

    def table(which, named, scaled):
        c0, c1 = (named[i : i + 1, :] for i in range(2))
        s0, s1 = (scaled[i : i + 1, :] for i in range(2))
        expert = lax.broadcasted_iota(jnp.int32, (n, count), 0)
        first, second = (c0 == expert, c1 == expert)
        member = jnp.where(first | second, 1.0, 0.0)
        row = lax.broadcasted_iota(jnp.int32, (count, count), 0)
        column = lax.broadcasted_iota(jnp.int32, (count, count), 1)
        before = jnp.where(row < column, 1.0, 0.0).astype(jnp.bfloat16)
        earlier = jnp.dot(
            member.astype(jnp.bfloat16), before, preferred_element_type=jnp.float32
        )
        keys[which] = jnp.where(member > 0.0, earlier, -1.0)
        weights[which] = jnp.where(first, s0, 0.0) + jnp.where(second, s1, 0.0)

    def placing(which, expert):
        slot = lax.broadcasted_iota(jnp.int32, (depth, count), 0).astype(jnp.float32)
        return slot == keys[which, pl.ds(expert, 1), :]

    def chosen(a, which, expert, values):
        mask = placing(which, expert)
        found = jnp.dot(
            jnp.where(mask, 1.0, 0.0).astype(jnp.bfloat16),
            values,
            preferred_element_type=jnp.float32,
        )
        if a == 1:
            weight = jnp.where(mask, weights[which, pl.ds(expert, 1), :], 0.0)
            found = found * jnp.sum(weight, axis=1, keepdims=True)
        return found.astype(jnp.bfloat16)

    def token_copy(a):
        return remote(
            sources[a].at[:, columns(tp, width)],
            arrived.at[a],
            tok_send.at[a],
            tok_recv.at[a],
            {"sp": other(half)},
        )

    def route_copies():
        pairs = ((choice, arrived_choice), (scales, arrived_scales))
        return [
            remote(source, target, tok_send.at[2 + i], tok_recv.at[2 + i], {"sp": other(half)})
            for i, (source, target) in enumerate(pairs)
        ]

    def slot_copy(a, s, k):
        return remote(
            sending.at[a, at(s)],
            slots.at[a, at(s), columns(tp, width)],
            slot_send.at[a],
            slot_recv.at[a, s],
            {"sp": other(k)},
        )

    def spread(a, s):
        part = slots.at[a, at(s), columns(tp, width)]
        remote(part, part, cross_send.at[a], cross_recv.at[a, s], {"tp": cross}).start()
        remote(part, part, near_send.at[a], near_recv.at[a, s], {"tp": partner}).start()

    def forward(a, s):
        part = slots.at[a, at(s), columns(cross, width)]
        remote(part, part, cross_send.at[a], cross_recv.at[a, s], {"tp": cross}).wait_recv()
        remote(part, part, fwd_send.at[a], near_recv.at[a, s], {"tp": partner}).start()

    def ready(s):
        for a in (0, 1):
            both = slots.at[a, at(s), pl.ds(0, 2 * width)]
            remote(both, both, near_send.at[a], near_recv.at[a, s], {"tp": partner}).wait_recv()

    def hand(j, s):
        return remote(
            partial.at[at(s), columns((partner, diagonal)[j], width)],
            near.at[j, at(s)],
            hand_send.at[j],
            hand_recv.at[j, s],
            {"tp": partner},
        )

    def across(s):
        return remote(
            far_out.at[at(s)], far_in.at[at(s)], far_send, far_recv.at[s], {"tp": cross}
        )

    def give(s):
        return remote(
            total.at[at(s)], back.at[at(s)], out_send, out_recv.at[s], {"sp": other(s)}
        )

    def halo_later():
        peer = lax.rem(me + 1, n)
        return remote(
            extended.at[pl.ds(count, 8)],
            extended.at[pl.ds(0, 8)],
            halo_send.at[0],
            halo_recv.at[0],
            {"sp": peer},
        )

    def halo_earlier():
        peer = lax.rem(me + n - 1, n)
        return remote(
            extended_grad.at[pl.ds(0, 8)],
            extended_grad.at[pl.ds(count, 8)],
            halo_send.at[1],
            halo_recv.at[1],
            {"sp": peer},
        )

    def mix_copy(source, target, k):
        return remote(
            mixed.at[source], mixed.at[target], mix_send, mix_recv.at[target], {"sp": other(k)}
        )

    with jax.named_scope("prep"):
        loop(0, count // 32, normalize)
        table(0, choice, scales)
        product = in_gate[...].astype(jnp.float32) * conv_input[...].astype(jnp.float32)
        extended[pl.ds(8, count), :] = product

        @pl.when(me == 0)
        def _():
            extended[pl.ds(0, 8), :] = jnp.zeros((8, channels), jnp.float32)

        @pl.when(me == n - 1)
        def _():
            extended_grad[pl.ds(count, 8), :] = jnp.zeros((8, channels), jnp.float32)

    with jax.named_scope("barrier"):
        wait_all()

    def send_own(k):
        for a in (0, 1):
            values = sources[a][:, columns(tp, width)]
            sending[a, at(k), :] = chosen(a, 0, other(k), values)
            slot_copy(a, k, k).start()

    with jax.named_scope("send_own"):
        loop(1, half, send_own)
        for one in route_copies():
            one.start()
        token_copy(0).start()
        token_copy(1).start()

        @pl.when(me < n - 1)
        def _():
            halo_later().start()

    with jax.named_scope("own_block"):
        for a in (0, 1):
            for piece in range(wide // width):
                where = pl.ds(piece * width, width)
                slots[a, pl.ds(0, depth), where] = chosen(a, 0, me, sources[a][:, where])

    def land(s, k):
        for a in (0, 1):
            slot_copy(a, s, k).wait_recv()
            spread(a, s)

    def land_own(k):
        land(k, k)

    with jax.named_scope("land_own"):
        loop(1, half, land_own)

    with jax.named_scope("filter"):
        @pl.when(me > 0)
        def _():
            halo_later().wait_recv()

        filtered[...] = (
            taps[0:1, :] * extended[pl.ds(8, count), :]
            + taps[1:2, :] * extended[pl.ds(7, count), :]
            + taps[2:3, :] * extended[pl.ds(6, count), :]
        )
        mixed[0] = (out_gate[...].astype(jnp.float32) * filtered[...]).astype(jnp.bfloat16)

    for a in (0, 1):
        with jax.named_scope("await_tokens"):
            if a == 0:
                for one in route_copies():
                    one.wait_recv()
                table(1, arrived_choice, arrived_scales)
            token_copy(a).wait_recv()

        def send_other(k):
            sending[a, at(half + k), :] = chosen(a, 1, other(k), arrived[a])
            slot_copy(a, half + k, k).start()

        with jax.named_scope("send_other"):
            loop(1, half, send_other)
            slots[a, at(half), columns(tp, width)] = chosen(a, 1, me, arrived[a])
            spread(a, half)

    def forward_both(s):
        for a in (0, 1):
            forward(a, s)

    with jax.named_scope("forward_own"):
        mix_copy(0, half, half).start()

        def mix_own(k):
            mix_copy(0, k, k).start()

        loop(1, half, mix_own)
        loop(1, half, forward_both)

    def compute(g):
        rows = pl.ds(pl.multiple_of(g * span, span), span)
        picked, scaled = (slots[0, rows, :], slots[1, rows, :])
        gate_pre = jnp.dot(picked, w_gate[...], preferred_element_type=jnp.float32)
        up_pre = jnp.dot(picked, w_up[...], preferred_element_type=jnp.float32)
        hidden_grad = cols_product(scaled, w_down[...])
        sigmoid_gate = jax.nn.sigmoid(gate_pre)
        silu_gate = gate_pre * sigmoid_gate
        hidden[rows, :] = (silu_gate * up_pre).astype(jnp.bfloat16)
        gate = (
            hidden_grad * up_pre * sigmoid_gate * (1.0 + gate_pre * (1.0 - sigmoid_gate))
        ).astype(jnp.bfloat16)
        up = (hidden_grad * silu_gate).astype(jnp.bfloat16)
        across_hidden = gate.shape[1]
        both_grad[rows, pl.ds(0, across_hidden)] = gate
        both_grad[rows, pl.ds(across_hidden, across_hidden)] = up
        for piece in range(wide // width):
            where = pl.ds(piece * width, width)
            partial[rows, where] = (
                cols_product(gate, w_gate[where, :]) + cols_product(up, w_up[where, :])
            ).astype(jnp.bfloat16)

    def work(g):
        def await_one(i):
            s = g * group + i

            @pl.when(s > 0)
            def _():
                ready(s)

        loop(0, group, await_one)
        compute(g)

        def hand_one(i):
            s = g * group + i
            hand(1, s).start()
            hand(0, s).start()

        loop(0, group, hand_one)

    groups = n // group
    with jax.named_scope("work_own"):
        for i in range(3):
            loads[i].wait()
        loop(0, groups // 2, work)

    def land_other(k):
        land(half + k, k)

    def pair(s):
        hand(1, s).wait_recv()
        mine = partial[at(s), columns(cross, width)].astype(jnp.float32)
        far_out[at(s), :] = (mine + near[1, at(s), :].astype(jnp.float32)).astype(jnp.bfloat16)
        across(s).start()

    with jax.named_scope("land_other"):
        loop(1, half, land_other)
        mix_copy(half, half, half).wait_recv()

        def mix_other(k):
            mix_copy(half, half + k, k).start()

        loop(1, half, mix_other)

    def forward_group(g):
        loop(0, group, lambda i: forward_both(g * group + i))

    def pair_group(g):
        loop(0, group, lambda i: pair(g * group + i))

    def work_other(g):
        with jax.named_scope("forward_group"):
            forward_group(g)
        with jax.named_scope("work_group"):
            work(g)

        @pl.when(g < groups - 1)
        def _():
            pair_group(g)

    loop(groups // 2, groups, work_other)
    with jax.named_scope("pair_own"):
        loop(0, half, pair)
    with jax.named_scope("pair_last"):
        pair_group(groups - 1)

    def finish(s):
        hand(0, s).wait_recv()
        across(s).wait_recv()
        mine = partial[at(s), columns(tp, width)].astype(jnp.float32)
        return (
            mine + near[0, at(s), :].astype(jnp.float32) + far_in[at(s), :].astype(jnp.float32)
        ).astype(jnp.bfloat16)

    def finish_one(s):
        total[at(s), :] = finish(s)
        give(s).start()

    def grads(c):
        rows = pl.ds(pl.multiple_of(c * chunk, chunk), chunk)
        sums = rows_product(slots[0, :, rows], both_grad[...])
        gate_sum[rows, :] = sums[:, : sums.shape[1] // 2]
        up_sum[rows, :] = sums[:, sums.shape[1] // 2 :]
        down_sum[:, rows] = rows_product(hidden[...], slots[1, :, rows])

    pieces_of = wide // chunk
    with jax.named_scope("finish_other"):
        loop(half, n - group, finish_one)
    with jax.named_scope("grads"):
        loop(0, pieces_of // 2, grads)
    with jax.named_scope("finish_own"):
        loop(1, half, finish_one)
        back[pl.ds(0, depth), :] = finish(0)
    with jax.named_scope("finish_last"):
        loop(n - group, n, finish_one)
    with jax.named_scope("grads"):
        loop(pieces_of // 2, pieces_of, grads)
    acc[...] = jnp.zeros_like(acc)

    def combine(s):
        @pl.when(s > 0)
        def _():
            give(s).wait_recv()

        mask = jnp.where(placing(0, other(s)), 1.0, 0.0).astype(jnp.bfloat16)
        acc[...] += rows_product(mask, back[at(s), :])

    with jax.named_scope("combine"):
        loop(0, n, combine)
    pieces = all_cross.shape[0]
    tall = count // pieces

    def shared(i, column, send, recv, peer):
        part = token.at[pl.ds(i * tall, tall), columns(column, width)]
        return remote(part, part, send, recv, {"tp": peer})

    with jax.named_scope("share"):
        token[:, columns(tp, width)] = acc[...].astype(jnp.bfloat16)
        for i in range(pieces):
            shared(i, tp, all_send.at[0, i], all_cross.at[i], cross).start()
            shared(i, tp, all_send.at[1, i], all_near.at[0, i], partner).start()
        for i in range(pieces):
            shared(i, cross, all_send.at[0, i], all_cross.at[i], cross).wait_recv()
            shared(i, cross, all_send.at[2, i], all_near.at[1, i], partner).start()
        for i in range(pieces):
            for j in (0, 1):
                shared(i, tp, all_send.at[j + 1, i], all_near.at[j, i], partner).wait()
            shared(i, tp, all_send.at[0, i], all_cross.at[i], cross).wait_send()

    def reduce_along(i):
        rows = pl.ds(pl.multiple_of(i * 32, 32), 32)
        unit = stream[rows, :].astype(jnp.float32) * inverse[rows, :]
        unit_grad = token[rows, :].astype(jnp.float32) * gain[...]
        along[rows, :] = jnp.mean(unit * unit_grad, axis=-1, keepdims=True)

    def total_grad(c):
        where = pl.ds(pl.multiple_of(c * chunk, chunk), chunk)
        scale = inverse[...]
        unit = stream[:, where].astype(jnp.float32) * scale
        unit_grad = token[:, where].astype(jnp.float32) * gain[:, where]
        value = cot[:, where].astype(jnp.float32) + scale * (unit_grad - unit * along[...])
        value = value.astype(jnp.bfloat16)
        stream_grad[:, where] = value
        turned[where, :] = jnp.transpose(value.astype(jnp.float32)).astype(jnp.bfloat16)

    with jax.named_scope("stream_grad"):
        loop(0, count // 32, reduce_along)
        loop(0, wide // chunk, total_grad)

    def turned_rows(owner, part):
        return pl.ds(pl.multiple_of(owner * block + part * share, share), share)

    def part_rows(part):
        return pl.ds(pl.multiple_of(part * share, share), share)

    mine_part = tp if shared_parts > 1 else 0
    cross_part = cross if shared_parts > 1 else 0

    def turn_copy(s):
        return remote(
            turned.at[turned_rows(other(s), mine_part)],
            turned_all.at[s, part_rows(mine_part)],
            turn_send.at[0],
            turn_recv.at[s],
            {"sp": other(s)},
        )

    def turn_part(s, part, send, recv, peer):
        rows = turned_all.at[s, part_rows(part)]
        return remote(rows, rows, send, recv, {"tp": peer})

    def turn_start(s):
        turn_copy(s).start()

    with jax.named_scope("mixed_grad"):
        loop(1, n, turn_start)
        stream_out[...] = stream_grad[:, columns(tp, width)]
        loads[3].wait()
        mixed_grad = jnp.dot(stream_grad[...], w_out[...], preferred_element_type=jnp.float32)
        small_out[0] = (mixed_grad * filtered[...]).astype(jnp.bfloat16)
        extended_grad[pl.ds(0, count), :] = mixed_grad * out_gate[...].astype(jnp.float32)

        @pl.when(me > 0)
        def _():
            halo_earlier().start()

    def turn_land(s):
        turn_copy(s).wait_recv()
        if shared_parts > 1:
            turn_part(s, tp, turn_send.at[1], turn_cross.at[s], cross).start()
            turn_part(s, tp, turn_send.at[2], turn_near.at[s], partner).start()

    def turn_forward(s):
        turn_part(s, cross, turn_send.at[1], turn_cross.at[s], cross).wait_recv()
        turn_part(s, cross, turn_send.at[3], turn_near.at[s], partner).start()

    with jax.named_scope("turn_land"):
        loop(1, n, turn_land)
    with jax.named_scope("turn_forward"):
        if shared_parts > 1:
            loop(1, n, turn_forward)

    with jax.named_scope("conv_grad"):
        @pl.when(me < n - 1)
        def _():
            halo_earlier().wait_recv()

        product_grad = (
            taps[0:1, :] * extended_grad[pl.ds(0, count), :]
            + taps[1:2, :] * extended_grad[pl.ds(1, count), :]
            + taps[2:3, :] * extended_grad[pl.ds(2, count), :]
        )
        small_out[1] = (product_grad * conv_input[...].astype(jnp.float32)).astype(jnp.bfloat16)
        small_out[2] = (product_grad * in_gate[...].astype(jnp.float32)).astype(jnp.bfloat16)

    w_out_sum[...] = jnp.dot(
        turned[pl.ds(pl.multiple_of(me * block, block), block), :],
        mixed[0],
        preferred_element_type=jnp.float32,
    )

    def out_step(s):
        if shared_parts > 1:
            pair_rows = turned_all.at[s, pl.ds(0, 2 * share)]
            remote(
                pair_rows, pair_rows, turn_send.at[2], turn_near.at[s], {"tp": partner}
            ).wait_recv()

        @pl.when(s < half)
        def _():
            mix_copy(0, s, s).wait_recv()

        @pl.when(s > half)
        def _():
            mix_copy(half, s, s - half).wait_recv()

        w_out_sum[...] += jnp.dot(turned_all[s], mixed[s], preferred_element_type=jnp.float32)

    with jax.named_scope("w_out_grad"):
        loop(1, n, out_step)

    with jax.named_scope("drain"):
        for one in route_copies():
            one.wait_send()
        for a in (0, 1):
            token_copy(a).wait_send()
            sent = sending.at[a, pl.ds(0, (n - 2) * depth)]
            remote(sent, sent, slot_send.at[a], slot_recv.at[a, 0], {"tp": partner}).wait_send()
            most = slots.at[a, pl.ds(0, (n - 1) * depth), pl.ds(0, width)]
            for sem in (cross_send, near_send, fwd_send):
                remote(most, most, sem.at[a], near_recv.at[a, 0], {"tp": partner}).wait_send()
            remote(far_out, far_in, hand_send.at[a], hand_recv.at[a, 0], {"tp": partner}).wait_send()
        remote(far_out, far_in, far_send, far_recv.at[0], {"tp": cross}).wait_send()
        rest = total.at[pl.ds(0, (n - 1) * depth)]
        remote(rest, rest, out_send, out_recv.at[0], {"tp": partner}).wait_send()
        sent = mixed.at[pl.ds(0, n - 1)]
        remote(sent, sent, mix_send, mix_recv.at[0], {"tp": partner}).wait_send()
        sent = turned_all.at[pl.ds(0, n - 1), pl.ds(0, share)]
        for kind in range(4 if shared_parts > 1 else 1):
            remote(sent, sent, turn_send.at[kind], turn_recv.at[0], {"tp": partner}).wait_send()

        @pl.when(me < n - 1)
        def _():
            halo_later().wait_send()

        @pl.when(me > 0)
        def _():
            halo_earlier().wait_send()


def store_kernel(stream, small, w_out, gate, up, down, *rest):
    outs, local = rest[:8], rest[8]
    ins = (stream, small.at[0], small.at[1], small.at[2], w_out, gate, up, down)
    copies = [
        pltpu.make_async_copy(source, target, local.at[i])
        for i, (source, target) in enumerate(zip(ins, outs))
    ]
    for one in copies:
        one.start()
    for one in copies:
        one.wait()


def shards(
    cotangent,
    stream_in,
    norm_gain,
    out_gate,
    in_gate,
    conv_input,
    conv_taps,
    out_weight,
    expert_gate,
    expert_up,
    expert_down,
    expert_choice,
    route_scale,
):
    n = lax.axis_size("sp")
    count, wide = stream_in.shape
    channels = out_gate.shape[1]
    hidden = expert_gate.shape[2]
    width = wide // lax.axis_size("tp")
    depth = 4 * count // n
    rows = n * depth
    block = wide // n
    pieces = 2
    kind = stream_in.dtype

    def out(*shape, dtype=kind):
        return jax.ShapeDtypeStruct(shape, dtype)

    def full(*shape):
        return pltpu.VMEM(shape, jnp.float32)

    def held(*shape):
        return pltpu.VMEM(shape, kind)

    vmem, anywhere = (pl.BlockSpec(memory_space=pltpu.VMEM), pl.BlockSpec(memory_space=pl.ANY))
    dma = pltpu.SemaphoreType.DMA
    results = pl.pallas_call(
        functools.partial(step_kernel, n),
        out_shape=[
            out(count, width),
            out(3, count, channels),
            out(block, channels, dtype=jnp.float32),
            out(wide, hidden, dtype=jnp.float32),
            out(wide, hidden, dtype=jnp.float32),
            out(hidden, wide, dtype=jnp.float32),
        ],
        in_specs=[vmem] * 9 + [anywhere] * 4,
        out_specs=[vmem] * 6,
        scratch_shapes=[
            held(count, wide),
            full(count, 1),
            full(count, 1),
            held(wide, channels),
            held(wide, hidden),
            held(wide, hidden),
            held(hidden, wide),
            full(2, n, count),
            full(2, n, count),
            held(2, count, width),
            pltpu.VMEM((2, count), jnp.int32),
            full(2, count),
            held(2, rows, width),
            held(2, rows, wide),
            held(rows, hidden),
            held(rows, 2 * hidden),
            held(rows, wide),
            held(2, rows, width),
            held(rows, width),
            held(rows, width),
            held(rows, width),
            held(rows, width),
            full(count, width),
            held(count, wide),
            full(count + 8, channels),
            full(count, channels),
            full(count + 8, channels),
            held(n, count, channels),
            held(count, wide),
            held(wide, count),
            held(n, block, count),
            dma((4,)),
            dma((4,)),
            dma((4,)),
            dma((2,)),
            dma((2, n)),
            dma((2,)),
            dma((2, n)),
            dma((2,)),
            dma((2,)),
            dma((2, n)),
            dma((2,)),
            dma((2, n)),
            dma,
            dma((n,)),
            dma,
            dma((n,)),
            dma((3, pieces)),
            dma((pieces,)),
            dma((2, pieces)),
            dma((2,)),
            dma((2,)),
            dma,
            dma((n,)),
            dma((4,)),
            dma((n,)),
            dma((n,)),
            dma((n,)),
        ],
        compiler_params=pltpu.CompilerParams(
            collective_id=1, has_side_effects=True, vmem_limit_bytes=VMEM + 2 * n * count * channels
        ),
    )(
        stream_in,
        cotangent,
        norm_gain[None],
        expert_choice.T,
        route_scale.T,
        out_gate,
        in_gate,
        conv_input,
        conv_taps,
        *(
            pltpu.with_memory_space_constraint(weight, pltpu.HBM)
            for weight in (out_weight, expert_gate[0], expert_up[0], expert_down[0])
        ),
    )
    stored = pl.pallas_call(
        store_kernel,
        out_shape=[
            out(count, width),
            out(count, channels),
            out(count, channels),
            out(count, channels),
            out(block, channels, dtype=jnp.float32),
            out(wide, hidden, dtype=jnp.float32),
            out(wide, hidden, dtype=jnp.float32),
            out(hidden, wide, dtype=jnp.float32),
        ],
        in_specs=[vmem] * 6,
        out_specs=[anywhere] * 8,
        scratch_shapes=[dma((8,))],
        compiler_params=pltpu.CompilerParams(vmem_limit_bytes=9 * 1024 * 1024),
    )(*results)
    return (*stored[:5], *(grad[None] for grad in stored[5:]))


def solution(mesh):
    placed = (
        P("sp", None),
        P("sp", None),
        P(),
        P("sp", "tp"),
        P("sp", "tp"),
        P("sp", "tp"),
        P(None, "tp"),
        P(None, "tp"),
        P("sp", None, "tp"),
        P("sp", None, "tp"),
        P("sp", "tp", None),
        P("sp", None),
        P("sp", None),
    )
    return jax.shard_map(
        shards,
        mesh=mesh,
        in_specs=placed,
        out_specs=(
            P("sp", "tp"),
            P("sp", "tp"),
            P("sp", "tp"),
            P("sp", "tp"),
            P("sp", "tp"),
            P("sp", None, "tp"),
            P("sp", None, "tp"),
            P("sp", "tp", None),
        ),
        check_vma=False,
    )
```

```python
import functools

import jax
import jax.numpy as jnp
from jax import lax
from jax.experimental import pallas as pl
from jax.experimental.pallas import tpu as pltpu
from jax.sharding import PartitionSpec as P

norm_eps = 1e-06
VMEM = 42 * 1024 * 1024


def rows_product(left, right):
    return lax.dot_general(
        left, right, (((0,), (0,)), ((), ())), preferred_element_type=jnp.float32
    )


def cols_product(left, right):
    return lax.dot_general(
        left, right, (((1,), (1,)), ((), ())), preferred_element_type=jnp.float32
    )


MESH = pl.DeviceIdType.MESH


def remote(source, target, send_sem, recv_sem, device):
    return pltpu.make_async_remote_copy(
        src_ref=source,
        dst_ref=target,
        send_sem=send_sem,
        recv_sem=recv_sem,
        device_id=device,
        device_id_type=MESH,
    )


def columns(index, width):
    return pl.ds(pl.multiple_of(index * width, width), width)


def mirrored(me, mask, n):
    found, unit = 0, 1
    while unit < n:
        found = found + lax.rem(lax.div(me, unit) + lax.div(mask, unit), 2) * unit
        unit = 2 * unit
    return found


def tp_places():
    tp, count = lax.axis_index("tp"), lax.axis_size("tp")
    cross = lax.rem(tp + count // 2, count)
    partner = tp + 1 - 2 * lax.rem(tp, 2)
    return (tp, cross, partner, lax.rem(partner + count // 2, count))


def greet(cross, partner):
    barrier = pltpu.get_barrier_semaphore()
    for peer in (cross, partner):
        pl.semaphore_signal(barrier, inc=1, device_id={"tp": peer}, device_id_type=MESH)
    me, n = lax.axis_index("sp"), lax.axis_size("sp")

    def greet_one(k, carry):
        peer = lax.rem(me + k, n)
        pl.semaphore_signal(barrier, inc=1, device_id={"sp": peer}, device_id_type=MESH)
        return carry

    lax.fori_loop(1, n, greet_one, 0)
    return lambda: pl.semaphore_wait(barrier, n + 1)


def loop(low, high, body):
    def step(k, carry):
        body(k)
        return carry

    lax.fori_loop(low, high, step, 0)


def step_kernel(
    n,
    *refs,
):
    inputs, refs = refs[:13], refs[13:]
    (
        stream_out,
        small_out,
        w_out_sum,
        gate_sum,
        up_sum,
        down_sum,
        normed,
        inverse,
        along,
        keys,
        weights,
        arrived,
        arrived_choice,
        arrived_scales,
        sending,
        slots,
        hidden,
        both_grad,
        partial,
        near,
        far_out,
        far_in,
        total,
        back,
        acc,
        token,
        extended,
        filtered,
        extended_grad,
        mixed,
        stream_grad,
        turned,
        turned_all,
        load,
        tok_send,
        tok_recv,
        slot_send,
        slot_recv,
        cross_send,
        cross_recv,
        near_send,
        fwd_send,
        near_recv,
        hand_send,
        hand_recv,
        far_send,
        far_recv,
        out_send,
        out_recv,
        all_send,
        all_cross,
        all_near,
        halo_send,
        halo_recv,
        mix_send,
        mix_recv,
        turn_send,
        turn_recv,
        turn_cross,
        turn_near,
    ) = refs[:6] + refs[19:]
    loaded = refs[6:19]
    (
        stream,
        cot,
        gain,
        choice,
        scales,
        out_gate,
        in_gate,
        conv_input,
        taps,
        w_out,
        w_gate,
        w_up,
        w_down,
    ) = loaded
    me = lax.axis_index("sp")
    tp, cross, partner, diagonal = tp_places()
    half = n // 2
    count, wide = normed.shape
    width = acc.shape[1]
    depth = near.shape[1] // n
    group = max(1, n // 4)
    span = group * depth
    chunk = min(256, width)
    channels = filtered.shape[1]
    block = wide // n
    shared_parts = wide // width
    shared_parts = shared_parts if block % (16 * shared_parts) == 0 else 1
    share = block // shared_parts
    wait_all = greet(cross, partner)
    sources = (normed, cot)
    edge = lax.rem(lax.div(me, max(1, n // 4)) + 1, 4) < 2
    inner = jnp.logical_not(edge)
    loads = [
        pltpu.make_async_copy(source, target, load.at[i])
        for i, (source, target) in enumerate(zip(inputs, loaded))
    ]
    for one in loads:
        one.start()

    def other(s):
        return mirrored(me, jnp.int32(s), n)

    def at(s):
        return pl.ds(pl.multiple_of(s * depth, depth), depth)

    def normalize(i):
        rows = pl.ds(pl.multiple_of(i * 32, 32), 32)
        values = stream[rows, :].astype(jnp.float32)
        scale = lax.rsqrt(jnp.mean(values * values, axis=-1, keepdims=True) + norm_eps)
        inverse[rows, :] = scale
        normed[rows, :] = (values * scale * gain[...]).astype(jnp.bfloat16)

    def table(which, named, scaled):
        c0, c1 = (named[i : i + 1, :] for i in range(2))
        s0, s1 = (scaled[i : i + 1, :] for i in range(2))
        expert = lax.broadcasted_iota(jnp.int32, (n, count), 0)
        first, second = (c0 == expert, c1 == expert)
        member = jnp.where(first | second, 1.0, 0.0)
        row = lax.broadcasted_iota(jnp.int32, (count, count), 0)
        column = lax.broadcasted_iota(jnp.int32, (count, count), 1)
        before = jnp.where(row < column, 1.0, 0.0).astype(jnp.bfloat16)
        earlier = jnp.dot(
            member.astype(jnp.bfloat16), before, preferred_element_type=jnp.float32
        )
        keys[which] = jnp.where(member > 0.0, earlier, -1.0)
        weights[which] = jnp.where(first, s0, 0.0) + jnp.where(second, s1, 0.0)

    def placing(which, expert):
        slot = lax.broadcasted_iota(jnp.int32, (depth, count), 0).astype(jnp.float32)
        return slot == keys[which, pl.ds(expert, 1), :]

    def chosen(a, which, expert, values):
        mask = placing(which, expert)
        found = jnp.dot(
            jnp.where(mask, 1.0, 0.0).astype(jnp.bfloat16),
            values,
            preferred_element_type=jnp.float32,
        )
        if a == 1:
            weight = jnp.where(mask, weights[which, pl.ds(expert, 1), :], 0.0)
            found = found * jnp.sum(weight, axis=1, keepdims=True)
        return found.astype(jnp.bfloat16)

    def token_copy(a):
        return remote(
            sources[a].at[:, columns(tp, width)],
            arrived.at[a],
            tok_send.at[a],
            tok_recv.at[a],
            {"sp": other(half)},
        )

    def route_copies():
        pairs = ((choice, arrived_choice), (scales, arrived_scales))
        return [
            remote(source, target, tok_send.at[2 + i], tok_recv.at[2 + i], {"sp": other(half)})
            for i, (source, target) in enumerate(pairs)
        ]

    def slot_copy(a, s, k):
        return remote(
            sending.at[a, at(s)],
            slots.at[a, at(s), columns(tp, width)],
            slot_send.at[a],
            slot_recv.at[a, s],
            {"sp": other(k)},
        )

    def spread(a, s):
        part = slots.at[a, at(s), columns(tp, width)]
        remote(part, part, cross_send.at[a], cross_recv.at[a, s], {"tp": cross}).start()
        remote(part, part, near_send.at[a], near_recv.at[a, s], {"tp": partner}).start()

    def forward(a, s):
        part = slots.at[a, at(s), columns(cross, width)]
        remote(part, part, cross_send.at[a], cross_recv.at[a, s], {"tp": cross}).wait_recv()
        remote(part, part, fwd_send.at[a], near_recv.at[a, s], {"tp": partner}).start()

    def ready(s):
        for a in (0, 1):
            both = slots.at[a, at(s), pl.ds(0, 2 * width)]
            remote(both, both, near_send.at[a], near_recv.at[a, s], {"tp": partner}).wait_recv()

    def hand(j, s):
        return remote(
            partial.at[at(s), columns((partner, diagonal)[j], width)],
            near.at[j, at(s)],
            hand_send.at[j],
            hand_recv.at[j, s],
            {"tp": partner},
        )

    def across(s):
        return remote(
            far_out.at[at(s)], far_in.at[at(s)], far_send, far_recv.at[s], {"tp": cross}
        )

    def give(s):
        return remote(
            total.at[at(s)], back.at[at(s)], out_send, out_recv.at[s], {"sp": other(s)}
        )

    def halo_later():
        peer = lax.rem(me + 1, n)
        return remote(
            extended.at[pl.ds(count, 8)],
            extended.at[pl.ds(0, 8)],
            halo_send.at[0],
            halo_recv.at[0],
            {"sp": peer},
        )

    def halo_earlier():
        peer = lax.rem(me + n - 1, n)
        return remote(
            extended_grad.at[pl.ds(0, 8)],
            extended_grad.at[pl.ds(count, 8)],
            halo_send.at[1],
            halo_recv.at[1],
            {"sp": peer},
        )

    def mix_copy(source, target, k):
        return remote(
            mixed.at[source], mixed.at[target], mix_send, mix_recv.at[target], {"sp": other(k)}
        )

    with jax.named_scope("prep"):
        loads[0].wait()
        loads[2].wait()
        loop(0, count // 32, normalize)
        loads[3].wait()
        loads[4].wait()
        table(0, choice, scales)
        loads[6].wait()
        loads[7].wait()
        product = in_gate[...].astype(jnp.float32) * conv_input[...].astype(jnp.float32)
        extended[pl.ds(8, count), :] = product

        @pl.when(me == 0)
        def _():
            extended[pl.ds(0, 8), :] = jnp.zeros((8, channels), jnp.float32)

        @pl.when(me == n - 1)
        def _():
            extended_grad[pl.ds(count, 8), :] = jnp.zeros((8, channels), jnp.float32)

    with jax.named_scope("barrier"):
        wait_all()
        loads[1].wait()

    def send_own(k):
        for a in (0, 1):
            values = sources[a][:, columns(tp, width)]
            sending[a, at(k), :] = chosen(a, 0, other(k), values)
            slot_copy(a, k, k).start()

    with jax.named_scope("send_own"):
        loop(1, group, send_own)

        @pl.when(edge)
        def _():
            for one in route_copies():
                one.start()
            token_copy(0).start()
            token_copy(1).start()

        loop(group, half, send_own)

        @pl.when(me < n - 1)
        def _():
            halo_later().start()

    with jax.named_scope("own_block"):
        for a in (0, 1):
            for piece in range(wide // width):
                where = pl.ds(piece * width, width)
                slots[a, pl.ds(0, depth), where] = chosen(a, 0, me, sources[a][:, where])

    def land(s, k):
        for a in (0, 1):
            slot_copy(a, s, k).wait_recv()
            spread(a, s)

    def land_own(k):
        land(k, k)

    def land_other(k):
        land(half + k, k)

    def take_tokens():
        for a in (0, 1):
            if a == 0:
                for one in route_copies():
                    one.wait_recv()
                table(1, arrived_choice, arrived_scales)
            token_copy(a).wait_recv()

            @pl.when(inner)
            def _():
                if a == 0:
                    for one in route_copies():
                        one.start()
                token_copy(a).start()

            def send_other(k):
                sending[a, at(half + k), :] = chosen(a, 1, other(k), arrived[a])
                slot_copy(a, half + k, k).start()

            loop(1, half, send_other)
            slots[a, at(half), columns(tp, width)] = chosen(a, 1, me, arrived[a])
            spread(a, half)

    def forward_both(s):
        for a in (0, 1):
            forward(a, s)

    def mix_early():
        mix_copy(0, half, half).start()
        loop(1, half, lambda k: mix_copy(0, k, k).start())

    def mix_late():
        mix_copy(half, half, half).wait_recv()
        loop(1, half, lambda k: mix_copy(half, half + k, k).start())

    def compute(g):
        rows = pl.ds(pl.multiple_of(g * span, span), span)
        picked, scaled = (slots[0, rows, :], slots[1, rows, :])
        gate_pre = jnp.dot(picked, w_gate[...], preferred_element_type=jnp.float32)
        up_pre = jnp.dot(picked, w_up[...], preferred_element_type=jnp.float32)
        hidden_grad = cols_product(scaled, w_down[...])
        sigmoid_gate = jax.nn.sigmoid(gate_pre)
        silu_gate = gate_pre * sigmoid_gate
        hidden[rows, :] = (silu_gate * up_pre).astype(jnp.bfloat16)
        gate = (
            hidden_grad * up_pre * sigmoid_gate * (1.0 + gate_pre * (1.0 - sigmoid_gate))
        ).astype(jnp.bfloat16)
        up = (hidden_grad * silu_gate).astype(jnp.bfloat16)
        across_hidden = gate.shape[1]
        both_grad[rows, pl.ds(0, across_hidden)] = gate
        both_grad[rows, pl.ds(across_hidden, across_hidden)] = up
        for piece in range(wide // width):
            where = pl.ds(piece * width, width)
            partial[rows, where] = (
                cols_product(gate, w_gate[where, :]) + cols_product(up, w_up[where, :])
            ).astype(jnp.bfloat16)

    def work(g):
        def await_one(i):
            s = g * group + i

            @pl.when(s > 0)
            def _():
                ready(s)

        loop(0, group, await_one)
        compute(g)

        def hand_one(i):
            s = g * group + i
            hand(1, s).start()
            hand(0, s).start()

        loop(0, group, hand_one)

    def pair(s):
        hand(1, s).wait_recv()
        mine = partial[at(s), columns(cross, width)].astype(jnp.float32)
        far_out[at(s), :] = (mine + near[1, at(s), :].astype(jnp.float32)).astype(jnp.bfloat16)
        across(s).start()

    def pair_group(g):
        loop(0, group, lambda i: pair(g * group + i))

    def step(g):
        def forward_one(i):
            s = g * group + i

            @pl.when(s > 0)
            def _():
                forward_both(s)

        with jax.named_scope("forward_group"):
            loop(0, group, forward_one)
        with jax.named_scope("work_group"):
            work(g)

    def finish(s):
        hand(0, s).wait_recv()
        across(s).wait_recv()
        mine = partial[at(s), columns(tp, width)].astype(jnp.float32)
        return (
            mine + near[0, at(s), :].astype(jnp.float32) + far_in[at(s), :].astype(jnp.float32)
        ).astype(jnp.bfloat16)

    def finish_one(s):
        total[at(s), :] = finish(s)
        give(s).start()

    def grads(c):
        rows = pl.ds(pl.multiple_of(c * chunk, chunk), chunk)
        sums = rows_product(slots[0, :, rows], both_grad[...])
        gate_sum[rows, :] = sums[:, : sums.shape[1] // 2]
        up_sum[rows, :] = sums[:, sums.shape[1] // 2 :]
        down_sum[:, rows] = rows_product(hidden[...], slots[1, :, rows])

    def finish_group(g):
        def one(i):
            s = g * group + i

            @pl.when(s > 0)
            def _():
                finish_one(s)

            @pl.when(s == 0)
            def _():
                back[pl.ds(0, depth), :] = finish(0)

        loop(0, group, one)

    with jax.named_scope("land_near"):
        loop(1, group, land_own)
    with jax.named_scope("filter"):
        @pl.when(me > 0)
        def _():
            halo_later().wait_recv()

        loads[5].wait()
        loads[8].wait()
        filtered[...] = (
            taps[0:1, :] * extended[pl.ds(8, count), :]
            + taps[1:2, :] * extended[pl.ds(7, count), :]
            + taps[2:3, :] * extended[pl.ds(6, count), :]
        )
        mixed[0] = (out_gate[...].astype(jnp.float32) * filtered[...]).astype(jnp.bfloat16)

    with jax.named_scope("land_first"):

        @pl.when(inner)
        def _():
            take_tokens()
            loop(1, group, land_other)
            loop(group, half, land_own)

        @pl.when(edge)
        def _():
            loop(group, half, land_own)

    for i in range(10, 13):
        loads[i].wait()
    step(jnp.where(edge, 0, 2))
    with jax.named_scope("land_second"):

        @pl.when(inner)
        def _():
            pair_group(2)
            loop(group, half, land_other)

        @pl.when(edge)
        def _():
            take_tokens()
            loop(1, half, land_other)

    mix_early()
    step(jnp.where(edge, 1, 0))
    step(jnp.where(edge, 2, 1))
    with jax.named_scope("return_far"):

        @pl.when(inner)
        def _():
            finish_group(2)

        @pl.when(edge)
        def _():
            pair_group(2)

        mix_late()
    step(3)
    pieces_of = wide // chunk
    with jax.named_scope("pairs"):
        pair_group(0)
        pair_group(3)
        pair_group(1)

        @pl.when(edge)
        def _():
            finish_group(2)

    with jax.named_scope("grads"):
        loop(0, pieces_of // 2, grads)
    with jax.named_scope("finish"):
        finish_group(0)
        finish_group(3)
        finish_group(1)
    with jax.named_scope("grads"):
        loop(pieces_of // 2, pieces_of, grads)
    acc[...] = jnp.zeros_like(acc)

    def combine(s):
        @pl.when(s > 0)
        def _():
            give(s).wait_recv()

        mask = jnp.where(placing(0, other(s)), 1.0, 0.0).astype(jnp.bfloat16)
        acc[...] += rows_product(mask, back[at(s), :])

    with jax.named_scope("combine"):
        loop(0, n, combine)
    pieces = all_cross.shape[0]
    tall = count // pieces

    def shared(i, column, send, recv, peer):
        part = token.at[pl.ds(i * tall, tall), columns(column, width)]
        return remote(part, part, send, recv, {"tp": peer})

    with jax.named_scope("share"):
        token[:, columns(tp, width)] = acc[...].astype(jnp.bfloat16)
        for i in range(pieces):
            shared(i, tp, all_send.at[0, i], all_cross.at[i], cross).start()
            shared(i, tp, all_send.at[1, i], all_near.at[0, i], partner).start()
        for i in range(pieces):
            shared(i, cross, all_send.at[0, i], all_cross.at[i], cross).wait_recv()
            shared(i, cross, all_send.at[2, i], all_near.at[1, i], partner).start()
        for i in range(pieces):
            for j in (0, 1):
                shared(i, tp, all_send.at[j + 1, i], all_near.at[j, i], partner).wait()
            shared(i, tp, all_send.at[0, i], all_cross.at[i], cross).wait_send()

    def reduce_along(i):
        rows = pl.ds(pl.multiple_of(i * 32, 32), 32)
        unit = stream[rows, :].astype(jnp.float32) * inverse[rows, :]
        unit_grad = token[rows, :].astype(jnp.float32) * gain[...]
        along[rows, :] = jnp.mean(unit * unit_grad, axis=-1, keepdims=True)

    def total_grad(c):
        where = pl.ds(pl.multiple_of(c * chunk, chunk), chunk)
        scale = inverse[...]
        unit = stream[:, where].astype(jnp.float32) * scale
        unit_grad = token[:, where].astype(jnp.float32) * gain[:, where]
        value = cot[:, where].astype(jnp.float32) + scale * (unit_grad - unit * along[...])
        value = value.astype(jnp.bfloat16)
        stream_grad[:, where] = value
        turned[where, :] = jnp.transpose(value.astype(jnp.float32)).astype(jnp.bfloat16)

    with jax.named_scope("stream_grad"):
        loop(0, count // 32, reduce_along)
        loop(0, wide // chunk, total_grad)

    def turned_rows(owner, part):
        return pl.ds(pl.multiple_of(owner * block + part * share, share), share)

    def part_rows(part):
        return pl.ds(pl.multiple_of(part * share, share), share)

    mine_part = tp if shared_parts > 1 else 0
    cross_part = cross if shared_parts > 1 else 0

    def turn_copy(s):
        return remote(
            turned.at[turned_rows(other(s), mine_part)],
            turned_all.at[s, part_rows(mine_part)],
            turn_send.at[0],
            turn_recv.at[s],
            {"sp": other(s)},
        )

    def turn_part(s, part, send, recv, peer):
        rows = turned_all.at[s, part_rows(part)]
        return remote(rows, rows, send, recv, {"tp": peer})

    def turn_start(k):
        turn_copy(n - k).start()

    with jax.named_scope("mixed_grad"):
        loop(1, n, turn_start)
        stream_out[...] = stream_grad[:, columns(tp, width)]
        loads[9].wait()
        mixed_grad = jnp.dot(stream_grad[...], w_out[...], preferred_element_type=jnp.float32)
        small_out[0] = (mixed_grad * filtered[...]).astype(jnp.bfloat16)
        extended_grad[pl.ds(0, count), :] = mixed_grad * out_gate[...].astype(jnp.float32)

        @pl.when(me > 0)
        def _():
            halo_earlier().start()

    def turn_land(s):
        turn_copy(s).wait_recv()
        if shared_parts > 1:
            turn_part(s, tp, turn_send.at[1], turn_cross.at[s], cross).start()
            turn_part(s, tp, turn_send.at[2], turn_near.at[s], partner).start()

    def turn_forward(s):
        turn_part(s, cross, turn_send.at[1], turn_cross.at[s], cross).wait_recv()
        turn_part(s, cross, turn_send.at[3], turn_near.at[s], partner).start()

    with jax.named_scope("turn_land"):
        loop(1, n, turn_land)
    with jax.named_scope("turn_forward"):
        if shared_parts > 1:
            loop(1, n, turn_forward)

    with jax.named_scope("conv_grad"):
        @pl.when(me < n - 1)
        def _():
            halo_earlier().wait_recv()

        product_grad = (
            taps[0:1, :] * extended_grad[pl.ds(0, count), :]
            + taps[1:2, :] * extended_grad[pl.ds(1, count), :]
            + taps[2:3, :] * extended_grad[pl.ds(2, count), :]
        )
        small_out[1] = (product_grad * conv_input[...].astype(jnp.float32)).astype(jnp.bfloat16)
        small_out[2] = (product_grad * in_gate[...].astype(jnp.float32)).astype(jnp.bfloat16)

    w_out_sum[...] = jnp.dot(
        turned[pl.ds(pl.multiple_of(me * block, block), block), :],
        mixed[0],
        preferred_element_type=jnp.float32,
    )

    def out_step(s):
        if shared_parts > 1:
            pair_rows = turned_all.at[s, pl.ds(0, 2 * share)]
            remote(
                pair_rows, pair_rows, turn_send.at[2], turn_near.at[s], {"tp": partner}
            ).wait_recv()

        @pl.when(s < half)
        def _():
            mix_copy(0, s, s).wait_recv()

        @pl.when(s > half)
        def _():
            mix_copy(half, s, s - half).wait_recv()

        w_out_sum[...] += jnp.dot(turned_all[s], mixed[s], preferred_element_type=jnp.float32)

    with jax.named_scope("w_out_grad"):
        loop(1, n, out_step)

    with jax.named_scope("drain"):
        for one in route_copies():
            one.wait_send()
        for a in (0, 1):
            token_copy(a).wait_send()
            sent = sending.at[a, pl.ds(0, (n - 2) * depth)]
            remote(sent, sent, slot_send.at[a], slot_recv.at[a, 0], {"tp": partner}).wait_send()
            most = slots.at[a, pl.ds(0, (n - 1) * depth), pl.ds(0, width)]
            for sem in (cross_send, near_send, fwd_send):
                remote(most, most, sem.at[a], near_recv.at[a, 0], {"tp": partner}).wait_send()
            remote(far_out, far_in, hand_send.at[a], hand_recv.at[a, 0], {"tp": partner}).wait_send()
        remote(far_out, far_in, far_send, far_recv.at[0], {"tp": cross}).wait_send()
        rest = total.at[pl.ds(0, (n - 1) * depth)]
        remote(rest, rest, out_send, out_recv.at[0], {"tp": partner}).wait_send()
        sent = mixed.at[pl.ds(0, n - 1)]
        remote(sent, sent, mix_send, mix_recv.at[0], {"tp": partner}).wait_send()
        sent = turned_all.at[pl.ds(0, n - 1), pl.ds(0, share)]
        for kind in range(4 if shared_parts > 1 else 1):
            remote(sent, sent, turn_send.at[kind], turn_recv.at[0], {"tp": partner}).wait_send()

        @pl.when(me < n - 1)
        def _():
            halo_later().wait_send()

        @pl.when(me > 0)
        def _():
            halo_earlier().wait_send()


def store_kernel(stream, small, w_out, gate, up, down, *rest):
    outs, local = rest[:8], rest[8]
    ins = (stream, small.at[0], small.at[1], small.at[2], w_out, gate, up, down)
    copies = [
        pltpu.make_async_copy(source, target, local.at[i])
        for i, (source, target) in enumerate(zip(ins, outs))
    ]
    for one in copies:
        one.start()
    for one in copies:
        one.wait()


def shards(
    cotangent,
    stream_in,
    norm_gain,
    out_gate,
    in_gate,
    conv_input,
    conv_taps,
    out_weight,
    expert_gate,
    expert_up,
    expert_down,
    expert_choice,
    route_scale,
):
    n = lax.axis_size("sp")
    count, wide = stream_in.shape
    channels = out_gate.shape[1]
    hidden = expert_gate.shape[2]
    width = wide // lax.axis_size("tp")
    depth = 4 * count // n
    rows = n * depth
    block = wide // n
    pieces = 2
    kind = stream_in.dtype

    def out(*shape, dtype=kind):
        return jax.ShapeDtypeStruct(shape, dtype)

    def full(*shape):
        return pltpu.VMEM(shape, jnp.float32)

    def held(*shape):
        return pltpu.VMEM(shape, kind)

    vmem, anywhere = (pl.BlockSpec(memory_space=pltpu.VMEM), pl.BlockSpec(memory_space=pl.ANY))
    dma = pltpu.SemaphoreType.DMA
    operands = (
        stream_in,
        cotangent,
        norm_gain[None],
        expert_choice.T,
        route_scale.T,
        out_gate,
        in_gate,
        conv_input,
        conv_taps,
        out_weight,
        expert_gate[0],
        expert_up[0],
        expert_down[0],
    )
    results = pl.pallas_call(
        functools.partial(step_kernel, n),
        out_shape=[
            out(count, width),
            out(3, count, channels),
            out(block, channels, dtype=jnp.float32),
            out(wide, hidden, dtype=jnp.float32),
            out(wide, hidden, dtype=jnp.float32),
            out(hidden, wide, dtype=jnp.float32),
        ],
        in_specs=[anywhere] * 13,
        out_specs=[vmem] * 6,
        scratch_shapes=[pltpu.VMEM(x.shape, x.dtype) for x in operands]
        + [
            held(count, wide),
            full(count, 1),
            full(count, 1),
            full(2, n, count),
            full(2, n, count),
            held(2, count, width),
            pltpu.VMEM((2, count), jnp.int32),
            full(2, count),
            held(2, rows, width),
            held(2, rows, wide),
            held(rows, hidden),
            held(rows, 2 * hidden),
            held(rows, wide),
            held(2, rows, width),
            held(rows, width),
            held(rows, width),
            held(rows, width),
            held(rows, width),
            full(count, width),
            held(count, wide),
            full(count + 8, channels),
            full(count, channels),
            full(count + 8, channels),
            held(n, count, channels),
            held(count, wide),
            held(wide, count),
            held(n, block, count),
            dma((13,)),
            dma((4,)),
            dma((4,)),
            dma((2,)),
            dma((2, n)),
            dma((2,)),
            dma((2, n)),
            dma((2,)),
            dma((2,)),
            dma((2, n)),
            dma((2,)),
            dma((2, n)),
            dma,
            dma((n,)),
            dma,
            dma((n,)),
            dma((3, pieces)),
            dma((pieces,)),
            dma((2, pieces)),
            dma((2,)),
            dma((2,)),
            dma,
            dma((n,)),
            dma((4,)),
            dma((n,)),
            dma((n,)),
            dma((n,)),
        ],
        compiler_params=pltpu.CompilerParams(
            collective_id=1, has_side_effects=True, vmem_limit_bytes=VMEM + 2 * n * count * channels
        ),
    )(*(pltpu.with_memory_space_constraint(x, pltpu.HBM) for x in operands))
    stored = pl.pallas_call(
        store_kernel,
        out_shape=[
            out(count, width),
            out(count, channels),
            out(count, channels),
            out(count, channels),
            out(block, channels, dtype=jnp.float32),
            out(wide, hidden, dtype=jnp.float32),
            out(wide, hidden, dtype=jnp.float32),
            out(hidden, wide, dtype=jnp.float32),
        ],
        in_specs=[vmem] * 6,
        out_specs=[anywhere] * 8,
        scratch_shapes=[dma((8,))],
        compiler_params=pltpu.CompilerParams(vmem_limit_bytes=9 * 1024 * 1024),
    )(*results)
    return (*stored[:5], *(grad[None] for grad in stored[5:]))


def solution(mesh):
    placed = (
        P("sp", None),
        P("sp", None),
        P(),
        P("sp", "tp"),
        P("sp", "tp"),
        P("sp", "tp"),
        P(None, "tp"),
        P(None, "tp"),
        P("sp", None, "tp"),
        P("sp", None, "tp"),
        P("sp", "tp", None),
        P("sp", None),
        P("sp", None),
    )
    return jax.shard_map(
        shards,
        mesh=mesh,
        in_specs=placed,
        out_specs=(
            P("sp", "tp"),
            P("sp", "tp"),
            P("sp", "tp"),
            P("sp", "tp"),
            P("sp", "tp"),
            P("sp", None, "tp"),
            P("sp", None, "tp"),
            P("sp", "tp", None),
        ),
        check_vma=False,
    )
```

```python
import functools

import jax
import jax.numpy as jnp
from jax import lax
from jax.experimental import pallas as pl
from jax.experimental.pallas import tpu as pltpu
from jax.sharding import PartitionSpec as P

norm_eps = 1e-06
VMEM = 83 * 512 * 1024


def rows_product(left, right):
    return lax.dot_general(
        left, right, (((0,), (0,)), ((), ())), preferred_element_type=jnp.float32
    )


def cols_product(left, right):
    return lax.dot_general(
        left, right, (((1,), (1,)), ((), ())), preferred_element_type=jnp.float32
    )


MESH = pl.DeviceIdType.MESH


def remote(source, target, send_sem, recv_sem, device):
    return pltpu.make_async_remote_copy(
        src_ref=source,
        dst_ref=target,
        send_sem=send_sem,
        recv_sem=recv_sem,
        device_id=device,
        device_id_type=MESH,
    )


def columns(index, width):
    return pl.ds(pl.multiple_of(index * width, width), width)


def mirrored(me, mask, n):
    found, unit = 0, 1
    while unit < n:
        found = found + lax.rem(lax.div(me, unit) + lax.div(mask, unit), 2) * unit
        unit = 2 * unit
    return found


def tp_places():
    tp, count = lax.axis_index("tp"), lax.axis_size("tp")
    cross = lax.rem(tp + count // 2, count)
    partner = tp + 1 - 2 * lax.rem(tp, 2)
    return (tp, cross, partner, lax.rem(partner + count // 2, count))


def greet(peers):
    barrier = pltpu.get_barrier_semaphore()
    for peer in peers:
        pl.semaphore_signal(barrier, inc=1, device_id={"tp": peer}, device_id_type=MESH)
    me, n = lax.axis_index("sp"), lax.axis_size("sp")

    def greet_one(k, carry):
        peer = lax.rem(me + k, n)
        pl.semaphore_signal(barrier, inc=1, device_id={"sp": peer}, device_id_type=MESH)
        return carry

    lax.fori_loop(1, n, greet_one, 0)
    return lambda: pl.semaphore_wait(barrier, n - 1 + len(peers))


def loop(low, high, body):
    def step(k, carry):
        body(k)
        return carry

    lax.fori_loop(low, high, step, 0)


def step_kernel(
    n,
    *refs,
):
    inputs, refs = refs[:13], refs[13:]
    (
        stream_out,
        small_out,
        w_out_sum,
        gate_sum,
        up_sum,
        down_sum,
        normed,
        inverse,
        keys,
        weights,
        arrived,
        arrived_choice,
        arrived_scales,
        sending,
        slots,
        hidden,
        both_grad,
        partial,
        near,
        far_out,
        far_in,
        total,
        back,
        acc,
        token,
        token_out,
        extended,
        filtered,
        extended_grad,
        mixed,
        stream_grad,
        turned,
        turned_all,
        load,
        tok_send,
        tok_recv,
        slot_send,
        slot_recv,
        cross_send,
        cross_recv,
        near_send,
        fwd_send,
        near_recv,
        hand_send,
        hand_recv,
        far_send,
        far_recv,
        out_send,
        out_recv,
        all_send,
        all_recv,
        row_send,
        row_recv,
        halo_send,
        halo_recv,
        mix_send,
        mix_recv,
        turn_send,
        turn_recv,
        turn_cross,
        turn_near,
    ) = refs[:6] + refs[19:]
    loaded = refs[6:19]
    (
        stream,
        cot,
        gain,
        choice,
        scales,
        out_gate,
        in_gate,
        conv_input,
        taps,
        w_out,
        w_gate,
        w_up,
        w_down,
    ) = loaded
    me = lax.axis_index("sp")
    tp, cross, partner, diagonal = tp_places()
    half = n // 2
    count, wide = normed.shape
    width = acc.shape[1]
    depth = near.shape[1] // n
    group = max(1, n // 4)
    span = group * depth
    chunk = min(256, width)
    channels = filtered.shape[1]
    block = wide // n
    wait_all = greet((cross, partner, diagonal))
    sources = (normed, cot)
    loads = [
        pltpu.make_async_copy(source, target, load.at[i])
        for i, (source, target) in enumerate(zip(inputs, loaded))
    ]
    for i in (3, 4, 1, 0, 2, 6, 7, 5, 8, 10, 11, 12, 9):
        loads[i].start()

    def other(s):
        return mirrored(me, jnp.int32(s), n)

    def at(s):
        return pl.ds(pl.multiple_of(s * depth, depth), depth)

    def normalize(i):
        rows = pl.ds(pl.multiple_of(i * 32, 32), 32)
        values = stream[rows, :].astype(jnp.float32)
        scale = lax.rsqrt(jnp.mean(values * values, axis=-1, keepdims=True) + norm_eps)
        inverse[rows, :] = scale
        normed[rows, :] = (values * scale * gain[...]).astype(jnp.bfloat16)

    def table(which, named, scaled):
        c0, c1 = (named[i : i + 1, :] for i in range(2))
        s0, s1 = (scaled[i : i + 1, :] for i in range(2))
        expert = lax.broadcasted_iota(jnp.int32, (n, count), 0)
        first, second = (c0 == expert, c1 == expert)
        member = jnp.where(first | second, 1.0, 0.0)
        row = lax.broadcasted_iota(jnp.int32, (count, count), 0)
        column = lax.broadcasted_iota(jnp.int32, (count, count), 1)
        before = jnp.where(row < column, 1.0, 0.0).astype(jnp.bfloat16)
        earlier = jnp.dot(
            member.astype(jnp.bfloat16), before, preferred_element_type=jnp.float32
        )
        keys[which] = jnp.where(member > 0.0, earlier, -1.0)
        weights[which] = jnp.where(first, s0, 0.0) + jnp.where(second, s1, 0.0)

    def placing(which, expert):
        slot = lax.broadcasted_iota(jnp.int32, (depth, count), 0).astype(jnp.float32)
        return slot == keys[which, pl.ds(expert, 1), :]

    def chosen(a, which, expert, values):
        mask = placing(which, expert)
        found = jnp.dot(
            jnp.where(mask, 1.0, 0.0).astype(jnp.bfloat16),
            values,
            preferred_element_type=jnp.float32,
        )
        if a == 1:
            weight = jnp.where(mask, weights[which, pl.ds(expert, 1), :], 0.0)
            found = found * jnp.sum(weight, axis=1, keepdims=True)
        return found.astype(jnp.bfloat16)

    def token_copy(a):
        return remote(
            sources[a].at[:, columns(tp, width)],
            arrived.at[a],
            tok_send.at[a],
            tok_recv.at[a],
            {"sp": other(half)},
        )

    def route_copies():
        pairs = ((choice, arrived_choice), (scales, arrived_scales))
        return [
            remote(source, target, tok_send.at[2 + i], tok_recv.at[2 + i], {"sp": other(half)})
            for i, (source, target) in enumerate(pairs)
        ]

    def slot_copy(a, s, k):
        return remote(
            sending.at[a, at(s)],
            slots.at[a, at(s), columns(tp, width)],
            slot_send.at[a],
            slot_recv.at[a, s],
            {"sp": other(k)},
        )

    def spread(a, s):
        part = slots.at[a, at(s), columns(tp, width)]
        remote(part, part, cross_send.at[a], cross_recv.at[a, s], {"tp": cross}).start()
        remote(part, part, near_send.at[a], near_recv.at[a, s], {"tp": partner}).start()

    def forward(a, s):
        part = slots.at[a, at(s), columns(cross, width)]
        remote(part, part, cross_send.at[a], cross_recv.at[a, s], {"tp": cross}).wait_recv()
        remote(part, part, fwd_send.at[a], near_recv.at[a, s], {"tp": partner}).start()

    def ready(s):
        for a in (0, 1):
            both = slots.at[a, at(s), pl.ds(0, 2 * width)]
            remote(both, both, near_send.at[a], near_recv.at[a, s], {"tp": partner}).wait_recv()

    def hand(j, s):
        return remote(
            partial.at[at(s), columns((partner, diagonal)[j], width)],
            near.at[j, at(s)],
            hand_send.at[j],
            hand_recv.at[j, s],
            {"tp": partner},
        )

    def across(s):
        return remote(
            far_out.at[at(s)], far_in.at[at(s)], far_send, far_recv.at[s], {"tp": cross}
        )

    def give(s):
        return remote(
            total.at[at(s)], back.at[at(s)], out_send, out_recv.at[s], {"sp": other(s)}
        )

    def halo_later():
        peer = lax.rem(me + 1, n)
        return remote(
            extended.at[pl.ds(count, 8)],
            extended.at[pl.ds(0, 8)],
            halo_send.at[0],
            halo_recv.at[0],
            {"sp": peer},
        )

    def halo_earlier():
        peer = lax.rem(me + n - 1, n)
        return remote(
            extended_grad.at[pl.ds(0, 8)],
            extended_grad.at[pl.ds(count, 8)],
            halo_send.at[1],
            halo_recv.at[1],
            {"sp": peer},
        )

    def mix_copy(source, target, k):
        return remote(
            mixed.at[source], mixed.at[target], mix_send, mix_recv.at[target], {"sp": other(k)}
        )

    def send_own(a, k):
        values = sources[a][:, columns(tp, width)]
        sending[a, at(k), :] = chosen(a, 0, other(k), values)
        slot_copy(a, k, k).start()

    with jax.named_scope("prep"):
        loads[3].wait()
        loads[4].wait()
        table(0, choice, scales)
        loads[1].wait()
    with jax.named_scope("barrier"):
        wait_all()
    with jax.named_scope("send_own"):
        loop(1, half, lambda k: send_own(1, k))
        loads[0].wait()
        loads[2].wait()
        loop(0, count // 32, normalize)
        loop(1, half, lambda k: send_own(0, k))
        for one in route_copies():
            one.start()
        token_copy(0).start()
        token_copy(1).start()
    with jax.named_scope("conv"):
        loads[6].wait()
        loads[7].wait()
        product = in_gate[...].astype(jnp.float32) * conv_input[...].astype(jnp.float32)
        extended[pl.ds(8, count), :] = product

        @pl.when(me == 0)
        def _():
            extended[pl.ds(0, 8), :] = jnp.zeros((8, channels), jnp.float32)

        @pl.when(me == n - 1)
        def _():
            extended_grad[pl.ds(count, 8), :] = jnp.zeros((8, channels), jnp.float32)

        @pl.when(me < n - 1)
        def _():
            halo_later().start()

    with jax.named_scope("own_block"):
        for a in (0, 1):
            for piece in range(wide // width):
                where = pl.ds(piece * width, width)
                slots[a, pl.ds(0, depth), where] = chosen(a, 0, me, sources[a][:, where])

    def land(s, k):
        for a in (1, 0):
            slot_copy(a, s, k).wait_recv()
            spread(a, s)

    def land_own(k):
        land(k, k)

    def land_other(k):
        land(half + k, k)

    def take_tokens():
        for a in (0, 1):
            if a == 0:
                for one in route_copies():
                    one.wait_recv()
                table(1, arrived_choice, arrived_scales)
            token_copy(a).wait_recv()

            def send_other(k):
                sending[a, at(half + k), :] = chosen(a, 1, other(k), arrived[a])
                slot_copy(a, half + k, k).start()

            loop(1, half, send_other)
            slots[a, at(half), columns(tp, width)] = chosen(a, 1, me, arrived[a])
            spread(a, half)

    def forward_both(s):
        for a in (0, 1):
            forward(a, s)

    def mix_early():
        mix_copy(0, half, half).start()
        loop(1, half, lambda k: mix_copy(0, k, k).start())

    def mix_late():
        mix_copy(half, half, half).wait_recv()
        loop(1, half, lambda k: mix_copy(half, half + k, k).start())

    def compute(g):
        rows = pl.ds(pl.multiple_of(g * span, span), span)
        picked, scaled = (slots[0, rows, :], slots[1, rows, :])
        gate_pre = jnp.dot(picked, w_gate[...], preferred_element_type=jnp.float32)
        up_pre = jnp.dot(picked, w_up[...], preferred_element_type=jnp.float32)
        hidden_grad = cols_product(scaled, w_down[...])
        sigmoid_gate = jax.nn.sigmoid(gate_pre)
        silu_gate = gate_pre * sigmoid_gate
        hidden[rows, :] = (silu_gate * up_pre).astype(jnp.bfloat16)
        gate = (
            hidden_grad * up_pre * sigmoid_gate * (1.0 + gate_pre * (1.0 - sigmoid_gate))
        ).astype(jnp.bfloat16)
        up = (hidden_grad * silu_gate).astype(jnp.bfloat16)
        across_hidden = gate.shape[1]
        both_grad[rows, pl.ds(0, across_hidden)] = gate
        both_grad[rows, pl.ds(across_hidden, across_hidden)] = up
        for piece in range(wide // width):
            where = pl.ds(piece * width, width)
            partial[rows, where] = (
                cols_product(gate, w_gate[where, :]) + cols_product(up, w_up[where, :])
            ).astype(jnp.bfloat16)

    def work(g):
        def await_one(i):
            s = g * group + i

            @pl.when(s > 0)
            def _():
                ready(s)

        loop(0, group, await_one)
        compute(g)

        def hand_one(i):
            s = g * group + i
            hand(1, s).start()
            hand(0, s).start()

        loop(0, group, hand_one)

    def pair(s):
        hand(1, s).wait_recv()
        mine = partial[at(s), columns(cross, width)].astype(jnp.float32)
        far_out[at(s), :] = (mine + near[1, at(s), :].astype(jnp.float32)).astype(jnp.bfloat16)
        across(s).start()

    def pair_group(g):
        loop(0, group, lambda i: pair(g * group + i))

    def step(g):
        def forward_one(i):
            s = g * group + i

            @pl.when(s > 0)
            def _():
                forward_both(s)

        with jax.named_scope("forward_group"):
            loop(0, group, forward_one)
        with jax.named_scope("work_group"):
            work(g)

    def finish(s):
        hand(0, s).wait_recv()
        across(s).wait_recv()
        mine = partial[at(s), columns(tp, width)].astype(jnp.float32)
        return (
            mine + near[0, at(s), :].astype(jnp.float32) + far_in[at(s), :].astype(jnp.float32)
        ).astype(jnp.bfloat16)

    def finish_one(s):
        total[at(s), :] = finish(s)
        give(s).start()

    def grads(c):
        rows = pl.ds(pl.multiple_of(c * chunk, chunk), chunk)
        sums = rows_product(slots[0, :, rows], both_grad[...])
        gate_sum[rows, :] = sums[:, : sums.shape[1] // 2]
        up_sum[rows, :] = sums[:, sums.shape[1] // 2 :]
        down_sum[:, rows] = rows_product(hidden[...], slots[1, :, rows])

    def finish_group(g):
        def one(i):
            s = g * group + i

            @pl.when(s > 0)
            def _():
                finish_one(s)

            @pl.when(s == 0)
            def _():
                back[pl.ds(0, depth), :] = finish(0)

        loop(0, group, one)

    with jax.named_scope("land_near"):
        loop(1, group, land_own)
    with jax.named_scope("filter"):
        @pl.when(me > 0)
        def _():
            halo_later().wait_recv()

        loads[5].wait()
        loads[8].wait()
        filtered[...] = (
            taps[0:1, :] * extended[pl.ds(8, count), :]
            + taps[1:2, :] * extended[pl.ds(7, count), :]
            + taps[2:3, :] * extended[pl.ds(6, count), :]
        )
        mixed[0] = (out_gate[...].astype(jnp.float32) * filtered[...]).astype(jnp.bfloat16)

    with jax.named_scope("land_first"):
        loop(group, half, land_own)
    for i in range(10, 13):
        loads[i].wait()
    step(0)
    with jax.named_scope("land_second"):
        take_tokens()
        loop(1, half, land_other)
    mix_early()
    step(1)
    step(2)
    with jax.named_scope("return_far"):
        pair_group(2)
        mix_late()
    step(3)
    pieces_of = wide // chunk
    with jax.named_scope("pairs"):
        pair_group(0)
        pair_group(3)
        pair_group(1)
        finish_group(2)
    with jax.named_scope("grads"):
        loop(0, pieces_of // 2, grads)
    with jax.named_scope("finish"):
        finish_group(0)
        finish_group(3)
        finish_group(1)
    with jax.named_scope("grads"):
        loop(pieces_of // 2, pieces_of, grads)
    acc[...] = jnp.zeros_like(acc)

    def combine(s):
        @pl.when(s > 0)
        def _():
            give(s).wait_recv()

        mask = jnp.where(placing(0, other(s)), 1.0, 0.0).astype(jnp.bfloat16)
        acc[...] += rows_product(mask, back[at(s), :])

    with jax.named_scope("combine"):
        loop(0, n, combine)
    quarter = token.shape[0]

    def quarter_rows(column):
        return pl.ds(pl.multiple_of(column * quarter, quarter), quarter)

    def exchange(j):
        peer = (cross, diagonal, partner)[j]
        return remote(
            token_out.at[quarter_rows(peer)],
            token.at[:, columns(tp, width)],
            all_send.at[j],
            all_recv.at[j],
            {"tp": peer},
        )

    with jax.named_scope("share"):
        token_out[...] = acc[...].astype(jnp.bfloat16)
        for j in range(3):
            exchange(j).start()
        token[:, columns(tp, width)] = token_out[quarter_rows(tp), :]
        for j in (2, 0, 1):
            exchange(j).wait_recv()

    def total_grad(i):
        here = pl.ds(pl.multiple_of(i * 16, 16), 16)
        rows = pl.ds(pl.multiple_of(tp * quarter + i * 16, 16), 16)
        scale = inverse[rows, :]
        unit = stream[rows, :].astype(jnp.float32) * scale
        unit_grad = token[here, :].astype(jnp.float32) * gain[...]
        along = jnp.mean(unit * unit_grad, axis=-1, keepdims=True)
        value = cot[rows, :].astype(jnp.float32) + scale * (unit_grad - unit * along)
        value = value.astype(jnp.bfloat16)
        stream_grad[rows, :] = value
        for owner in range(n):
            turned[owner, here, :] = value[:, owner * block : (owner + 1) * block]

    with jax.named_scope("stream_grad"):
        loop(0, quarter // 16, total_grad)

    def turn_copy(s):
        return remote(
            turned.at[other(s)],
            turned_all.at[s, quarter_rows(tp)],
            turn_send.at[0],
            turn_recv.at[s],
            {"sp": other(s)},
        )

    def turn_part(s, column, send, recv, peer):
        rows = turned_all.at[s, quarter_rows(column)]
        return remote(rows, rows, send, recv, {"tp": peer})

    def gather(column, j, recv, peer):
        rows = stream_grad.at[quarter_rows(column)]
        return remote(rows, rows, row_send.at[j], row_recv.at[recv], {"tp": peer})

    def turn_spread(s):
        turn_part(s, tp, turn_send.at[1], turn_cross.at[s], cross).start()
        turn_part(s, tp, turn_send.at[2], turn_near.at[s], partner).start()

    def turn_land(s):
        turn_copy(s).wait_recv()
        turn_spread(s)

    def turn_forward(s):
        turn_part(s, cross, turn_send.at[1], turn_cross.at[s], cross).wait_recv()
        turn_part(s, cross, turn_send.at[3], turn_near.at[s], partner).start()

    with jax.named_scope("turn_start"):
        loop(1, n, lambda k: turn_copy(n - k).start())
        gather(tp, 0, 0, cross).start()
        gather(tp, 1, 1, partner).start()
        turned_all[0, quarter_rows(tp), :] = turned[me]
        turn_spread(0)
    with jax.named_scope("gather"):
        gather(cross, 0, 0, cross).wait_recv()
        gather(cross, 2, 2, partner).start()
    with jax.named_scope("turn_land"):
        loop(1, n, turn_land)
    with jax.named_scope("mixed_grad"):
        gather(tp, 1, 1, partner).wait_recv()
        gather(tp, 2, 2, partner).wait_recv()
        loads[9].wait()
        mixed_grad = jnp.dot(stream_grad[...], w_out[...], preferred_element_type=jnp.float32)
        small_out[0] = (mixed_grad * filtered[...]).astype(jnp.bfloat16)
        extended_grad[pl.ds(0, count), :] = mixed_grad * out_gate[...].astype(jnp.float32)

        @pl.when(me > 0)
        def _():
            halo_earlier().start()

        stream_out[...] = stream_grad[:, columns(tp, width)]
    with jax.named_scope("turn_forward"):
        loop(0, n, turn_forward)
    with jax.named_scope("conv_grad"):
        @pl.when(me < n - 1)
        def _():
            halo_earlier().wait_recv()

        product_grad = (
            taps[0:1, :] * extended_grad[pl.ds(0, count), :]
            + taps[1:2, :] * extended_grad[pl.ds(1, count), :]
            + taps[2:3, :] * extended_grad[pl.ds(2, count), :]
        )
        small_out[1] = (product_grad * conv_input[...].astype(jnp.float32)).astype(jnp.bfloat16)
        small_out[2] = (product_grad * in_gate[...].astype(jnp.float32)).astype(jnp.bfloat16)

    w_out_sum[...] = jnp.zeros_like(w_out_sum)

    def out_step(s):
        both = turned_all.at[s, pl.ds(0, 2 * quarter)]
        remote(both, both, turn_send.at[2], turn_near.at[s], {"tp": partner}).wait_recv()

        @pl.when((s > 0) & (s < half))
        def _():
            mix_copy(0, s, s).wait_recv()

        @pl.when(s > half)
        def _():
            mix_copy(half, s, s - half).wait_recv()

        w_out_sum[...] += rows_product(turned_all[s], mixed[s])

    with jax.named_scope("w_out_grad"):
        loop(0, n, out_step)

    with jax.named_scope("drain"):
        for one in route_copies():
            one.wait_send()
        for a in (0, 1):
            token_copy(a).wait_send()
            sent = sending.at[a, pl.ds(0, (n - 2) * depth)]
            remote(sent, sent, slot_send.at[a], slot_recv.at[a, 0], {"tp": partner}).wait_send()
            most = slots.at[a, pl.ds(0, (n - 1) * depth), pl.ds(0, width)]
            for sem in (cross_send, near_send, fwd_send):
                remote(most, most, sem.at[a], near_recv.at[a, 0], {"tp": partner}).wait_send()
            remote(far_out, far_in, hand_send.at[a], hand_recv.at[a, 0], {"tp": partner}).wait_send()
        remote(far_out, far_in, far_send, far_recv.at[0], {"tp": cross}).wait_send()
        rest = total.at[pl.ds(0, (n - 1) * depth)]
        remote(rest, rest, out_send, out_recv.at[0], {"tp": partner}).wait_send()
        sent = mixed.at[pl.ds(0, n - 1)]
        remote(sent, sent, mix_send, mix_recv.at[0], {"tp": partner}).wait_send()
        sent = turned_all.at[pl.ds(0, n - 1), pl.ds(0, quarter)]
        remote(sent, sent, turn_send.at[0], turn_recv.at[0], {"tp": partner}).wait_send()
        sent = turned_all.at[:, pl.ds(0, quarter)]
        for kind in range(1, 4):
            remote(sent, sent, turn_send.at[kind], turn_recv.at[0], {"tp": partner}).wait_send()
        for j in range(3):
            exchange(j).wait_send()
            gather(tp, j, j, partner).wait_send()

        @pl.when(me < n - 1)
        def _():
            halo_later().wait_send()

        @pl.when(me > 0)
        def _():
            halo_earlier().wait_send()


def store_kernel(stream, small, w_out, gate, up, down, *rest):
    outs, local = rest[:8], rest[8]
    ins = (stream, small.at[0], small.at[1], small.at[2], w_out, gate, up, down)
    copies = [
        pltpu.make_async_copy(source, target, local.at[i])
        for i, (source, target) in enumerate(zip(ins, outs))
    ]
    for one in copies:
        one.start()
    for one in copies:
        one.wait()


def shards(
    cotangent,
    stream_in,
    norm_gain,
    out_gate,
    in_gate,
    conv_input,
    conv_taps,
    out_weight,
    expert_gate,
    expert_up,
    expert_down,
    expert_choice,
    route_scale,
):
    n = lax.axis_size("sp")
    count, wide = stream_in.shape
    channels = out_gate.shape[1]
    hidden = expert_gate.shape[2]
    width = wide // lax.axis_size("tp")
    depth = 4 * count // n
    rows = n * depth
    block = wide // n
    quarter = count // lax.axis_size("tp")
    kind = stream_in.dtype

    def out(*shape, dtype=kind):
        return jax.ShapeDtypeStruct(shape, dtype)

    def full(*shape):
        return pltpu.VMEM(shape, jnp.float32)

    def held(*shape):
        return pltpu.VMEM(shape, kind)

    vmem, anywhere = (pl.BlockSpec(memory_space=pltpu.VMEM), pl.BlockSpec(memory_space=pl.ANY))
    dma = pltpu.SemaphoreType.DMA
    operands = (
        stream_in,
        cotangent,
        norm_gain[None],
        expert_choice.T,
        route_scale.T,
        out_gate,
        in_gate,
        conv_input,
        conv_taps,
        out_weight,
        expert_gate[0],
        expert_up[0],
        expert_down[0],
    )
    results = pl.pallas_call(
        functools.partial(step_kernel, n),
        out_shape=[
            out(count, width),
            out(3, count, channels),
            out(block, channels, dtype=jnp.float32),
            out(wide, hidden, dtype=jnp.float32),
            out(wide, hidden, dtype=jnp.float32),
            out(hidden, wide, dtype=jnp.float32),
        ],
        in_specs=[anywhere] * 13,
        out_specs=[vmem] * 6,
        scratch_shapes=[pltpu.VMEM(x.shape, x.dtype) for x in operands]
        + [
            held(count, wide),
            full(count, 1),
            full(2, n, count),
            full(2, n, count),
            held(2, count, width),
            pltpu.VMEM((2, count), jnp.int32),
            full(2, count),
            held(2, rows, width),
            held(2, rows, wide),
            held(rows, hidden),
            held(rows, 2 * hidden),
            held(rows, wide),
            held(2, rows, width),
            held(rows, width),
            held(rows, width),
            held(rows, width),
            held(rows, width),
            full(count, width),
            held(quarter, wide),
            held(count, width),
            full(count + 8, channels),
            full(count, channels),
            full(count + 8, channels),
            held(n, count, channels),
            held(count, wide),
            held(n, quarter, block),
            held(n, count, block),
            dma((13,)),
            dma((4,)),
            dma((4,)),
            dma((2,)),
            dma((2, n)),
            dma((2,)),
            dma((2, n)),
            dma((2,)),
            dma((2,)),
            dma((2, n)),
            dma((2,)),
            dma((2, n)),
            dma,
            dma((n,)),
            dma,
            dma((n,)),
            dma((3,)),
            dma((3,)),
            dma((3,)),
            dma((3,)),
            dma((2,)),
            dma((2,)),
            dma,
            dma((n,)),
            dma((4,)),
            dma((n,)),
            dma((n,)),
            dma((n,)),
        ],
        compiler_params=pltpu.CompilerParams(
            collective_id=1, has_side_effects=True, vmem_limit_bytes=VMEM + 3 * n * count * channels
        ),
    )(*(pltpu.with_memory_space_constraint(x, pltpu.HBM) for x in operands))
    stored = pl.pallas_call(
        store_kernel,
        out_shape=[
            out(count, width),
            out(count, channels),
            out(count, channels),
            out(count, channels),
            out(block, channels, dtype=jnp.float32),
            out(wide, hidden, dtype=jnp.float32),
            out(wide, hidden, dtype=jnp.float32),
            out(hidden, wide, dtype=jnp.float32),
        ],
        in_specs=[vmem] * 6,
        out_specs=[anywhere] * 8,
        scratch_shapes=[dma((8,))],
        compiler_params=pltpu.CompilerParams(vmem_limit_bytes=9 * 1024 * 1024),
    )(*results)
    return (*stored[:5], *(grad[None] for grad in stored[5:]))


def solution(mesh):
    placed = (
        P("sp", None),
        P("sp", None),
        P(),
        P("sp", "tp"),
        P("sp", "tp"),
        P("sp", "tp"),
        P(None, "tp"),
        P(None, "tp"),
        P("sp", None, "tp"),
        P("sp", None, "tp"),
        P("sp", "tp", None),
        P("sp", None),
        P("sp", None),
    )
    return jax.shard_map(
        shards,
        mesh=mesh,
        in_specs=placed,
        out_specs=(
            P("sp", "tp"),
            P("sp", "tp"),
            P("sp", "tp"),
            P("sp", "tp"),
            P("sp", "tp"),
            P("sp", None, "tp"),
            P("sp", None, "tp"),
            P("sp", "tp", None),
        ),
        check_vma=False,
    )
```

```python
import functools

import jax
import jax.numpy as jnp
from jax import lax
from jax.experimental import pallas as pl
from jax.experimental.pallas import tpu as pltpu
from jax.sharding import PartitionSpec as P

norm_eps = 1e-06
VMEM = 83 * 512 * 1024


def rows_product(left, right):
    return lax.dot_general(
        left, right, (((0,), (0,)), ((), ())), preferred_element_type=jnp.float32
    )


def cols_product(left, right):
    return lax.dot_general(
        left, right, (((1,), (1,)), ((), ())), preferred_element_type=jnp.float32
    )


MESH = pl.DeviceIdType.MESH


def remote(source, target, send_sem, recv_sem, device):
    return pltpu.make_async_remote_copy(
        src_ref=source,
        dst_ref=target,
        send_sem=send_sem,
        recv_sem=recv_sem,
        device_id=device,
        device_id_type=MESH,
    )


def columns(index, width):
    return pl.ds(pl.multiple_of(index * width, width), width)


def mirrored(me, mask, n):
    found, unit = 0, 1
    while unit < n:
        found = found + lax.rem(lax.div(me, unit) + lax.div(mask, unit), 2) * unit
        unit = 2 * unit
    return found


def tp_places():
    tp, count = lax.axis_index("tp"), lax.axis_size("tp")
    cross = lax.rem(tp + count // 2, count)
    partner = tp + 1 - 2 * lax.rem(tp, 2)
    return (tp, cross, partner, lax.rem(partner + count // 2, count))


def greet(peers):
    barrier = pltpu.get_barrier_semaphore()
    for peer in peers:
        pl.semaphore_signal(barrier, inc=1, device_id={"tp": peer}, device_id_type=MESH)
    me, n = lax.axis_index("sp"), lax.axis_size("sp")

    def greet_one(k, carry):
        peer = lax.rem(me + k, n)
        pl.semaphore_signal(barrier, inc=1, device_id={"sp": peer}, device_id_type=MESH)
        return carry

    lax.fori_loop(1, n, greet_one, 0)
    return lambda: pl.semaphore_wait(barrier, n - 1 + len(peers))


def loop(low, high, body):
    def step(k, carry):
        body(k)
        return carry

    lax.fori_loop(low, high, step, 0)


def step_kernel(
    n,
    *refs,
):
    inputs, refs = refs[:13], refs[13:]
    (
        stream_out,
        small_out,
        w_out_sum,
        gate_sum,
        up_sum,
        down_sum,
        normed,
        inverse,
        keys,
        weights,
        arrived,
        arrived_choice,
        arrived_scales,
        sending,
        slots,
        hidden,
        both_grad,
        partial,
        near,
        far_out,
        far_in,
        total,
        back,
        acc,
        token,
        token_out,
        extended,
        filtered,
        extended_grad,
        mixed,
        stream_grad,
        turned,
        turned_all,
        load,
        tok_send,
        tok_recv,
        slot_send,
        slot_recv,
        cross_send,
        cross_recv,
        near_send,
        fwd_send,
        near_recv,
        hand_send,
        hand_recv,
        far_send,
        far_recv,
        out_send,
        out_recv,
        all_send,
        all_recv,
        row_send,
        row_recv,
        halo_send,
        halo_recv,
        mix_send,
        mix_recv,
        turn_send,
        turn_recv,
        turn_cross,
        turn_near,
    ) = refs[:6] + refs[19:]
    loaded = refs[6:19]
    (
        stream,
        cot,
        gain,
        choice,
        scales,
        out_gate,
        in_gate,
        conv_input,
        taps,
        w_out,
        w_gate,
        w_up,
        w_down,
    ) = loaded
    me = lax.axis_index("sp")
    tp, cross, partner, diagonal = tp_places()
    half = n // 2
    count, wide = normed.shape
    width = acc.shape[1]
    depth = near.shape[1] // n
    group = max(1, n // 4)
    span = group * depth
    chunk = min(256, width)
    channels = filtered.shape[1]
    block = wide // n
    wait_all = greet((cross, partner, diagonal))
    sources = (normed, cot)
    loads = [
        pltpu.make_async_copy(source, target, load.at[i])
        for i, (source, target) in enumerate(zip(inputs, loaded))
    ]
    for i in (3, 4, 1, 0, 2, 6, 7, 5, 8, 10, 11, 12, 9):
        loads[i].start()

    def other(s):
        return mirrored(me, jnp.int32(s), n)

    def at(s):
        return pl.ds(pl.multiple_of(s * depth, depth), depth)

    def normalize(i):
        rows = pl.ds(pl.multiple_of(i * 32, 32), 32)
        values = stream[rows, :].astype(jnp.float32)
        scale = lax.rsqrt(jnp.mean(values * values, axis=-1, keepdims=True) + norm_eps)
        inverse[rows, :] = scale
        normed[rows, :] = (values * scale * gain[...]).astype(jnp.bfloat16)

    def table(which, named, scaled):
        c0, c1 = (named[i : i + 1, :] for i in range(2))
        s0, s1 = (scaled[i : i + 1, :] for i in range(2))
        expert = lax.broadcasted_iota(jnp.int32, (n, count), 0)
        first, second = (c0 == expert, c1 == expert)
        member = jnp.where(first | second, 1.0, 0.0)
        row = lax.broadcasted_iota(jnp.int32, (count, count), 0)
        column = lax.broadcasted_iota(jnp.int32, (count, count), 1)
        before = jnp.where(row < column, 1.0, 0.0).astype(jnp.bfloat16)
        earlier = jnp.dot(
            member.astype(jnp.bfloat16), before, preferred_element_type=jnp.float32
        )
        keys[which] = jnp.where(member > 0.0, earlier, -1.0)
        weights[which] = jnp.where(first, s0, 0.0) + jnp.where(second, s1, 0.0)

    def placing(which, expert):
        slot = lax.broadcasted_iota(jnp.int32, (depth, count), 0).astype(jnp.float32)
        return slot == keys[which, pl.ds(expert, 1), :]

    def chosen(a, which, expert, values):
        mask = placing(which, expert)
        found = jnp.dot(
            jnp.where(mask, 1.0, 0.0).astype(jnp.bfloat16),
            values,
            preferred_element_type=jnp.float32,
        )
        if a == 1:
            weight = jnp.where(mask, weights[which, pl.ds(expert, 1), :], 0.0)
            found = found * jnp.sum(weight, axis=1, keepdims=True)
        return found.astype(jnp.bfloat16)

    def token_copy(a):
        return remote(
            sources[a].at[:, columns(tp, width)],
            arrived.at[a],
            tok_send.at[a],
            tok_recv.at[a],
            {"sp": other(half)},
        )

    def route_copies():
        pairs = ((choice, arrived_choice), (scales, arrived_scales))
        return [
            remote(source, target, tok_send.at[2 + i], tok_recv.at[2 + i], {"sp": other(half)})
            for i, (source, target) in enumerate(pairs)
        ]

    def slot_copy(a, s, k):
        return remote(
            sending.at[a, at(s)],
            slots.at[a, at(s), columns(tp, width)],
            slot_send.at[a],
            slot_recv.at[a, s],
            {"sp": other(k)},
        )

    def spread(a, s):
        part = slots.at[a, at(s), columns(tp, width)]
        remote(part, part, cross_send.at[a], cross_recv.at[a, s], {"tp": cross}).start()
        remote(part, part, near_send.at[a], near_recv.at[a, s], {"tp": partner}).start()

    def forward(a, s):
        part = slots.at[a, at(s), columns(cross, width)]
        remote(part, part, cross_send.at[a], cross_recv.at[a, s], {"tp": cross}).wait_recv()
        remote(part, part, fwd_send.at[a], near_recv.at[a, s], {"tp": partner}).start()

    def ready(s):
        for a in (0, 1):
            both = slots.at[a, at(s), pl.ds(0, 2 * width)]
            remote(both, both, near_send.at[a], near_recv.at[a, s], {"tp": partner}).wait_recv()

    def hand(j, s):
        return remote(
            partial.at[at(s), columns((partner, diagonal)[j], width)],
            near.at[j, at(s)],
            hand_send.at[j],
            hand_recv.at[j, s],
            {"tp": partner},
        )

    def across(s):
        return remote(
            far_out.at[at(s)], far_in.at[at(s)], far_send, far_recv.at[s], {"tp": cross}
        )

    def give(s):
        return remote(
            total.at[at(s)], back.at[at(s)], out_send, out_recv.at[s], {"sp": other(s)}
        )

    def halo_later():
        peer = lax.rem(me + 1, n)
        return remote(
            extended.at[pl.ds(count, 8)],
            extended.at[pl.ds(0, 8)],
            halo_send.at[0],
            halo_recv.at[0],
            {"sp": peer},
        )

    def halo_earlier():
        peer = lax.rem(me + n - 1, n)
        return remote(
            extended_grad.at[pl.ds(0, 8)],
            extended_grad.at[pl.ds(count, 8)],
            halo_send.at[1],
            halo_recv.at[1],
            {"sp": peer},
        )

    def mix_copy(source, target, k):
        return remote(
            mixed.at[source], mixed.at[target], mix_send, mix_recv.at[target], {"sp": other(k)}
        )

    def send_own(a, k):
        values = sources[a][:, columns(tp, width)]
        sending[a, at(k), :] = chosen(a, 0, other(k), values)
        slot_copy(a, k, k).start()

    with jax.named_scope("prep"):
        loads[3].wait()
        loads[4].wait()
        table(0, choice, scales)
        loads[1].wait()
    with jax.named_scope("barrier"):
        wait_all()
    with jax.named_scope("send_own"):
        for one in route_copies():
            one.start()
        loop(1, half, lambda k: send_own(1, k))
        token_copy(1).start()
        with jax.named_scope("conv"):
            loads[6].wait()
            loads[7].wait()
            product = in_gate[...].astype(jnp.float32) * conv_input[...].astype(jnp.float32)
            extended[pl.ds(8, count), :] = product

            @pl.when(me == 0)
            def _():
                extended[pl.ds(0, 8), :] = jnp.zeros((8, channels), jnp.float32)

            @pl.when(me == n - 1)
            def _():
                extended_grad[pl.ds(count, 8), :] = jnp.zeros((8, channels), jnp.float32)

            @pl.when(me < n - 1)
            def _():
                halo_later().start()
        loads[0].wait()
        loads[2].wait()
        loop(0, count // 32, normalize)
        loop(1, half, lambda k: send_own(0, k))
        token_copy(0).start()
    with jax.named_scope("own_block"):
        for a in (0, 1):
            for piece in range(wide // width):
                where = pl.ds(piece * width, width)
                slots[a, pl.ds(0, depth), where] = chosen(a, 0, me, sources[a][:, where])

    def land(a, s, k):
        slot_copy(a, s, k).wait_recv()
        spread(a, s)

    def take_tokens():
        for a in (1, 0):
            if a == 1:
                for one in route_copies():
                    one.wait_recv()
                table(1, arrived_choice, arrived_scales)
            token_copy(a).wait_recv()

            def send_other(k):
                sending[a, at(half + k), :] = chosen(a, 1, other(k), arrived[a])
                slot_copy(a, half + k, k).start()

            loop(1, half, send_other)
            slots[a, at(half), columns(tp, width)] = chosen(a, 1, me, arrived[a])
            spread(a, half)

    def forward_both(s):
        for a in (0, 1):
            forward(a, s)

    def mix_early():
        mix_copy(0, half, half).start()
        loop(1, half, lambda k: mix_copy(0, k, k).start())

    def mix_late():
        mix_copy(half, half, half).wait_recv()
        loop(1, half, lambda k: mix_copy(half, half + k, k).start())

    def compute(g):
        rows = pl.ds(pl.multiple_of(g * span, span), span)
        picked, scaled = (slots[0, rows, :], slots[1, rows, :])
        gate_pre = jnp.dot(picked, w_gate[...], preferred_element_type=jnp.float32)
        up_pre = jnp.dot(picked, w_up[...], preferred_element_type=jnp.float32)
        hidden_grad = cols_product(scaled, w_down[...])
        sigmoid_gate = jax.nn.sigmoid(gate_pre)
        silu_gate = gate_pre * sigmoid_gate
        hidden[rows, :] = (silu_gate * up_pre).astype(jnp.bfloat16)
        gate = (
            hidden_grad * up_pre * sigmoid_gate * (1.0 + gate_pre * (1.0 - sigmoid_gate))
        ).astype(jnp.bfloat16)
        up = (hidden_grad * silu_gate).astype(jnp.bfloat16)
        across_hidden = gate.shape[1]
        both_grad[rows, pl.ds(0, across_hidden)] = gate
        both_grad[rows, pl.ds(across_hidden, across_hidden)] = up
        for piece in range(wide // width):
            where = pl.ds(piece * width, width)
            partial[rows, where] = (
                cols_product(gate, w_gate[where, :]) + cols_product(up, w_up[where, :])
            ).astype(jnp.bfloat16)

    def work(g):
        def await_one(i):
            s = g * group + i

            @pl.when(s > 0)
            def _():
                ready(s)

        loop(0, group, await_one)
        compute(g)

        def hand_one(i):
            s = g * group + i
            hand(1, s).start()
            hand(0, s).start()

        loop(0, group, hand_one)

    def pair(s):
        hand(1, s).wait_recv()
        mine = partial[at(s), columns(cross, width)].astype(jnp.float32)
        far_out[at(s), :] = (mine + near[1, at(s), :].astype(jnp.float32)).astype(jnp.bfloat16)
        across(s).start()

    def pair_group(g):
        loop(0, group, lambda i: pair(g * group + i))

    def step(g):
        def forward_one(i):
            s = g * group + i

            @pl.when(s > 0)
            def _():
                forward_both(s)

        with jax.named_scope("forward_group"):
            loop(0, group, forward_one)
        with jax.named_scope("work_group"):
            work(g)

    def finish(s):
        hand(0, s).wait_recv()
        across(s).wait_recv()
        mine = partial[at(s), columns(tp, width)].astype(jnp.float32)
        return (
            mine + near[0, at(s), :].astype(jnp.float32) + far_in[at(s), :].astype(jnp.float32)
        ).astype(jnp.bfloat16)

    def finish_one(s):
        total[at(s), :] = finish(s)
        give(s).start()

    def grads(c):
        rows = pl.ds(pl.multiple_of(c * chunk, chunk), chunk)
        sums = rows_product(slots[0, :, rows], both_grad[...])
        gate_sum[rows, :] = sums[:, : sums.shape[1] // 2]
        up_sum[rows, :] = sums[:, sums.shape[1] // 2 :]
        down_sum[:, rows] = rows_product(hidden[...], slots[1, :, rows])

    def finish_group(g):
        def one(i):
            s = g * group + i

            @pl.when(s > 0)
            def _():
                finish_one(s)

            @pl.when(s == 0)
            def _():
                back[pl.ds(0, depth), :] = finish(0)

        loop(0, group, one)

    with jax.named_scope("land_first"):
        for a in (1, 0):
            loop(1, half, lambda k: land(a, k, k))
    for i in range(10, 13):
        loads[i].wait()
    with jax.named_scope("tokens"):
        take_tokens()
    with jax.named_scope("land_second"):
        for a in (1,):
            loop(1, half, lambda k: land(a, half + k, k))
    step(0)
    with jax.named_scope("land_second"):
        for a in (0,):
            loop(1, half, lambda k: land(a, half + k, k))
    with jax.named_scope("pair0"):
        pair_group(0)
    with jax.named_scope("filter"):
        @pl.when(me > 0)
        def _():
            halo_later().wait_recv()

        loads[5].wait()
        loads[8].wait()
        filtered[...] = (
            taps[0:1, :] * extended[pl.ds(8, count), :]
            + taps[1:2, :] * extended[pl.ds(7, count), :]
            + taps[2:3, :] * extended[pl.ds(6, count), :]
        )
        mixed[0] = (out_gate[...].astype(jnp.float32) * filtered[...]).astype(jnp.bfloat16)

    mix_early()
    pieces_of = wide // chunk
    step(1)
    step(2)
    with jax.named_scope("pair2"):
        pair_group(2)
    mix_late()
    step(3)
    with jax.named_scope("pair3"):
        pair_group(3)
    with jax.named_scope("pair1"):
        pair_group(1)
    with jax.named_scope("fin0"):
        finish_group(0)
    with jax.named_scope("fin2"):
        finish_group(2)
    with jax.named_scope("grads"):
        loop(0, pieces_of // 4, grads)
    with jax.named_scope("grads"):
        loop(pieces_of // 4, pieces_of // 2, grads)
    with jax.named_scope("fin3"):
        finish_group(3)
    with jax.named_scope("fin1"):
        finish_group(1)
    with jax.named_scope("grads"):
        loop(pieces_of // 2, 3 * pieces_of // 4, grads)
    with jax.named_scope("grads"):
        loop(3 * pieces_of // 4, pieces_of, grads)
    acc[...] = jnp.zeros_like(acc)

    def combine(s):
        @pl.when(s > 0)
        def _():
            give(s).wait_recv()

        mask = jnp.where(placing(0, other(s)), 1.0, 0.0).astype(jnp.bfloat16)
        acc[...] += rows_product(mask, back[at(s), :])

    with jax.named_scope("combine"):
        loop(0, n, combine)
    quarter = token.shape[0]

    def quarter_rows(column):
        return pl.ds(pl.multiple_of(column * quarter, quarter), quarter)

    def exchange(j):
        peer = (cross, diagonal, partner)[j]
        return remote(
            token_out.at[quarter_rows(peer)],
            token.at[:, columns(tp, width)],
            all_send.at[j],
            all_recv.at[j],
            {"tp": peer},
        )

    with jax.named_scope("share"):
        token_out[...] = acc[...].astype(jnp.bfloat16)
        for j in range(3):
            exchange(j).start()
        token[:, columns(tp, width)] = token_out[quarter_rows(tp), :]
        for j in (2, 0, 1):
            exchange(j).wait_recv()

    def total_grad(i):
        here = pl.ds(pl.multiple_of(i * 16, 16), 16)
        rows = pl.ds(pl.multiple_of(tp * quarter + i * 16, 16), 16)
        scale = inverse[rows, :]
        unit = stream[rows, :].astype(jnp.float32) * scale
        unit_grad = token[here, :].astype(jnp.float32) * gain[...]
        along = jnp.mean(unit * unit_grad, axis=-1, keepdims=True)
        value = cot[rows, :].astype(jnp.float32) + scale * (unit_grad - unit * along)
        value = value.astype(jnp.bfloat16)
        stream_grad[rows, :] = value
        for owner in range(n):
            turned[owner, here, :] = value[:, owner * block : (owner + 1) * block]

    with jax.named_scope("stream_grad"):
        loop(0, quarter // 16, total_grad)

    def turn_copy(s):
        return remote(
            turned.at[other(s)],
            turned_all.at[s, quarter_rows(tp)],
            turn_send.at[0],
            turn_recv.at[s],
            {"sp": other(s)},
        )

    def turn_part(s, column, send, recv, peer):
        rows = turned_all.at[s, quarter_rows(column)]
        return remote(rows, rows, send, recv, {"tp": peer})

    def gather(column, j, recv, peer):
        rows = stream_grad.at[quarter_rows(column)]
        return remote(rows, rows, row_send.at[j], row_recv.at[recv], {"tp": peer})

    def turn_spread(s):
        turn_part(s, tp, turn_send.at[1], turn_cross.at[s], cross).start()
        turn_part(s, tp, turn_send.at[2], turn_near.at[s], partner).start()

    def turn_land(s):
        turn_copy(s).wait_recv()
        turn_spread(s)

    def turn_forward(s):
        turn_part(s, cross, turn_send.at[1], turn_cross.at[s], cross).wait_recv()
        turn_part(s, cross, turn_send.at[3], turn_near.at[s], partner).start()

    with jax.named_scope("turn_start"):
        loop(1, n, lambda k: turn_copy(n - k).start())
        gather(tp, 0, 0, cross).start()
        gather(tp, 1, 1, partner).start()
        turned_all[0, quarter_rows(tp), :] = turned[me]
        turn_spread(0)
    with jax.named_scope("gather"):
        gather(cross, 0, 0, cross).wait_recv()
        gather(cross, 2, 2, partner).start()
    with jax.named_scope("turn_land"):
        loop(1, n, turn_land)
    with jax.named_scope("mixed_grad"):
        gather(tp, 1, 1, partner).wait_recv()
        gather(tp, 2, 2, partner).wait_recv()
        loads[9].wait()
        mixed_grad = jnp.dot(stream_grad[...], w_out[...], preferred_element_type=jnp.float32)
        small_out[0] = (mixed_grad * filtered[...]).astype(jnp.bfloat16)
        extended_grad[pl.ds(0, count), :] = mixed_grad * out_gate[...].astype(jnp.float32)

        @pl.when(me > 0)
        def _():
            halo_earlier().start()

        stream_out[...] = stream_grad[:, columns(tp, width)]
    with jax.named_scope("turn_forward"):
        loop(0, n, turn_forward)
    with jax.named_scope("conv_grad"):
        @pl.when(me < n - 1)
        def _():
            halo_earlier().wait_recv()

        product_grad = (
            taps[0:1, :] * extended_grad[pl.ds(0, count), :]
            + taps[1:2, :] * extended_grad[pl.ds(1, count), :]
            + taps[2:3, :] * extended_grad[pl.ds(2, count), :]
        )
        small_out[1] = (product_grad * conv_input[...].astype(jnp.float32)).astype(jnp.bfloat16)
        small_out[2] = (product_grad * in_gate[...].astype(jnp.float32)).astype(jnp.bfloat16)

    w_out_sum[...] = jnp.zeros_like(w_out_sum)

    def out_step(s):
        both = turned_all.at[s, pl.ds(0, 2 * quarter)]
        remote(both, both, turn_send.at[2], turn_near.at[s], {"tp": partner}).wait_recv()

        @pl.when((s > 0) & (s < half))
        def _():
            mix_copy(0, s, s).wait_recv()

        @pl.when(s > half)
        def _():
            mix_copy(half, s, s - half).wait_recv()

        w_out_sum[...] += rows_product(turned_all[s], mixed[s])

    with jax.named_scope("w_out_grad"):
        loop(0, n, out_step)

    with jax.named_scope("drain"):
        for one in route_copies():
            one.wait_send()
        for a in (0, 1):
            token_copy(a).wait_send()
            sent = sending.at[a, pl.ds(0, (n - 2) * depth)]
            remote(sent, sent, slot_send.at[a], slot_recv.at[a, 0], {"tp": partner}).wait_send()
            most = slots.at[a, pl.ds(0, (n - 1) * depth), pl.ds(0, width)]
            for sem in (cross_send, near_send, fwd_send):
                remote(most, most, sem.at[a], near_recv.at[a, 0], {"tp": partner}).wait_send()
            remote(far_out, far_in, hand_send.at[a], hand_recv.at[a, 0], {"tp": partner}).wait_send()
        remote(far_out, far_in, far_send, far_recv.at[0], {"tp": cross}).wait_send()
        rest = total.at[pl.ds(0, (n - 1) * depth)]
        remote(rest, rest, out_send, out_recv.at[0], {"tp": partner}).wait_send()
        sent = mixed.at[pl.ds(0, n - 1)]
        remote(sent, sent, mix_send, mix_recv.at[0], {"tp": partner}).wait_send()
        sent = turned_all.at[pl.ds(0, n - 1), pl.ds(0, quarter)]
        remote(sent, sent, turn_send.at[0], turn_recv.at[0], {"tp": partner}).wait_send()
        sent = turned_all.at[:, pl.ds(0, quarter)]
        for kind in range(1, 4):
            remote(sent, sent, turn_send.at[kind], turn_recv.at[0], {"tp": partner}).wait_send()
        for j in range(3):
            exchange(j).wait_send()
            gather(tp, j, j, partner).wait_send()

        @pl.when(me < n - 1)
        def _():
            halo_later().wait_send()

        @pl.when(me > 0)
        def _():
            halo_earlier().wait_send()


def store_kernel(stream, small, w_out, gate, up, down, *rest):
    outs, local = rest[:8], rest[8]
    ins = (stream, small.at[0], small.at[1], small.at[2], w_out, gate, up, down)
    copies = [
        pltpu.make_async_copy(source, target, local.at[i])
        for i, (source, target) in enumerate(zip(ins, outs))
    ]
    for one in copies:
        one.start()
    for one in copies:
        one.wait()


def shards(
    cotangent,
    stream_in,
    norm_gain,
    out_gate,
    in_gate,
    conv_input,
    conv_taps,
    out_weight,
    expert_gate,
    expert_up,
    expert_down,
    expert_choice,
    route_scale,
):
    n = lax.axis_size("sp")
    count, wide = stream_in.shape
    channels = out_gate.shape[1]
    hidden = expert_gate.shape[2]
    width = wide // lax.axis_size("tp")
    depth = 4 * count // n
    rows = n * depth
    block = wide // n
    quarter = count // lax.axis_size("tp")
    kind = stream_in.dtype

    def out(*shape, dtype=kind):
        return jax.ShapeDtypeStruct(shape, dtype)

    def full(*shape):
        return pltpu.VMEM(shape, jnp.float32)

    def held(*shape):
        return pltpu.VMEM(shape, kind)

    vmem, anywhere = (pl.BlockSpec(memory_space=pltpu.VMEM), pl.BlockSpec(memory_space=pl.ANY))
    dma = pltpu.SemaphoreType.DMA
    operands = (
        stream_in,
        cotangent,
        norm_gain[None],
        expert_choice.T,
        route_scale.T,
        out_gate,
        in_gate,
        conv_input,
        conv_taps,
        out_weight,
        expert_gate[0],
        expert_up[0],
        expert_down[0],
    )
    results = pl.pallas_call(
        functools.partial(step_kernel, n),
        out_shape=[
            out(count, width),
            out(3, count, channels),
            out(block, channels, dtype=jnp.float32),
            out(wide, hidden, dtype=jnp.float32),
            out(wide, hidden, dtype=jnp.float32),
            out(hidden, wide, dtype=jnp.float32),
        ],
        in_specs=[anywhere] * 13,
        out_specs=[vmem] * 6,
        scratch_shapes=[pltpu.VMEM(x.shape, x.dtype) for x in operands]
        + [
            held(count, wide),
            full(count, 1),
            full(2, n, count),
            full(2, n, count),
            held(2, count, width),
            pltpu.VMEM((2, count), jnp.int32),
            full(2, count),
            held(2, rows, width),
            held(2, rows, wide),
            held(rows, hidden),
            held(rows, 2 * hidden),
            held(rows, wide),
            held(2, rows, width),
            held(rows, width),
            held(rows, width),
            held(rows, width),
            held(rows, width),
            full(count, width),
            held(quarter, wide),
            held(count, width),
            full(count + 8, channels),
            full(count, channels),
            full(count + 8, channels),
            held(n, count, channels),
            held(count, wide),
            held(n, quarter, block),
            held(n, count, block),
            dma((13,)),
            dma((4,)),
            dma((4,)),
            dma((2,)),
            dma((2, n)),
            dma((2,)),
            dma((2, n)),
            dma((2,)),
            dma((2,)),
            dma((2, n)),
            dma((2,)),
            dma((2, n)),
            dma,
            dma((n,)),
            dma,
            dma((n,)),
            dma((3,)),
            dma((3,)),
            dma((3,)),
            dma((3,)),
            dma((2,)),
            dma((2,)),
            dma,
            dma((n,)),
            dma((4,)),
            dma((n,)),
            dma((n,)),
            dma((n,)),
        ],
        compiler_params=pltpu.CompilerParams(
            collective_id=1, has_side_effects=True, vmem_limit_bytes=VMEM + 3 * n * count * channels
        ),
    )(*(pltpu.with_memory_space_constraint(x, pltpu.HBM) for x in operands))
    stored = pl.pallas_call(
        store_kernel,
        out_shape=[
            out(count, width),
            out(count, channels),
            out(count, channels),
            out(count, channels),
            out(block, channels, dtype=jnp.float32),
            out(wide, hidden, dtype=jnp.float32),
            out(wide, hidden, dtype=jnp.float32),
            out(hidden, wide, dtype=jnp.float32),
        ],
        in_specs=[vmem] * 6,
        out_specs=[anywhere] * 8,
        scratch_shapes=[dma((8,))],
        compiler_params=pltpu.CompilerParams(vmem_limit_bytes=9 * 1024 * 1024),
    )(*results)
    return (*stored[:5], *(grad[None] for grad in stored[5:]))


def solution(mesh):
    placed = (
        P("sp", None),
        P("sp", None),
        P(),
        P("sp", "tp"),
        P("sp", "tp"),
        P("sp", "tp"),
        P(None, "tp"),
        P(None, "tp"),
        P("sp", None, "tp"),
        P("sp", None, "tp"),
        P("sp", "tp", None),
        P("sp", None),
        P("sp", None),
    )
    return jax.shard_map(
        shards,
        mesh=mesh,
        in_specs=placed,
        out_specs=(
            P("sp", "tp"),
            P("sp", "tp"),
            P("sp", "tp"),
            P("sp", "tp"),
            P("sp", "tp"),
            P("sp", None, "tp"),
            P("sp", None, "tp"),
            P("sp", "tp", None),
        ),
        check_vma=False,
    )
```

```python
import functools

import jax
import jax.numpy as jnp
from jax import lax
from jax.experimental import pallas as pl
from jax.experimental.pallas import tpu as pltpu
from jax.sharding import PartitionSpec as P

norm_eps = 1e-06
VMEM = 83 * 512 * 1024


def rows_product(left, right):
    return lax.dot_general(
        left, right, (((0,), (0,)), ((), ())), preferred_element_type=jnp.float32
    )


def cols_product(left, right):
    return lax.dot_general(
        left, right, (((1,), (1,)), ((), ())), preferred_element_type=jnp.float32
    )


MESH = pl.DeviceIdType.MESH


def remote(source, target, send_sem, recv_sem, device):
    return pltpu.make_async_remote_copy(
        src_ref=source,
        dst_ref=target,
        send_sem=send_sem,
        recv_sem=recv_sem,
        device_id=device,
        device_id_type=MESH,
    )


def columns(index, width):
    return pl.ds(pl.multiple_of(index * width, width), width)


def mirrored(me, mask, n):
    found, unit = 0, 1
    while unit < n:
        found = found + lax.rem(lax.div(me, unit) + lax.div(mask, unit), 2) * unit
        unit = 2 * unit
    return found


def tp_places():
    tp, count = lax.axis_index("tp"), lax.axis_size("tp")
    cross = lax.rem(tp + count // 2, count)
    partner = tp + 1 - 2 * lax.rem(tp, 2)
    return (tp, cross, partner, lax.rem(partner + count // 2, count))


def greet(peers):
    barrier = pltpu.get_barrier_semaphore()
    for peer in peers:
        pl.semaphore_signal(barrier, inc=1, device_id={"tp": peer}, device_id_type=MESH)
    me, n = lax.axis_index("sp"), lax.axis_size("sp")

    def greet_one(k, carry):
        peer = lax.rem(me + k, n)
        pl.semaphore_signal(barrier, inc=1, device_id={"sp": peer}, device_id_type=MESH)
        return carry

    lax.fori_loop(1, n, greet_one, 0)
    return lambda: pl.semaphore_wait(barrier, n - 1 + len(peers))


def loop(low, high, body):
    def step(k, carry):
        body(k)
        return carry

    lax.fori_loop(low, high, step, 0)


def step_kernel(
    n,
    *refs,
):
    inputs, refs = refs[:13], refs[13:]
    (
        stream_out,
        small_out,
        w_out_sum,
        gate_sum,
        up_sum,
        down_sum,
        normed,
        inverse,
        keys,
        weights,
        arrived,
        arrived_choice,
        arrived_scales,
        sending,
        slots,
        hidden,
        both_grad,
        partial,
        near,
        far_out,
        far_in,
        total,
        back,
        acc,
        token,
        token_out,
        extended,
        filtered,
        extended_grad,
        mixed,
        stream_grad,
        turned,
        turned_all,
        load,
        tok_send,
        tok_recv,
        slot_send,
        slot_recv,
        cross_send,
        cross_recv,
        near_send,
        fwd_send,
        near_recv,
        hand_send,
        hand_recv,
        far_send,
        far_recv,
        out_send,
        out_recv,
        all_send,
        all_recv,
        row_send,
        row_recv,
        halo_send,
        halo_recv,
        mix_send,
        mix_recv,
        turn_send,
        turn_recv,
        turn_cross,
        turn_near,
    ) = refs[:6] + refs[19:]
    loaded = refs[6:19]
    (
        stream,
        cot,
        gain,
        choice,
        scales,
        out_gate,
        in_gate,
        conv_input,
        taps,
        w_out,
        w_gate,
        w_up,
        w_down,
    ) = loaded
    me = lax.axis_index("sp")
    tp, cross, partner, diagonal = tp_places()
    half = n // 2
    count, wide = normed.shape
    width = acc.shape[1]
    depth = near.shape[1] // n
    group = max(1, n // 4)
    span = group * depth
    chunk = min(256, width)
    channels = filtered.shape[1]
    block = wide // n
    wait_all = greet((cross, partner, diagonal))
    sources = (normed, cot)
    loads = [
        pltpu.make_async_copy(source, target, load.at[i])
        for i, (source, target) in enumerate(zip(inputs, loaded))
    ]
    for i in (3, 4, 1, 0, 2, 6, 7, 5, 8, 10, 11, 12, 9):
        loads[i].start()

    def other(s):
        return mirrored(me, jnp.int32(s), n)

    def at(s):
        return pl.ds(pl.multiple_of(s * depth, depth), depth)

    def normalize(i):
        rows = pl.ds(pl.multiple_of(i * 32, 32), 32)
        values = stream[rows, :].astype(jnp.float32)
        scale = lax.rsqrt(jnp.mean(values * values, axis=-1, keepdims=True) + norm_eps)
        inverse[rows, :] = scale
        normed[rows, :] = (values * scale * gain[...]).astype(jnp.bfloat16)

    def table(which, named, scaled):
        c0, c1 = (named[i : i + 1, :] for i in range(2))
        s0, s1 = (scaled[i : i + 1, :] for i in range(2))
        expert = lax.broadcasted_iota(jnp.int32, (n, count), 0)
        first, second = (c0 == expert, c1 == expert)
        member = jnp.where(first | second, 1.0, 0.0)
        row = lax.broadcasted_iota(jnp.int32, (count, count), 0)
        column = lax.broadcasted_iota(jnp.int32, (count, count), 1)
        before = jnp.where(row < column, 1.0, 0.0).astype(jnp.bfloat16)
        earlier = jnp.dot(
            member.astype(jnp.bfloat16), before, preferred_element_type=jnp.float32
        )
        keys[which] = jnp.where(member > 0.0, earlier, -1.0)
        weights[which] = jnp.where(first, s0, 0.0) + jnp.where(second, s1, 0.0)

    def placing(which, expert):
        slot = lax.broadcasted_iota(jnp.int32, (depth, count), 0).astype(jnp.float32)
        return slot == keys[which, pl.ds(expert, 1), :]

    def chosen(a, which, expert, values):
        mask = placing(which, expert)
        found = jnp.dot(
            jnp.where(mask, 1.0, 0.0).astype(jnp.bfloat16),
            values,
            preferred_element_type=jnp.float32,
        )
        if a == 1:
            weight = jnp.where(mask, weights[which, pl.ds(expert, 1), :], 0.0)
            found = found * jnp.sum(weight, axis=1, keepdims=True)
        return found.astype(jnp.bfloat16)

    def token_copy(a):
        return remote(
            sources[a].at[:, columns(tp, width)],
            arrived.at[a],
            tok_send.at[a],
            tok_recv.at[a],
            {"sp": other(half)},
        )

    def route_copies():
        pairs = ((choice, arrived_choice), (scales, arrived_scales))
        return [
            remote(source, target, tok_send.at[2 + i], tok_recv.at[2 + i], {"sp": other(half)})
            for i, (source, target) in enumerate(pairs)
        ]

    def slot_copy(a, s, k):
        return remote(
            sending.at[a, at(s)],
            slots.at[a, at(s), columns(tp, width)],
            slot_send.at[a],
            slot_recv.at[a, s],
            {"sp": other(k)},
        )

    def spread(a, s):
        part = slots.at[a, at(s), columns(tp, width)]
        remote(part, part, cross_send.at[a], cross_recv.at[a, s], {"tp": cross}).start()
        remote(part, part, near_send.at[a], near_recv.at[a, s], {"tp": partner}).start()

    def forward(a, s):
        part = slots.at[a, at(s), columns(cross, width)]
        remote(part, part, cross_send.at[a], cross_recv.at[a, s], {"tp": cross}).wait_recv()
        remote(part, part, fwd_send.at[a], near_recv.at[a, s], {"tp": partner}).start()

    def ready(s):
        for a in (0, 1):
            both = slots.at[a, at(s), pl.ds(0, 2 * width)]
            remote(both, both, near_send.at[a], near_recv.at[a, s], {"tp": partner}).wait_recv()

    def hand(j, s):
        return remote(
            partial.at[at(s), columns((partner, diagonal)[j], width)],
            near.at[j, at(s)],
            hand_send.at[j],
            hand_recv.at[j, s],
            {"tp": partner},
        )

    def across(s):
        return remote(
            far_out.at[at(s)], far_in.at[at(s)], far_send, far_recv.at[s], {"tp": cross}
        )

    def give(s):
        return remote(
            total.at[at(s)], back.at[at(s)], out_send, out_recv.at[s], {"sp": other(s)}
        )

    def halo_later():
        peer = lax.rem(me + 1, n)
        return remote(
            extended.at[pl.ds(count, 8)],
            extended.at[pl.ds(0, 8)],
            halo_send.at[0],
            halo_recv.at[0],
            {"sp": peer},
        )

    def halo_earlier():
        peer = lax.rem(me + n - 1, n)
        return remote(
            extended_grad.at[pl.ds(0, 8)],
            extended_grad.at[pl.ds(count, 8)],
            halo_send.at[1],
            halo_recv.at[1],
            {"sp": peer},
        )

    def mix_copy(source, target, k):
        return remote(
            mixed.at[source], mixed.at[target], mix_send, mix_recv.at[target], {"sp": other(k)}
        )

    def send_own(a, k):
        values = sources[a][:, columns(tp, width)]
        sending[a, at(k), :] = chosen(a, 0, other(k), values)
        slot_copy(a, k, k).start()

    def next_copy(a):
        return remote(
            sending.at[a, at(0)],
            slots.at[a, at(1), columns(cross, width)],
            slot_send.at[a],
            slot_recv.at[a, 1],
            {"sp": other(1)},
        )

    def send_next(a):
        send_own(a, 1)
        values = sources[a][:, columns(cross, width)]
        sending[a, at(0), :] = chosen(a, 0, other(1), values)
        next_copy(a).start()

    def land_next(a):
        both = slots.at[a, at(1), pl.ds(0, 2 * width)]
        remote(both, both, slot_send.at[a], slot_recv.at[a, 1], {"sp": other(1)}).wait_recv()
        for column, sem in ((tp, near_send), (cross, fwd_send)):
            part = slots.at[a, at(1), columns(column, width)]
            remote(part, part, sem.at[a], near_recv.at[a, 1], {"tp": partner}).start()

    with jax.named_scope("prep"):
        loads[3].wait()
        loads[4].wait()
        table(0, choice, scales)
        loads[1].wait()
    with jax.named_scope("barrier"):
        wait_all()
    with jax.named_scope("send_own"):
        for one in route_copies():
            one.start()
        loop(2, half, lambda k: send_own(1, k))
        send_next(1)
        token_copy(1).start()
        with jax.named_scope("conv"):
            loads[6].wait()
            loads[7].wait()
            product = in_gate[...].astype(jnp.float32) * conv_input[...].astype(jnp.float32)
            extended[pl.ds(8, count), :] = product

            @pl.when(me == 0)
            def _():
                extended[pl.ds(0, 8), :] = jnp.zeros((8, channels), jnp.float32)

            @pl.when(me == n - 1)
            def _():
                extended_grad[pl.ds(count, 8), :] = jnp.zeros((8, channels), jnp.float32)

            @pl.when(me < n - 1)
            def _():
                halo_later().start()
        loads[0].wait()
        loads[2].wait()
        loop(0, count // 32, normalize)
        loop(2, half, lambda k: send_own(0, k))
        send_next(0)
        token_copy(0).start()
    with jax.named_scope("own_block"):
        for a in (0, 1):
            for piece in range(wide // width):
                where = pl.ds(piece * width, width)
                slots[a, pl.ds(0, depth), where] = chosen(a, 0, me, sources[a][:, where])

    def land(a, s, k):
        slot_copy(a, s, k).wait_recv()
        spread(a, s)

    def take_tokens():
        for a in (1, 0):
            if a == 1:
                for one in route_copies():
                    one.wait_recv()
                table(1, arrived_choice, arrived_scales)
            token_copy(a).wait_recv()

            def send_other(k):
                sending[a, at(half + k), :] = chosen(a, 1, other(k), arrived[a])
                slot_copy(a, half + k, k).start()

            loop(1, half, send_other)
            slots[a, at(half), columns(tp, width)] = chosen(a, 1, me, arrived[a])
            spread(a, half)

    def forward_both(s):
        for a in (0, 1):
            forward(a, s)

    def mix_early():
        mix_copy(0, half, half).start()
        loop(1, half, lambda k: mix_copy(0, k, k).start())

    def mix_late():
        mix_copy(half, half, half).wait_recv()
        loop(1, half, lambda k: mix_copy(half, half + k, k).start())

    def compute(g):
        rows = pl.ds(pl.multiple_of(g * span, span), span)
        picked, scaled = (slots[0, rows, :], slots[1, rows, :])
        gate_pre = jnp.dot(picked, w_gate[...], preferred_element_type=jnp.float32)
        up_pre = jnp.dot(picked, w_up[...], preferred_element_type=jnp.float32)
        hidden_grad = cols_product(scaled, w_down[...])
        sigmoid_gate = jax.nn.sigmoid(gate_pre)
        silu_gate = gate_pre * sigmoid_gate
        hidden[rows, :] = (silu_gate * up_pre).astype(jnp.bfloat16)
        gate = (
            hidden_grad * up_pre * sigmoid_gate * (1.0 + gate_pre * (1.0 - sigmoid_gate))
        ).astype(jnp.bfloat16)
        up = (hidden_grad * silu_gate).astype(jnp.bfloat16)
        across_hidden = gate.shape[1]
        both_grad[rows, pl.ds(0, across_hidden)] = gate
        both_grad[rows, pl.ds(across_hidden, across_hidden)] = up
        for piece in range(wide // width):
            where = pl.ds(piece * width, width)
            partial[rows, where] = (
                cols_product(gate, w_gate[where, :]) + cols_product(up, w_up[where, :])
            ).astype(jnp.bfloat16)

    def work(g):
        def await_one(i):
            s = g * group + i

            @pl.when(s > 0)
            def _():
                ready(s)

        loop(0, group, await_one)
        compute(g)

        def hand_one(i):
            s = g * group + i
            hand(1, s).start()
            hand(0, s).start()

        loop(0, group, hand_one)

    def pair(s):
        hand(1, s).wait_recv()
        mine = partial[at(s), columns(cross, width)].astype(jnp.float32)
        far_out[at(s), :] = (mine + near[1, at(s), :].astype(jnp.float32)).astype(jnp.bfloat16)
        across(s).start()

    def pair_group(g):
        loop(0, group, lambda i: pair(g * group + i))

    def step(g):
        def forward_one(i):
            s = g * group + i

            @pl.when(s > 1)
            def _():
                forward_both(s)

        with jax.named_scope("forward_group"):
            loop(0, group, forward_one)
        with jax.named_scope("work_group"):
            work(g)

    def finish(s):
        hand(0, s).wait_recv()
        across(s).wait_recv()
        mine = partial[at(s), columns(tp, width)].astype(jnp.float32)
        return (
            mine + near[0, at(s), :].astype(jnp.float32) + far_in[at(s), :].astype(jnp.float32)
        ).astype(jnp.bfloat16)

    def finish_one(s):
        total[at(s), :] = finish(s)
        give(s).start()

    def grads(c):
        rows = pl.ds(pl.multiple_of(c * chunk, chunk), chunk)
        sums = rows_product(slots[0, :, rows], both_grad[...])
        gate_sum[rows, :] = sums[:, : sums.shape[1] // 2]
        up_sum[rows, :] = sums[:, sums.shape[1] // 2 :]
        down_sum[:, rows] = rows_product(hidden[...], slots[1, :, rows])

    def finish_group(g):
        def one(i):
            s = g * group + i

            @pl.when(s > 0)
            def _():
                finish_one(s)

            @pl.when(s == 0)
            def _():
                back[pl.ds(0, depth), :] = finish(0)

        loop(0, group, one)

    with jax.named_scope("land_first"):
        for a in (1, 0):
            loop(2, half, lambda k: land(a, k, k))
            land_next(a)
    for i in range(10, 13):
        loads[i].wait()
    with jax.named_scope("tokens"):
        take_tokens()
    with jax.named_scope("land_second"):
        for a in (1,):
            loop(1, half, lambda k: land(a, half + k, k))
    step(0)
    with jax.named_scope("land_second"):
        for a in (0,):
            loop(1, half, lambda k: land(a, half + k, k))
    with jax.named_scope("pair0"):
        pair_group(0)
    with jax.named_scope("filter"):
        @pl.when(me > 0)
        def _():
            halo_later().wait_recv()

        loads[5].wait()
        loads[8].wait()
        filtered[...] = (
            taps[0:1, :] * extended[pl.ds(8, count), :]
            + taps[1:2, :] * extended[pl.ds(7, count), :]
            + taps[2:3, :] * extended[pl.ds(6, count), :]
        )
        mixed[0] = (out_gate[...].astype(jnp.float32) * filtered[...]).astype(jnp.bfloat16)

    mix_early()
    pieces_of = wide // chunk
    step(1)
    step(2)
    with jax.named_scope("pair2"):
        pair_group(2)
    mix_late()
    step(3)
    with jax.named_scope("pair1"):
        pair_group(1)
    with jax.named_scope("pair3"):
        pair_group(3)
    with jax.named_scope("fin0"):
        finish_group(0)
    with jax.named_scope("fin2"):
        finish_group(2)
    with jax.named_scope("grads"):
        loop(0, pieces_of // 4, grads)
    with jax.named_scope("grads"):
        loop(pieces_of // 4, pieces_of // 2, grads)
    with jax.named_scope("fin1"):
        finish_group(1)
    with jax.named_scope("fin3"):
        finish_group(3)
    with jax.named_scope("grads"):
        loop(pieces_of // 2, 3 * pieces_of // 4, grads)
    with jax.named_scope("grads"):
        loop(3 * pieces_of // 4, pieces_of, grads)
    acc[...] = jnp.zeros_like(acc)

    def combine(s):
        @pl.when(s > 0)
        def _():
            give(s).wait_recv()

        mask = jnp.where(placing(0, other(s)), 1.0, 0.0).astype(jnp.bfloat16)
        acc[...] += rows_product(mask, back[at(s), :])

    with jax.named_scope("combine"):
        loop(0, n, combine)
    quarter = token.shape[0]

    def quarter_rows(column):
        return pl.ds(pl.multiple_of(column * quarter, quarter), quarter)

    def exchange(j):
        peer = (cross, diagonal, partner)[j]
        return remote(
            token_out.at[quarter_rows(peer)],
            token.at[:, columns(tp, width)],
            all_send.at[j],
            all_recv.at[j],
            {"tp": peer},
        )

    with jax.named_scope("share"):
        token_out[...] = acc[...].astype(jnp.bfloat16)
        for j in range(3):
            exchange(j).start()
        token[:, columns(tp, width)] = token_out[quarter_rows(tp), :]
        for j in (2, 0, 1):
            exchange(j).wait_recv()

    def total_grad(i):
        here = pl.ds(pl.multiple_of(i * 16, 16), 16)
        rows = pl.ds(pl.multiple_of(tp * quarter + i * 16, 16), 16)
        scale = inverse[rows, :]
        unit = stream[rows, :].astype(jnp.float32) * scale
        unit_grad = token[here, :].astype(jnp.float32) * gain[...]
        along = jnp.mean(unit * unit_grad, axis=-1, keepdims=True)
        value = cot[rows, :].astype(jnp.float32) + scale * (unit_grad - unit * along)
        value = value.astype(jnp.bfloat16)
        stream_grad[rows, :] = value
        for owner in range(n):
            turned[owner, here, :] = value[:, owner * block : (owner + 1) * block]

    with jax.named_scope("stream_grad"):
        loop(0, quarter // 16, total_grad)

    def turn_copy(s):
        return remote(
            turned.at[other(s)],
            turned_all.at[s, quarter_rows(tp)],
            turn_send.at[0],
            turn_recv.at[s],
            {"sp": other(s)},
        )

    def turn_part(s, column, send, recv, peer):
        rows = turned_all.at[s, quarter_rows(column)]
        return remote(rows, rows, send, recv, {"tp": peer})

    def gather(column, j, recv, peer):
        rows = stream_grad.at[quarter_rows(column)]
        return remote(rows, rows, row_send.at[j], row_recv.at[recv], {"tp": peer})

    def turn_spread(s):
        turn_part(s, tp, turn_send.at[1], turn_cross.at[s], cross).start()
        turn_part(s, tp, turn_send.at[2], turn_near.at[s], partner).start()

    def turn_land(s):
        turn_copy(s).wait_recv()
        turn_spread(s)

    def turn_forward(s):
        turn_part(s, cross, turn_send.at[1], turn_cross.at[s], cross).wait_recv()
        turn_part(s, cross, turn_send.at[3], turn_near.at[s], partner).start()

    with jax.named_scope("turn_start"):
        loop(1, n, lambda k: turn_copy(n - k).start())
        gather(tp, 0, 0, cross).start()
        gather(tp, 1, 1, partner).start()
        turned_all[0, quarter_rows(tp), :] = turned[me]
        turn_spread(0)
    with jax.named_scope("gather"):
        gather(cross, 0, 0, cross).wait_recv()
        gather(cross, 2, 2, partner).start()
    with jax.named_scope("turn_land"):
        loop(1, n, turn_land)
    with jax.named_scope("mixed_grad"):
        gather(tp, 1, 1, partner).wait_recv()
        gather(tp, 2, 2, partner).wait_recv()
        loads[9].wait()
        mixed_grad = jnp.dot(stream_grad[...], w_out[...], preferred_element_type=jnp.float32)
        small_out[0] = (mixed_grad * filtered[...]).astype(jnp.bfloat16)
        extended_grad[pl.ds(0, count), :] = mixed_grad * out_gate[...].astype(jnp.float32)

        @pl.when(me > 0)
        def _():
            halo_earlier().start()

        stream_out[...] = stream_grad[:, columns(tp, width)]
    with jax.named_scope("turn_forward"):
        loop(0, n, turn_forward)
    with jax.named_scope("conv_grad"):
        @pl.when(me < n - 1)
        def _():
            halo_earlier().wait_recv()

        product_grad = (
            taps[0:1, :] * extended_grad[pl.ds(0, count), :]
            + taps[1:2, :] * extended_grad[pl.ds(1, count), :]
            + taps[2:3, :] * extended_grad[pl.ds(2, count), :]
        )
        small_out[1] = (product_grad * conv_input[...].astype(jnp.float32)).astype(jnp.bfloat16)
        small_out[2] = (product_grad * in_gate[...].astype(jnp.float32)).astype(jnp.bfloat16)

    w_out_sum[...] = jnp.zeros_like(w_out_sum)

    def out_step(s):
        both = turned_all.at[s, pl.ds(0, 2 * quarter)]
        remote(both, both, turn_send.at[2], turn_near.at[s], {"tp": partner}).wait_recv()

        @pl.when((s > 0) & (s < half))
        def _():
            mix_copy(0, s, s).wait_recv()

        @pl.when(s > half)
        def _():
            mix_copy(half, s, s - half).wait_recv()

        w_out_sum[...] += rows_product(turned_all[s], mixed[s])

    with jax.named_scope("w_out_grad"):
        loop(0, n, out_step)

    with jax.named_scope("drain"):
        for one in route_copies():
            one.wait_send()
        for a in (0, 1):
            token_copy(a).wait_send()
            sent = sending.at[a, pl.ds(0, (n - 1) * depth)]
            remote(sent, sent, slot_send.at[a], slot_recv.at[a, 0], {"tp": partner}).wait_send()
            most = slots.at[a, pl.ds(0, (n - 1) * depth), pl.ds(0, width)]
            for sem in (near_send, fwd_send):
                remote(most, most, sem.at[a], near_recv.at[a, 0], {"tp": partner}).wait_send()
            most = slots.at[a, pl.ds(0, (n - 2) * depth), pl.ds(0, width)]
            remote(most, most, cross_send.at[a], near_recv.at[a, 0], {"tp": cross}).wait_send()
            remote(far_out, far_in, hand_send.at[a], hand_recv.at[a, 0], {"tp": partner}).wait_send()
        remote(far_out, far_in, far_send, far_recv.at[0], {"tp": cross}).wait_send()
        rest = total.at[pl.ds(0, (n - 1) * depth)]
        remote(rest, rest, out_send, out_recv.at[0], {"tp": partner}).wait_send()
        sent = mixed.at[pl.ds(0, n - 1)]
        remote(sent, sent, mix_send, mix_recv.at[0], {"tp": partner}).wait_send()
        sent = turned_all.at[pl.ds(0, n - 1), pl.ds(0, quarter)]
        remote(sent, sent, turn_send.at[0], turn_recv.at[0], {"tp": partner}).wait_send()
        sent = turned_all.at[:, pl.ds(0, quarter)]
        for kind in range(1, 4):
            remote(sent, sent, turn_send.at[kind], turn_recv.at[0], {"tp": partner}).wait_send()
        for j in range(3):
            exchange(j).wait_send()
            gather(tp, j, j, partner).wait_send()

        @pl.when(me < n - 1)
        def _():
            halo_later().wait_send()

        @pl.when(me > 0)
        def _():
            halo_earlier().wait_send()


def store_kernel(stream, small, w_out, gate, up, down, *rest):
    outs, local = rest[:8], rest[8]
    ins = (stream, small.at[0], small.at[1], small.at[2], w_out, gate, up, down)
    copies = [
        pltpu.make_async_copy(source, target, local.at[i])
        for i, (source, target) in enumerate(zip(ins, outs))
    ]
    for one in copies:
        one.start()
    for one in copies:
        one.wait()


def shards(
    cotangent,
    stream_in,
    norm_gain,
    out_gate,
    in_gate,
    conv_input,
    conv_taps,
    out_weight,
    expert_gate,
    expert_up,
    expert_down,
    expert_choice,
    route_scale,
):
    n = lax.axis_size("sp")
    count, wide = stream_in.shape
    channels = out_gate.shape[1]
    hidden = expert_gate.shape[2]
    width = wide // lax.axis_size("tp")
    depth = 4 * count // n
    rows = n * depth
    block = wide // n
    quarter = count // lax.axis_size("tp")
    kind = stream_in.dtype

    def out(*shape, dtype=kind):
        return jax.ShapeDtypeStruct(shape, dtype)

    def full(*shape):
        return pltpu.VMEM(shape, jnp.float32)

    def held(*shape):
        return pltpu.VMEM(shape, kind)

    vmem, anywhere = (pl.BlockSpec(memory_space=pltpu.VMEM), pl.BlockSpec(memory_space=pl.ANY))
    dma = pltpu.SemaphoreType.DMA
    operands = (
        stream_in,
        cotangent,
        norm_gain[None],
        expert_choice.T,
        route_scale.T,
        out_gate,
        in_gate,
        conv_input,
        conv_taps,
        out_weight,
        expert_gate[0],
        expert_up[0],
        expert_down[0],
    )
    results = pl.pallas_call(
        functools.partial(step_kernel, n),
        out_shape=[
            out(count, width),
            out(3, count, channels),
            out(block, channels, dtype=jnp.float32),
            out(wide, hidden, dtype=jnp.float32),
            out(wide, hidden, dtype=jnp.float32),
            out(hidden, wide, dtype=jnp.float32),
        ],
        in_specs=[anywhere] * 13,
        out_specs=[vmem] * 6,
        scratch_shapes=[pltpu.VMEM(x.shape, x.dtype) for x in operands]
        + [
            held(count, wide),
            full(count, 1),
            full(2, n, count),
            full(2, n, count),
            held(2, count, width),
            pltpu.VMEM((2, count), jnp.int32),
            full(2, count),
            held(2, rows, width),
            held(2, rows, wide),
            held(rows, hidden),
            held(rows, 2 * hidden),
            held(rows, wide),
            held(2, rows, width),
            held(rows, width),
            held(rows, width),
            held(rows, width),
            held(rows, width),
            full(count, width),
            held(quarter, wide),
            held(count, width),
            full(count + 8, channels),
            full(count, channels),
            full(count + 8, channels),
            held(n, count, channels),
            held(count, wide),
            held(n, quarter, block),
            held(n, count, block),
            dma((13,)),
            dma((4,)),
            dma((4,)),
            dma((2,)),
            dma((2, n)),
            dma((2,)),
            dma((2, n)),
            dma((2,)),
            dma((2,)),
            dma((2, n)),
            dma((2,)),
            dma((2, n)),
            dma,
            dma((n,)),
            dma,
            dma((n,)),
            dma((3,)),
            dma((3,)),
            dma((3,)),
            dma((3,)),
            dma((2,)),
            dma((2,)),
            dma,
            dma((n,)),
            dma((4,)),
            dma((n,)),
            dma((n,)),
            dma((n,)),
        ],
        compiler_params=pltpu.CompilerParams(
            collective_id=1, has_side_effects=True, vmem_limit_bytes=VMEM + 3 * n * count * channels
        ),
    )(*(pltpu.with_memory_space_constraint(x, pltpu.HBM) for x in operands))
    stored = pl.pallas_call(
        store_kernel,
        out_shape=[
            out(count, width),
            out(count, channels),
            out(count, channels),
            out(count, channels),
            out(block, channels, dtype=jnp.float32),
            out(wide, hidden, dtype=jnp.float32),
            out(wide, hidden, dtype=jnp.float32),
            out(hidden, wide, dtype=jnp.float32),
        ],
        in_specs=[vmem] * 6,
        out_specs=[anywhere] * 8,
        scratch_shapes=[dma((8,))],
        compiler_params=pltpu.CompilerParams(vmem_limit_bytes=9 * 1024 * 1024),
    )(*results)
    return (*stored[:5], *(grad[None] for grad in stored[5:]))


def solution(mesh):
    placed = (
        P("sp", None),
        P("sp", None),
        P(),
        P("sp", "tp"),
        P("sp", "tp"),
        P("sp", "tp"),
        P(None, "tp"),
        P(None, "tp"),
        P("sp", None, "tp"),
        P("sp", None, "tp"),
        P("sp", "tp", None),
        P("sp", None),
        P("sp", None),
    )
    return jax.shard_map(
        shards,
        mesh=mesh,
        in_specs=placed,
        out_specs=(
            P("sp", "tp"),
            P("sp", "tp"),
            P("sp", "tp"),
            P("sp", "tp"),
            P("sp", "tp"),
            P("sp", None, "tp"),
            P("sp", None, "tp"),
            P("sp", "tp", None),
        ),
        check_vma=False,
    )
```

```python
import functools

import jax
import jax.numpy as jnp
from jax import lax
from jax.experimental import pallas as pl
from jax.experimental.pallas import tpu as pltpu
from jax.sharding import PartitionSpec as P

norm_eps = 1e-06
VMEM = 83 * 512 * 1024


def rows_product(left, right):
    return lax.dot_general(
        left, right, (((0,), (0,)), ((), ())), preferred_element_type=jnp.float32
    )


def cols_product(left, right):
    return lax.dot_general(
        left, right, (((1,), (1,)), ((), ())), preferred_element_type=jnp.float32
    )


MESH = pl.DeviceIdType.MESH


def remote(source, target, send_sem, recv_sem, device):
    return pltpu.make_async_remote_copy(
        src_ref=source,
        dst_ref=target,
        send_sem=send_sem,
        recv_sem=recv_sem,
        device_id=device,
        device_id_type=MESH,
    )


def columns(index, width):
    return pl.ds(pl.multiple_of(index * width, width), width)


def mirrored(me, mask, n):
    found, unit = 0, 1
    while unit < n:
        found = found + lax.rem(lax.div(me, unit) + lax.div(mask, unit), 2) * unit
        unit = 2 * unit
    return found


def tp_places():
    tp, count = lax.axis_index("tp"), lax.axis_size("tp")
    cross = lax.rem(tp + count // 2, count)
    partner = tp + 1 - 2 * lax.rem(tp, 2)
    return (tp, cross, partner, lax.rem(partner + count // 2, count))


def greet(peers):
    barrier = pltpu.get_barrier_semaphore()
    for peer in peers:
        pl.semaphore_signal(barrier, inc=1, device_id={"tp": peer}, device_id_type=MESH)
    me, n = lax.axis_index("sp"), lax.axis_size("sp")

    def greet_one(k, carry):
        peer = lax.rem(me + k, n)
        pl.semaphore_signal(barrier, inc=1, device_id={"sp": peer}, device_id_type=MESH)
        return carry

    lax.fori_loop(1, n, greet_one, 0)
    return lambda: pl.semaphore_wait(barrier, n - 1 + len(peers))


def loop(low, high, body):
    def step(k, carry):
        body(k)
        return carry

    lax.fori_loop(low, high, step, 0)


def step_kernel(
    n,
    *refs,
):
    inputs, refs = refs[:13], refs[13:]
    (
        stream_out,
        small_out,
        w_out_sum,
        gate_sum,
        up_sum,
        down_sum,
        normed,
        inverse,
        keys,
        weights,
        arrived,
        arrived_choice,
        arrived_scales,
        sending,
        slots,
        hidden,
        both_grad,
        partial,
        near,
        far_out,
        far_in,
        total,
        back,
        acc,
        token,
        token_out,
        extended,
        filtered,
        extended_grad,
        mixed,
        stream_grad,
        turned,
        turned_all,
        load,
        tok_send,
        tok_recv,
        slot_send,
        slot_recv,
        cross_send,
        cross_recv,
        near_send,
        fwd_send,
        near_recv,
        hand_send,
        hand_recv,
        far_send,
        far_recv,
        out_send,
        out_recv,
        all_send,
        all_recv,
        row_send,
        row_recv,
        halo_send,
        halo_recv,
        mix_send,
        mix_recv,
        turn_send,
        turn_recv,
        turn_cross,
        turn_near,
    ) = refs[:6] + refs[19:]
    loaded = refs[6:19]
    (
        stream,
        cot,
        gain,
        choice,
        scales,
        out_gate,
        in_gate,
        conv_input,
        taps,
        w_out,
        w_gate,
        w_up,
        w_down,
    ) = loaded
    me = lax.axis_index("sp")
    tp, cross, partner, diagonal = tp_places()
    half = n // 2
    count, wide = normed.shape
    width = acc.shape[1]
    depth = near.shape[1] // n
    group = max(1, n // 4)
    span = group * depth
    chunk = min(256, width)
    channels = filtered.shape[1]
    block = wide // n
    wait_all = greet((cross, partner, diagonal))
    sources = (normed, cot)
    loads = [
        pltpu.make_async_copy(source, target, load.at[i])
        for i, (source, target) in enumerate(zip(inputs, loaded))
    ]
    for i in (3, 4, 1, 0, 2, 6, 7, 5, 8, 10, 11, 12, 9):
        loads[i].start()

    def other(s):
        return mirrored(me, jnp.int32(s), n)

    def at(s):
        return pl.ds(pl.multiple_of(s * depth, depth), depth)

    def normalize(i):
        rows = pl.ds(pl.multiple_of(i * 32, 32), 32)
        values = stream[rows, :].astype(jnp.float32)
        scale = lax.rsqrt(jnp.mean(values * values, axis=-1, keepdims=True) + norm_eps)
        inverse[rows, :] = scale
        normed[rows, :] = (values * scale * gain[...]).astype(jnp.bfloat16)

    def table(which, named, scaled):
        c0, c1 = (named[i : i + 1, :] for i in range(2))
        s0, s1 = (scaled[i : i + 1, :] for i in range(2))
        expert = lax.broadcasted_iota(jnp.int32, (n, count), 0)
        first, second = (c0 == expert, c1 == expert)
        member = jnp.where(first | second, 1.0, 0.0)
        row = lax.broadcasted_iota(jnp.int32, (count, count), 0)
        column = lax.broadcasted_iota(jnp.int32, (count, count), 1)
        before = jnp.where(row < column, 1.0, 0.0).astype(jnp.bfloat16)
        earlier = jnp.dot(
            member.astype(jnp.bfloat16), before, preferred_element_type=jnp.float32
        )
        keys[which] = jnp.where(member > 0.0, earlier, -1.0)
        weights[which] = jnp.where(first, s0, 0.0) + jnp.where(second, s1, 0.0)

    def placing(which, expert):
        slot = lax.broadcasted_iota(jnp.int32, (depth, count), 0).astype(jnp.float32)
        return slot == keys[which, pl.ds(expert, 1), :]

    def chosen(a, which, expert, values):
        mask = placing(which, expert)
        found = jnp.dot(
            jnp.where(mask, 1.0, 0.0).astype(jnp.bfloat16),
            values,
            preferred_element_type=jnp.float32,
        )
        if a == 1:
            weight = jnp.where(mask, weights[which, pl.ds(expert, 1), :], 0.0)
            found = found * jnp.sum(weight, axis=1, keepdims=True)
        return found.astype(jnp.bfloat16)

    def token_copy(a):
        return remote(
            sources[a].at[:, columns(tp, width)],
            arrived.at[a],
            tok_send.at[a],
            tok_recv.at[a],
            {"sp": other(half)},
        )

    def route_copies():
        pairs = ((choice, arrived_choice), (scales, arrived_scales))
        return [
            remote(source, target, tok_send.at[2 + i], tok_recv.at[2 + i], {"sp": other(half)})
            for i, (source, target) in enumerate(pairs)
        ]

    def slot_copy(a, s, k):
        return remote(
            sending.at[a, at(s)],
            slots.at[a, at(s), columns(tp, width)],
            slot_send.at[a],
            slot_recv.at[a, s],
            {"sp": other(k)},
        )

    def spread(a, s):
        part = slots.at[a, at(s), columns(tp, width)]
        remote(part, part, cross_send.at[a], cross_recv.at[a, s], {"tp": cross}).start()
        remote(part, part, near_send.at[a], near_recv.at[a, s], {"tp": partner}).start()

    def forward(a, s):
        part = slots.at[a, at(s), columns(cross, width)]
        remote(part, part, cross_send.at[a], cross_recv.at[a, s], {"tp": cross}).wait_recv()
        remote(part, part, fwd_send.at[a], near_recv.at[a, s], {"tp": partner}).start()

    def ready(s):
        for a in (0, 1):
            both = slots.at[a, at(s), pl.ds(0, 2 * width)]
            remote(both, both, near_send.at[a], near_recv.at[a, s], {"tp": partner}).wait_recv()

    def hand(j, s):
        return remote(
            partial.at[at(s), columns((partner, diagonal)[j], width)],
            near.at[j, at(s)],
            hand_send.at[j],
            hand_recv.at[j, s],
            {"tp": partner},
        )

    def across(s):
        return remote(
            far_out.at[at(s)], far_in.at[at(s)], far_send, far_recv.at[s], {"tp": cross}
        )

    def give(s):
        return remote(
            total.at[at(s)], back.at[at(s)], out_send, out_recv.at[s], {"sp": other(s)}
        )

    def halo_later():
        peer = lax.rem(me + 1, n)
        return remote(
            extended.at[pl.ds(count, 8)],
            extended.at[pl.ds(0, 8)],
            halo_send.at[0],
            halo_recv.at[0],
            {"sp": peer},
        )

    def halo_earlier():
        peer = lax.rem(me + n - 1, n)
        return remote(
            extended_grad.at[pl.ds(0, 8)],
            extended_grad.at[pl.ds(count, 8)],
            halo_send.at[1],
            halo_recv.at[1],
            {"sp": peer},
        )

    def mix_copy(source, target, k):
        return remote(
            mixed.at[source], mixed.at[target], mix_send, mix_recv.at[target], {"sp": other(k)}
        )

    def send_own(a, k):
        values = sources[a][:, columns(tp, width)]
        sending[a, at(k), :] = chosen(a, 0, other(k), values)
        slot_copy(a, k, k).start()

    def next_copy(a):
        return remote(
            sending.at[a, at(0)],
            slots.at[a, at(1), columns(cross, width)],
            slot_send.at[a],
            slot_recv.at[a, 1],
            {"sp": other(1)},
        )

    def send_next(a):
        send_own(a, 1)
        values = sources[a][:, columns(cross, width)]
        sending[a, at(0), :] = chosen(a, 0, other(1), values)
        next_copy(a).start()

    def land_next(a):
        both = slots.at[a, at(1), pl.ds(0, 2 * width)]
        remote(both, both, slot_send.at[a], slot_recv.at[a, 1], {"sp": other(1)}).wait_recv()
        for column, sem in ((tp, near_send), (cross, fwd_send)):
            part = slots.at[a, at(1), columns(column, width)]
            remote(part, part, sem.at[a], near_recv.at[a, 1], {"tp": partner}).start()

    with jax.named_scope("prep"):
        loads[3].wait()
        loads[4].wait()
        table(0, choice, scales)
        loads[1].wait()
    with jax.named_scope("barrier"):
        wait_all()
    with jax.named_scope("send_own"):
        for one in route_copies():
            one.start()
        loop(2, half, lambda k: send_own(1, k))
        send_next(1)
        token_copy(1).start()
        with jax.named_scope("conv"):
            loads[6].wait()
            loads[7].wait()
            product = in_gate[...].astype(jnp.float32) * conv_input[...].astype(jnp.float32)
            extended[pl.ds(8, count), :] = product

            @pl.when(me == 0)
            def _():
                extended[pl.ds(0, 8), :] = jnp.zeros((8, channels), jnp.float32)

            @pl.when(me == n - 1)
            def _():
                extended_grad[pl.ds(count, 8), :] = jnp.zeros((8, channels), jnp.float32)

            @pl.when(me < n - 1)
            def _():
                halo_later().start()
        loads[0].wait()
        loads[2].wait()
        loop(0, count // 32, normalize)
        loop(2, half, lambda k: send_own(0, k))
        send_next(0)
        token_copy(0).start()
    with jax.named_scope("own_block"):
        for a in (0, 1):
            for piece in range(wide // width):
                where = pl.ds(piece * width, width)
                slots[a, pl.ds(0, depth), where] = chosen(a, 0, me, sources[a][:, where])

    def land(a, s, k):
        slot_copy(a, s, k).wait_recv()
        spread(a, s)

    def take_tokens():
        for a in (1, 0):
            if a == 1:
                for one in route_copies():
                    one.wait_recv()
                table(1, arrived_choice, arrived_scales)
            token_copy(a).wait_recv()

            def send_other(k):
                sending[a, at(half + k), :] = chosen(a, 1, other(k), arrived[a])
                slot_copy(a, half + k, k).start()

            loop(1, half, send_other)
            slots[a, at(half), columns(tp, width)] = chosen(a, 1, me, arrived[a])
            spread(a, half)

    def forward_both(s):
        for a in (0, 1):
            forward(a, s)

    def mix_early():
        mix_copy(0, half, half).start()
        loop(1, half, lambda k: mix_copy(0, k, k).start())

    def mix_late():
        mix_copy(half, half, half).wait_recv()
        loop(1, half, lambda k: mix_copy(half, half + k, k).start())

    def compute(g):
        rows = pl.ds(pl.multiple_of(g * span, span), span)
        picked, scaled = (slots[0, rows, :], slots[1, rows, :])
        gate_pre = jnp.dot(picked, w_gate[...], preferred_element_type=jnp.float32)
        up_pre = jnp.dot(picked, w_up[...], preferred_element_type=jnp.float32)
        hidden_grad = cols_product(scaled, w_down[...])
        sigmoid_gate = jax.nn.sigmoid(gate_pre)
        silu_gate = gate_pre * sigmoid_gate
        hidden[rows, :] = (silu_gate * up_pre).astype(jnp.bfloat16)
        gate = (
            hidden_grad * up_pre * sigmoid_gate * (1.0 + gate_pre * (1.0 - sigmoid_gate))
        ).astype(jnp.bfloat16)
        up = (hidden_grad * silu_gate).astype(jnp.bfloat16)
        across_hidden = gate.shape[1]
        both_grad[rows, pl.ds(0, across_hidden)] = gate
        both_grad[rows, pl.ds(across_hidden, across_hidden)] = up
        for piece in range(wide // width):
            where = pl.ds(piece * width, width)
            partial[rows, where] = (
                cols_product(gate, w_gate[where, :]) + cols_product(up, w_up[where, :])
            ).astype(jnp.bfloat16)

    def work(g):
        def await_one(i):
            s = g * group + i

            @pl.when(s > 0)
            def _():
                ready(s)

        loop(0, group, await_one)
        compute(g)

        def hand_one(i):
            s = g * group + i
            hand(1, s).start()
            hand(0, s).start()

        loop(0, group, hand_one)

    def pair(s):
        hand(1, s).wait_recv()
        mine = partial[at(s), columns(cross, width)].astype(jnp.float32)
        far_out[at(s), :] = (mine + near[1, at(s), :].astype(jnp.float32)).astype(jnp.bfloat16)
        across(s).start()

    def pair_group(g):
        loop(0, group, lambda i: pair(g * group + i))

    def step(g):
        def forward_one(i):
            s = g * group + i

            @pl.when(s > 1)
            def _():
                forward_both(s)

        with jax.named_scope("forward_group"):
            loop(0, group, forward_one)
        with jax.named_scope("work_group"):
            work(g)

    def finish(s):
        hand(0, s).wait_recv()
        across(s).wait_recv()
        mine = partial[at(s), columns(tp, width)].astype(jnp.float32)
        return (
            mine + near[0, at(s), :].astype(jnp.float32) + far_in[at(s), :].astype(jnp.float32)
        ).astype(jnp.bfloat16)

    def finish_one(s):
        total[at(s), :] = finish(s)
        give(s).start()

    def grads(c):
        rows = pl.ds(pl.multiple_of(c * chunk, chunk), chunk)
        sums = rows_product(slots[0, :, rows], both_grad[...])
        gate_sum[rows, :] = sums[:, : sums.shape[1] // 2]
        up_sum[rows, :] = sums[:, sums.shape[1] // 2 :]
        down_sum[:, rows] = rows_product(hidden[...], slots[1, :, rows])

    def finish_group(g):
        def one(i):
            s = g * group + i

            @pl.when(s > 0)
            def _():
                finish_one(s)

            @pl.when(s == 0)
            def _():
                back[pl.ds(0, depth), :] = finish(0)

        loop(0, group, one)

    with jax.named_scope("land_first"):
        for a in (1, 0):
            loop(2, half, lambda k: land(a, k, k))
            land_next(a)
    for i in range(10, 13):
        loads[i].wait()
    with jax.named_scope("tokens"):
        take_tokens()
    with jax.named_scope("land_second"):
        for a in (1,):
            loop(1, half, lambda k: land(a, half + k, k))
    step(0)
    with jax.named_scope("land_second"):
        for a in (0,):
            loop(1, half, lambda k: land(a, half + k, k))
    with jax.named_scope("pair0"):
        pair_group(0)
    with jax.named_scope("filter"):
        @pl.when(me > 0)
        def _():
            halo_later().wait_recv()

        loads[5].wait()
        loads[8].wait()
        filtered[...] = (
            taps[0:1, :] * extended[pl.ds(8, count), :]
            + taps[1:2, :] * extended[pl.ds(7, count), :]
            + taps[2:3, :] * extended[pl.ds(6, count), :]
        )
        mixed[0] = (out_gate[...].astype(jnp.float32) * filtered[...]).astype(jnp.bfloat16)

    mix_early()
    pieces_of = wide // chunk
    step(1)
    step(2)
    with jax.named_scope("pair2"):
        pair_group(2)
    mix_late()
    step(3)
    with jax.named_scope("pair1"):
        pair_group(1)
    with jax.named_scope("pair3"):
        pair_group(3)
    with jax.named_scope("fin0"):
        finish_group(0)
    with jax.named_scope("fin2"):
        finish_group(2)
    with jax.named_scope("grads"):
        loop(0, pieces_of // 4, grads)
    with jax.named_scope("grads"):
        loop(pieces_of // 4, pieces_of // 2, grads)
    with jax.named_scope("fin1"):
        finish_group(1)
    with jax.named_scope("fin3"):
        finish_group(3)
    with jax.named_scope("grads"):
        loop(pieces_of // 2, 3 * pieces_of // 4, grads)
    with jax.named_scope("grads"):
        loop(3 * pieces_of // 4, pieces_of, grads)
    acc[...] = jnp.zeros_like(acc)

    def combine(s):
        @pl.when(s > 0)
        def _():
            give(s).wait_recv()

        mask = jnp.where(placing(0, other(s)), 1.0, 0.0).astype(jnp.bfloat16)
        acc[...] += rows_product(mask, back[at(s), :])

    with jax.named_scope("combine"):
        loop(0, n, combine)
    quarter = token.shape[0]

    def quarter_rows(column):
        return pl.ds(pl.multiple_of(column * quarter, quarter), quarter)

    def exchange(j):
        peer = (cross, diagonal, partner)[j]
        return remote(
            token_out.at[quarter_rows(peer)],
            token.at[:, columns(tp, width)],
            all_send.at[j],
            all_recv.at[j],
            {"tp": peer},
        )

    with jax.named_scope("share"):
        token_out[...] = acc[...].astype(jnp.bfloat16)
        for j in range(3):
            exchange(j).start()
        token[:, columns(tp, width)] = token_out[quarter_rows(tp), :]
        for j in (2, 0, 1):
            exchange(j).wait_recv()

    def total_grad(i):
        here = pl.ds(pl.multiple_of(i * 16, 16), 16)
        rows = pl.ds(pl.multiple_of(tp * quarter + i * 16, 16), 16)
        scale = inverse[rows, :]
        unit = stream[rows, :].astype(jnp.float32) * scale
        unit_grad = token[here, :].astype(jnp.float32) * gain[...]
        along = jnp.mean(unit * unit_grad, axis=-1, keepdims=True)
        value = cot[rows, :].astype(jnp.float32) + scale * (unit_grad - unit * along)
        value = value.astype(jnp.bfloat16)
        stream_grad[rows, :] = value
        for owner in range(n):
            turned[owner, here, :] = value[:, owner * block : (owner + 1) * block]

    with jax.named_scope("stream_grad"):
        loop(0, quarter // 16, total_grad)

    def turn_copy(s):
        return remote(
            turned.at[other(s)],
            turned_all.at[s, quarter_rows(tp)],
            turn_send.at[0],
            turn_recv.at[s],
            {"sp": other(s)},
        )

    def turn_part(s, column, send, recv, peer):
        rows = turned_all.at[s, quarter_rows(column)]
        return remote(rows, rows, send, recv, {"tp": peer})

    def gather(column, j, recv, peer):
        rows = stream_grad.at[quarter_rows(column)]
        return remote(rows, rows, row_send.at[j], row_recv.at[recv], {"tp": peer})

    def turn_spread(s):
        turn_part(s, tp, turn_send.at[1], turn_cross.at[s], cross).start()
        turn_part(s, tp, turn_send.at[2], turn_near.at[s], partner).start()

    def turn_land(s):
        turn_copy(s).wait_recv()
        turn_spread(s)

    def turn_forward(s):
        turn_part(s, cross, turn_send.at[1], turn_cross.at[s], cross).wait_recv()
        turn_part(s, cross, turn_send.at[3], turn_near.at[s], partner).start()

    with jax.named_scope("turn_start"):
        loop(1, n, lambda k: turn_copy(n - k).start())
        gather(tp, 1, 1, partner).start()
        turned_all[0, quarter_rows(tp), :] = turned[me]
        turn_spread(0)
        gather(tp, 0, 0, cross).start()
    with jax.named_scope("turn_land"):
        loop(1, n, turn_land)
    with jax.named_scope("gather"):
        gather(cross, 0, 0, cross).wait_recv()
        gather(cross, 2, 2, partner).start()
    with jax.named_scope("mixed_grad"):
        gather(tp, 1, 1, partner).wait_recv()
        gather(tp, 2, 2, partner).wait_recv()
        loads[9].wait()
        mixed_grad = jnp.dot(stream_grad[...], w_out[...], preferred_element_type=jnp.float32)
        small_out[0] = (mixed_grad * filtered[...]).astype(jnp.bfloat16)
        extended_grad[pl.ds(0, count), :] = mixed_grad * out_gate[...].astype(jnp.float32)

        @pl.when(me > 0)
        def _():
            halo_earlier().start()

        stream_out[...] = stream_grad[:, columns(tp, width)]
    with jax.named_scope("turn_forward"):
        loop(0, n, turn_forward)
    with jax.named_scope("conv_grad"):
        @pl.when(me < n - 1)
        def _():
            halo_earlier().wait_recv()

        product_grad = (
            taps[0:1, :] * extended_grad[pl.ds(0, count), :]
            + taps[1:2, :] * extended_grad[pl.ds(1, count), :]
            + taps[2:3, :] * extended_grad[pl.ds(2, count), :]
        )
        small_out[1] = (product_grad * conv_input[...].astype(jnp.float32)).astype(jnp.bfloat16)
        small_out[2] = (product_grad * in_gate[...].astype(jnp.float32)).astype(jnp.bfloat16)

    w_out_sum[...] = jnp.zeros_like(w_out_sum)

    def out_step(s):
        both = turned_all.at[s, pl.ds(0, 2 * quarter)]
        remote(both, both, turn_send.at[2], turn_near.at[s], {"tp": partner}).wait_recv()

        @pl.when((s > 0) & (s < half))
        def _():
            mix_copy(0, s, s).wait_recv()

        @pl.when(s > half)
        def _():
            mix_copy(half, s, s - half).wait_recv()

        w_out_sum[...] += rows_product(turned_all[s], mixed[s])

    with jax.named_scope("w_out_grad"):
        loop(0, n, out_step)

    with jax.named_scope("drain"):
        for one in route_copies():
            one.wait_send()
        for a in (0, 1):
            token_copy(a).wait_send()
            sent = sending.at[a, pl.ds(0, (n - 1) * depth)]
            remote(sent, sent, slot_send.at[a], slot_recv.at[a, 0], {"tp": partner}).wait_send()
            most = slots.at[a, pl.ds(0, (n - 1) * depth), pl.ds(0, width)]
            for sem in (near_send, fwd_send):
                remote(most, most, sem.at[a], near_recv.at[a, 0], {"tp": partner}).wait_send()
            most = slots.at[a, pl.ds(0, (n - 2) * depth), pl.ds(0, width)]
            remote(most, most, cross_send.at[a], near_recv.at[a, 0], {"tp": cross}).wait_send()
            remote(far_out, far_in, hand_send.at[a], hand_recv.at[a, 0], {"tp": partner}).wait_send()
        remote(far_out, far_in, far_send, far_recv.at[0], {"tp": cross}).wait_send()
        rest = total.at[pl.ds(0, (n - 1) * depth)]
        remote(rest, rest, out_send, out_recv.at[0], {"tp": partner}).wait_send()
        sent = mixed.at[pl.ds(0, n - 1)]
        remote(sent, sent, mix_send, mix_recv.at[0], {"tp": partner}).wait_send()
        sent = turned_all.at[pl.ds(0, n - 1), pl.ds(0, quarter)]
        remote(sent, sent, turn_send.at[0], turn_recv.at[0], {"tp": partner}).wait_send()
        sent = turned_all.at[:, pl.ds(0, quarter)]
        for kind in range(1, 4):
            remote(sent, sent, turn_send.at[kind], turn_recv.at[0], {"tp": partner}).wait_send()
        for j in range(3):
            exchange(j).wait_send()
            gather(tp, j, j, partner).wait_send()

        @pl.when(me < n - 1)
        def _():
            halo_later().wait_send()

        @pl.when(me > 0)
        def _():
            halo_earlier().wait_send()


def store_kernel(stream, small, w_out, gate, up, down, *rest):
    outs, local = rest[:8], rest[8]
    ins = (stream, small.at[0], small.at[1], small.at[2], w_out, gate, up, down)
    copies = [
        pltpu.make_async_copy(source, target, local.at[i])
        for i, (source, target) in enumerate(zip(ins, outs))
    ]
    for one in copies:
        one.start()
    for one in copies:
        one.wait()


def shards(
    cotangent,
    stream_in,
    norm_gain,
    out_gate,
    in_gate,
    conv_input,
    conv_taps,
    out_weight,
    expert_gate,
    expert_up,
    expert_down,
    expert_choice,
    route_scale,
):
    n = lax.axis_size("sp")
    count, wide = stream_in.shape
    channels = out_gate.shape[1]
    hidden = expert_gate.shape[2]
    width = wide // lax.axis_size("tp")
    depth = 4 * count // n
    rows = n * depth
    block = wide // n
    quarter = count // lax.axis_size("tp")
    kind = stream_in.dtype

    def out(*shape, dtype=kind):
        return jax.ShapeDtypeStruct(shape, dtype)

    def full(*shape):
        return pltpu.VMEM(shape, jnp.float32)

    def held(*shape):
        return pltpu.VMEM(shape, kind)

    vmem, anywhere = (pl.BlockSpec(memory_space=pltpu.VMEM), pl.BlockSpec(memory_space=pl.ANY))
    dma = pltpu.SemaphoreType.DMA
    operands = (
        stream_in,
        cotangent,
        norm_gain[None],
        expert_choice.T,
        route_scale.T,
        out_gate,
        in_gate,
        conv_input,
        conv_taps,
        out_weight,
        expert_gate[0],
        expert_up[0],
        expert_down[0],
    )
    results = pl.pallas_call(
        functools.partial(step_kernel, n),
        out_shape=[
            out(count, width),
            out(3, count, channels),
            out(block, channels, dtype=jnp.float32),
            out(wide, hidden, dtype=jnp.float32),
            out(wide, hidden, dtype=jnp.float32),
            out(hidden, wide, dtype=jnp.float32),
        ],
        in_specs=[anywhere] * 13,
        out_specs=[vmem] * 6,
        scratch_shapes=[pltpu.VMEM(x.shape, x.dtype) for x in operands]
        + [
            held(count, wide),
            full(count, 1),
            full(2, n, count),
            full(2, n, count),
            held(2, count, width),
            pltpu.VMEM((2, count), jnp.int32),
            full(2, count),
            held(2, rows, width),
            held(2, rows, wide),
            held(rows, hidden),
            held(rows, 2 * hidden),
            held(rows, wide),
            held(2, rows, width),
            held(rows, width),
            held(rows, width),
            held(rows, width),
            held(rows, width),
            full(count, width),
            held(quarter, wide),
            held(count, width),
            full(count + 8, channels),
            full(count, channels),
            full(count + 8, channels),
            held(n, count, channels),
            held(count, wide),
            held(n, quarter, block),
            held(n, count, block),
            dma((13,)),
            dma((4,)),
            dma((4,)),
            dma((2,)),
            dma((2, n)),
            dma((2,)),
            dma((2, n)),
            dma((2,)),
            dma((2,)),
            dma((2, n)),
            dma((2,)),
            dma((2, n)),
            dma,
            dma((n,)),
            dma,
            dma((n,)),
            dma((3,)),
            dma((3,)),
            dma((3,)),
            dma((3,)),
            dma((2,)),
            dma((2,)),
            dma,
            dma((n,)),
            dma((4,)),
            dma((n,)),
            dma((n,)),
            dma((n,)),
        ],
        compiler_params=pltpu.CompilerParams(
            collective_id=1, has_side_effects=True, vmem_limit_bytes=VMEM + 3 * n * count * channels
        ),
    )(*(pltpu.with_memory_space_constraint(x, pltpu.HBM) for x in operands))
    stored = pl.pallas_call(
        store_kernel,
        out_shape=[
            out(count, width),
            out(count, channels),
            out(count, channels),
            out(count, channels),
            out(block, channels, dtype=jnp.float32),
            out(wide, hidden, dtype=jnp.float32),
            out(wide, hidden, dtype=jnp.float32),
            out(hidden, wide, dtype=jnp.float32),
        ],
        in_specs=[vmem] * 6,
        out_specs=[anywhere] * 8,
        scratch_shapes=[dma((8,))],
        compiler_params=pltpu.CompilerParams(vmem_limit_bytes=9 * 1024 * 1024),
    )(*results)
    return (*stored[:5], *(grad[None] for grad in stored[5:]))


def solution(mesh):
    placed = (
        P("sp", None),
        P("sp", None),
        P(),
        P("sp", "tp"),
        P("sp", "tp"),
        P("sp", "tp"),
        P(None, "tp"),
        P(None, "tp"),
        P("sp", None, "tp"),
        P("sp", None, "tp"),
        P("sp", "tp", None),
        P("sp", None),
        P("sp", None),
    )
    return jax.shard_map(
        shards,
        mesh=mesh,
        in_specs=placed,
        out_specs=(
            P("sp", "tp"),
            P("sp", "tp"),
            P("sp", "tp"),
            P("sp", "tp"),
            P("sp", "tp"),
            P("sp", None, "tp"),
            P("sp", None, "tp"),
            P("sp", "tp", None),
        ),
        check_vma=False,
    )
```
